256 devices in a mesh: ep: 64 (over z, x, core), tp: 4 (over y).
Axes of the slice: x: 4, y: 4, z: 8, core: 2. Of those that a mesh axis runs over, the one named last changes fastest.
Arguments:
- pool_in: bfloat16 [65536, 1024], P(('ep', 'tp')), may hold values from -6 to 6
- w_pool: bfloat16 [8, 128, 128], replicated, may hold values from -0.5 to 0.5
- pool_scale: float32 [1024], replicated, may hold values from 0.1 to 1.9
- w_out: bfloat16 [1024, 2048], replicated, may hold values from -0.1875 to 0.1875
- expert_in: bfloat16 [32768, 2048], P('ep'), may hold values from -6 to 6
- ffn_gain: float32 [2048], replicated, may hold values from 0.1 to 1.9
- routes: int32 [32768, 2], P('ep'), may hold values from 0 to 63, all different within a row; in each aligned block of 128 rows (0 to 127, 128 to 255, ...) at most 6 rows name the same one
- route_weight: float32 [32768, 2], P('ep'), may hold values from 0.25 to 1
- w_gate: bfloat16 [64, 2048, 1024], P('ep', None, 'tp'), may hold values from -0.125 to 0.125
- w_up: bfloat16 [64, 2048, 1024], P('ep', None, 'tp'), may hold values from -0.125 to 0.125
- w_down: bfloat16 [64, 1024, 2048], P('ep', 'tp'), may hold values from -0.1875 to 0.1875
Outputs:
- mixer_out: bfloat16 [65536, 2048], P(('ep', 'tp'))
- expert_out: bfloat16 [32768, 2048], P(('ep', 'tp'))
The draws below stay inside these ranges and needn't reach their ends.
Inputs may be any that keep to these rules, and one draw needn't show every extreme that they name: `routes`: each row names 2 different experts. In each aligned block of 128 rows no expert is named by more than 6 rows, and in some block some expert is named by exactly 6 rows.
All inputs are finite; a program needn't handle non-finite values.
Results may differ from the reference program's by a relative error of at most 0.012.
Values may be sent and summed in bfloat16 or wider, within the bound.
No kernel may reach another device: no remote copies, remote signals or barrier semaphores. Data moves between devices by JAX's collectives and lax.ppermute only.
A program may use at most 128 MiB of HBM per device.

```python
import math
import jax
import jax.numpy as jnp
import numpy as np
from jax import lax

D = 2048
GDIM = 128
GROUPS = 8
PW = 1024
WMAX = 16
FF_E = 1024
EXPERTS = 64
K = 2
TB_DEV = 128
CAP = 6
TOKENS_A = 65536
TOKENS_B = 32768
N_EP = 64
N_TP = 4


def steps_of(stream_key, shape, cuts, smallest, largest):
    def one(axis_at, shards_of):
        steps = jax.random.uniform(jax.random.fold_in(jax.random.fold_in(stream_key, 6), axis_at), (shards_of,), jnp.float32, smallest / len(cuts), largest / len(cuts))
        return jnp.repeat(jnp.exp(steps), shape[axis_at] // shards_of).reshape((-1,) + (1,) * (len(shape) - axis_at - 1))

    factor_of = one(*cuts[0])
    for cut in cuts[1:]:
        factor_of = factor_of * one(*cut)
    return factor_of


def routed_block(stream_key, own, number, rows, count, top, limit, skew):
    sequence = jax.random.permutation(stream_key, count)
    crowded, ordinary = load_shares(count, rows * top, limit, skew, True), load_shares(count, rows * top, limit, skew, False)
    places = jnp.arange(count)

    def named(sizes, rotation):
        used = int((sizes > 0).sum())
        fixed = max(1, used // 4)
        passed = fixed + (places - fixed + rotation * (used - fixed)) % max(1, count - fixed)
        return jnp.zeros((count,), jnp.int32).at[sequence[jnp.where(places < fixed, places, passed)]].set(jnp.asarray(sizes, jnp.int32))

    sizes = jnp.where(number % 4 == 0, named(crowded, number // 4), named(ordinary, number - number // 4 - 1))
    mixed = jax.random.permutation(jax.random.fold_in(own, 3), count)
    donor, receiver = mixed[0:count // 2 * 2:2], mixed[1:count // 2 * 2:2]
    room = jnp.minimum(sizes[donor] - 1, limit - sizes[receiver]) // 2
    room = jnp.where((donor == sequence[0]) | (receiver == sequence[0]) | (sizes[receiver] == 0), 0, jnp.maximum(room, 0))
    passed = jax.random.randint(jax.random.fold_in(own, 4), (count // 2,), 0, 1 << 20) % (room + 1)
    sizes = sizes.at[donor].add(-passed).at[receiver].add(passed)
    labels = jnp.searchsorted(jnp.cumsum(sizes), jnp.arange(rows * top), side="right").astype(jnp.int32)
    listing = labels.reshape(top, rows).T
    listing = listing[jax.random.permutation(jax.random.fold_in(own, 1), rows)]
    rotation = jax.random.randint(jax.random.fold_in(own, 2), (rows, 1), 0, top)
    return jnp.take_along_axis(listing, (jnp.arange(top)[None, :] + rotation) % top, axis=1)


def load_shares(count, total, reach, skew, full):
    weights = [(1 << 20) // math.isqrt(standing ** skew) + 1 for standing in range(1, count + 1)]
    largest = reach if full else min(reach, max(-(-total // count), total * weights[0] // sum(weights)))
    least = 1 if total - largest >= count - 1 else 0
    counts, surplus = [largest] + [least] * (count - 1), total - largest - least * (count - 1)
    while surplus > 0:
        candidates = [i for i in range(1, count) if counts[i] < largest] or [i for i in range(1, count) if counts[i] < reach]
        mass, budget = sum([weights[i] for i in candidates]), surplus
        for i in candidates:
            more = min(reach - counts[i], max(1, budget * weights[i] // mass), surplus)
            counts[i] = counts[i] + more
            surplus = surplus - more
    return np.array(counts)


def scatter_about(stream_key, dims, scale, most, split=(), kind=jnp.bfloat16):
    array = scale * jax.random.normal(stream_key, dims, jnp.float32)
    if split:
        array = array * steps_of(stream_key, dims, split, -0.22, 0.18)
    return jnp.clip(array, -most, most).astype(kind)


def setup_inputs(seed: int = 0) -> dict:
    key_of = jax.random.split(jax.random.key(seed), 12)
    pool_in = scatter_about(key_of[0], (TOKENS_A, PW), 1.0, 6.0, ((0, 256),))
    w_pool = scatter_about(key_of[1], (GROUPS, GDIM, GDIM), GDIM ** -0.5, 0.5)
    pool_scale = jnp.clip(1.0 + 0.18 * jax.random.normal(key_of[2], (PW,), jnp.float32), 0.1, 1.9)
    w_out = scatter_about(key_of[3], (PW, D), PW ** -0.5, 0.1875)
    expert_in = scatter_about(key_of[4], (TOKENS_B, D), 1.0, 6.0, ((0, 64),))
    ffn_gain = jnp.clip(1.0 + 0.18 * jax.random.normal(key_of[5], (D,), jnp.float32), 0.1, 1.9)
    routes_keys = jax.random.split(jax.random.fold_in(key_of[6], 1), TOKENS_B // TB_DEV)
    routes_turns = jax.random.permutation(jax.random.fold_in(key_of[6], 3), TOKENS_B // TB_DEV)
    routes = jax.vmap(lambda own, number: routed_block(jax.random.fold_in(key_of[6], 2), own, number, TB_DEV, EXPERTS, K, CAP, 1))(routes_keys, routes_turns).reshape((TOKENS_B, K))
    route_weight = jnp.clip(0.25 + 0.75 * jax.random.uniform(key_of[7], (TOKENS_B, K), jnp.float32) ** steps_of(key_of[7], (TOKENS_B, K), ((0, 64),), -0.2, 0.2), 0.25, 1.0)
    w_gate = scatter_about(key_of[8], (EXPERTS, D, FF_E), D ** -0.5, 0.125, ((0, 64), (2, 4)))
    w_up = scatter_about(key_of[9], (EXPERTS, D, FF_E), D ** -0.5, 0.125, ((0, 64), (2, 4)))
    w_down = scatter_about(key_of[10], (EXPERTS, FF_E, D), FF_E ** -0.5, 0.1875, ((0, 64), (1, 4)))
    return {"pool_in": pool_in, "w_pool": w_pool, "pool_scale": pool_scale, "w_out": w_out, "expert_in": expert_in, "ffn_gain": ffn_gain, "routes": routes, "route_weight": route_weight, "w_gate": w_gate, "w_up": w_up, "w_down": w_down}


EPS = 0.05

def window_sizes(width):
    group_of = jnp.arange(width) // GDIM
    level = group_of % 4
    return jnp.where(level == 0, 2.0, jnp.where(level == 1, 4.0, jnp.where(level == 2, 8.0, 16.0))).astype(jnp.float32)

def pooled_rows(extended, positions):
    extent = extended.shape[0] - (WMAX - 1)
    window = window_sizes(extended.shape[1])
    running = jnp.zeros((extent, extended.shape[1]), jnp.float32)
    picked = running
    for offset in range(WMAX):
        running = running + extended[WMAX - 1 - offset:WMAX - 1 - offset + extent]
        if offset + 1 in (2, 4, 8, 16):
            picked = jnp.where(window[None, :] == offset + 1, running, picked)
    counted = jnp.minimum(positions[:, None] + 1.0, window[None, :])
    return (picked / counted - extended[WMAX - 1:]).astype(jnp.bfloat16)

def reference(pool_in, w_pool, pool_scale, w_out, expert_in, ffn_gain, routes, route_weight, w_gate, w_up, w_down):
    extended = jnp.pad(pool_in.astype(jnp.float32), ((WMAX - 1, 0), (0, 0)))
    positions = jnp.arange(TOKENS_A).astype(jnp.float32)
    pooled = pooled_rows(extended, positions)
    grouped = jnp.einsum('lgc,gcd->lgd', pooled.reshape(TOKENS_A, GROUPS, GDIM).astype(jnp.float32), w_pool.astype(jnp.float32))
    scaled = (grouped.reshape(TOKENS_A, PW) * pool_scale).astype(jnp.bfloat16)
    mixer_out = jnp.dot(scaled, w_out, preferred_element_type=jnp.float32).astype(jnp.bfloat16)
    features = expert_in.astype(jnp.float32)
    inverse = lax.rsqrt(lax.optimization_barrier(jnp.mean(features * features, axis=-1, keepdims=True)) + EPS)
    normed = (features * inverse * ffn_gain).astype(jnp.bfloat16)
    flat_ids = routes.reshape(-1).astype(jnp.int32)
    flat_weights = route_weight.reshape(-1)
    most_rows = N_EP * N_TP * CAP
    quarter = FF_E // N_TP

    def one_expert(expert, running):
        chosen = flat_ids == expert
        slot_index = jnp.nonzero(chosen, size=most_rows, fill_value=0)[0].astype(jnp.int32)
        filled = jnp.arange(most_rows) < jnp.sum(chosen.astype(jnp.int32))
        token_rows = (slot_index // K).astype(jnp.int32)
        picked_rows = normed[token_rows]
        gate_val = jnp.dot(picked_rows, w_gate[expert], preferred_element_type=jnp.float32)
        up_val = jnp.dot(picked_rows, w_up[expert], preferred_element_type=jnp.float32)
        hidden = (jax.nn.silu(gate_val) * up_val).astype(jnp.bfloat16)
        down_rows = w_down[expert]
        summed = jnp.zeros((most_rows, D), jnp.float32)
        for block in range(N_TP):
            partial_val = jnp.dot(hidden[:, block * quarter:(block + 1) * quarter], down_rows[block * quarter:(block + 1) * quarter], preferred_element_type=jnp.float32).astype(jnp.bfloat16)
            partial_val = lax.optimization_barrier(partial_val)
            summed = summed + partial_val.astype(jnp.float32)
        expert_val = summed.astype(jnp.bfloat16)
        weights = jnp.where(filled, flat_weights[slot_index], jnp.zeros((), jnp.float32))
        return running.at[token_rows].add(weights[:, None] * expert_val.astype(jnp.float32))
    combined = lax.fori_loop(0, EXPERTS, one_expert, jnp.zeros((TOKENS_B, D), jnp.float32))
    return (mixer_out, combined.astype(jnp.bfloat16))
```

```python
from functools import partial

import jax
import jax.numpy as jnp
from jax import lax
from jax.experimental import pallas as pl
from jax.experimental.pallas import tpu as pltpu
from jax.sharding import PartitionSpec as P

GDIM = 128
WMAX = 16
K = 2
EPS = 0.05

CAP = 6
SUB = 8
MAIN = 1536
TAIL = 512
FOLD = MAIN // TAIL
BF16 = jnp.bfloat16
F32 = jnp.float32


def passed_along(array, axis, by):
    length = lax.axis_size(axis)
    pairs = [(i, i + by) for i in range(length) if 0 <= i + by < length]
    return lax.ppermute(array, axis, pairs)


def swapped(array, flip):
    eps, tps = lax.axis_size("ep"), lax.axis_size("tp")
    pairs = []
    for e in range(eps):
        for y in range(tps):
            other = y ^ 1 if (e + flip) % 2 == 0 else tps - 1 - y
            pairs.append((e * tps + y, e * tps + other))
    return lax.ppermute(array, ("ep", "tp"), pairs)


def window_sizes(width):
    group_of = jnp.arange(width) // GDIM
    level = group_of % 4
    return jnp.where(
        level == 0, 2.0, jnp.where(level == 1, 4.0, jnp.where(level == 2, 8.0, 16.0))
    ).astype(F32)


def pooled_rows(extended, positions):
    extent = extended.shape[0] - (WMAX - 1)
    window = window_sizes(extended.shape[1])
    running = jnp.zeros((extent, extended.shape[1]), F32)
    picked = running
    for offset in range(WMAX):
        running = running + extended[WMAX - 1 - offset : WMAX - 1 - offset + extent]
        if offset + 1 in (2, 4, 8, 16):
            picked = jnp.where(window[None, :] == offset + 1, running, picked)
    counted = jnp.minimum(positions[:, None] + 1.0, window[None, :])
    return (picked / counted - extended[WMAX - 1 :]).astype(BF16)


def slot_ranks(routes_ref, rows, tokens):
    first, second = routes_ref[0:1, :], routes_ref[1:2, :]
    row = lax.broadcasted_iota(jnp.int32, (rows, tokens), 0)
    expert, sub = row // SUB, row % SUB
    by_first, by_second = expert == first, expert == second
    named = by_first | by_second
    before = lax.broadcasted_iota(jnp.int32, (tokens, tokens), 0) < lax.broadcasted_iota(
        jnp.int32, (tokens, tokens), 1
    )
    rank = jnp.dot(
        named.astype(F32).astype(BF16), before.astype(F32).astype(BF16), preferred_element_type=F32
    ).astype(jnp.int32)
    return by_first, named, rank, sub


def send_kernel(own_ref, rows_ref, gain_ref, routes_ref, out_ref):
    del own_ref
    tokens = rows_ref.shape[0]
    features = rows_ref[...].astype(F32)
    inverse = lax.rsqrt(jnp.mean(features * features, axis=-1, keepdims=True) + EPS)
    normed = (features * inverse * gain_ref[...]).astype(BF16)
    _, named, rank, sub = slot_ranks(routes_ref, out_ref.shape[0], tokens)
    head = (named & (rank == sub) & (sub < CAP)).astype(F32).astype(BF16)
    for c in range(FOLD):
        tail = (named & (sub >= CAP) & (rank == (sub - CAP) * FOLD + c)).astype(F32).astype(BF16)
        out_ref[:, c * TAIL : (c + 1) * TAIL] = (
            jnp.dot(head, normed[:, c * TAIL : (c + 1) * TAIL], preferred_element_type=F32)
            + jnp.dot(tail, normed[:, MAIN:], preferred_element_type=F32)
        ).astype(BF16)


def send_rows(expert_in, gain, routes_t, own, experts):
    tokens = expert_in.shape[0] // lax.axis_size("tp")
    width = expert_in.shape[1]
    return pl.pallas_call(
        send_kernel,
        out_shape=jax.ShapeDtypeStruct((experts * SUB, MAIN), BF16),
        grid_spec=pltpu.PrefetchScalarGridSpec(
            num_scalar_prefetch=1,
            grid=(1,),
            in_specs=[
                pl.BlockSpec((tokens, width), lambda i, own: (own[0], 0)),
                pl.BlockSpec((1, width), lambda i, own: (0, 0)),
                pl.BlockSpec((K, tokens), lambda i, own: (0, own[0])),
            ],
            out_specs=pl.BlockSpec((experts * SUB, MAIN), lambda i, own: (0, 0)),
        ),
        cost_estimate=pl.CostEstimate(flops=400_000_000, bytes_accessed=2_100_000, transcendentals=128),
        name="send_rows",
    )(own, expert_in, gain.reshape(1, width), routes_t)


def spread(rows, c, turned):
    a = lax.broadcasted_iota(jnp.int32, (rows, rows), 1 if turned else 0)
    b = lax.broadcasted_iota(jnp.int32, (rows, rows), 0 if turned else 1)
    k, s = a % SUB, b % SUB
    return (
        ((a // SUB) == (b // SUB)) & (k < CAP) & (s >= CAP) & (k == (s - CAP) * FOLD + c)
    ).astype(F32).astype(BF16)


def ffn_kernel(x_ref, ga_ref, gb_ref, ua_ref, ub_ref, da_ref, db_ref, out_ref):
    rows = x_ref.shape[0]
    part = 128
    tails = []
    gathers = [spread(part, c, False) for c in range(FOLD)]
    for r in range(rows // part):
        here = slice(r * part, (r + 1) * part)
        tails.append(
            sum(
                jnp.dot(gathers[c], x_ref[here, c * TAIL : (c + 1) * TAIL], preferred_element_type=F32)
                for c in range(FOLD)
            ).astype(BF16)
        )
    tail = jnp.concatenate(tails, axis=0)
    x = x_ref[...]

    def times(w_ref):
        return jnp.dot(x, w_ref[:MAIN, :], preferred_element_type=F32) + jnp.dot(
            tail, w_ref[MAIN:, :], preferred_element_type=F32
        )

    hidden_a = (jax.nn.silu(times(ga_ref)) * times(ua_ref)).astype(BF16)
    hidden_b = (jax.nn.silu(times(gb_ref)) * times(ub_ref)).astype(BF16)

    def down(columns):
        return (
            jnp.dot(hidden_a, da_ref[:, columns], preferred_element_type=F32)
            + jnp.dot(hidden_b, db_ref[:, columns], preferred_element_type=F32)
        ).astype(BF16)

    last = down(slice(MAIN, MAIN + TAIL))
    keep = (lax.broadcasted_iota(jnp.int32, (part, TAIL), 0) % SUB) < CAP
    scatters = [spread(part, c, True) for c in range(FOLD)]
    for c in range(FOLD):
        columns = slice(c * TAIL, (c + 1) * TAIL)
        block = down(columns).astype(F32)
        for r in range(rows // part):
            here = slice(r * part, (r + 1) * part)
            folded = jnp.dot(scatters[c], last[here], preferred_element_type=F32)
            out_ref[here, columns] = jnp.where(keep, block[here], folded).astype(BF16)


def half_ffn(x, ga, gb, ua, ub, da, db):
    rows = x.shape[0]
    step = min(rows, 256)
    whole = lambda w: pl.BlockSpec(w.shape, lambda i: (0, 0))
    hidden = ga.shape[1] + gb.shape[1]
    return pl.pallas_call(
        ffn_kernel,
        out_shape=jax.ShapeDtypeStruct(x.shape, BF16),
        grid=(rows // step,),
        in_specs=[pl.BlockSpec((step, MAIN), lambda i: (i, 0))]
        + [whole(w) for w in (ga, gb, ua, ub, da, db)],
        out_specs=pl.BlockSpec((step, MAIN), lambda i: (i, 0)),
        cost_estimate=pl.CostEstimate(
            flops=rows * hidden * (MAIN + TAIL) * 6,
            bytes_accessed=rows * MAIN * 4 + 6 * ga.size * 2,
            transcendentals=rows * hidden,
        ),
        compiler_params=pltpu.CompilerParams(vmem_limit_bytes=40 * 1024 * 1024),
        name="half_ffn",
    )(x, ga, gb, ua, ub, da, db)


def combine_kernel(own_ref, values_ref, routes_ref, weight_ref, out_ref):
    del own_ref
    rows, tokens = values_ref.shape[0], out_ref.shape[0]
    by_first, named, rank, sub = slot_ranks(routes_ref, rows, tokens)
    weight = jnp.where(by_first, weight_ref[0:1, :], weight_ref[1:2, :])

    def taken(chosen, columns):
        picked = jnp.where(chosen, weight, 0.0).T
        high = picked.astype(BF16)
        low = (picked - high.astype(F32)).astype(BF16)
        values = values_ref[:, columns]
        return jnp.dot(high, values, preferred_element_type=F32) + jnp.dot(
            low, values, preferred_element_type=F32
        )

    head = named & (rank == sub) & (sub < CAP)
    tail = jnp.zeros((tokens, TAIL), F32)
    for c in range(FOLD):
        columns = slice(c * TAIL, (c + 1) * TAIL)
        out_ref[:, columns] = taken(head, columns).astype(BF16)
        tail += taken(named & (sub >= CAP) & (rank == (sub - CAP) * FOLD + c), columns)
    out_ref[:, MAIN:] = tail.astype(BF16)


def combine(values, routes_t, weight_t, own, tokens):
    rows = values.shape[0]
    width = MAIN + TAIL
    return pl.pallas_call(
        combine_kernel,
        out_shape=jax.ShapeDtypeStruct((tokens, width), BF16),
        grid_spec=pltpu.PrefetchScalarGridSpec(
            num_scalar_prefetch=1,
            grid=(1,),
            in_specs=[
                pl.BlockSpec((rows, MAIN), lambda i, own: (0, 0)),
                pl.BlockSpec((K, tokens), lambda i, own: (0, own[0])),
                pl.BlockSpec((K, tokens), lambda i, own: (0, own[0])),
            ],
            out_specs=pl.BlockSpec((tokens, width), lambda i, own: (0, 0)),
        ),
        cost_estimate=pl.CostEstimate(flops=600_000_000, bytes_accessed=2_100_000, transcendentals=0),
        name="combine",
    )(own, values, routes_t, weight_t)


def on_device(
    pool_in,
    w_pool,
    pool_scale,
    w_out,
    expert_in,
    ffn_gain,
    routes,
    route_weight,
    w_gate,
    w_up,
    w_down,
):
    rows_here = pool_in.shape[0]
    tokens = routes.shape[0] // lax.axis_size("tp")
    experts = lax.axis_size("ep") * w_gate.shape[0]
    own = lax.axis_index("tp").astype(jnp.int32).reshape(1)
    routes_t, weight_t = routes.T, route_weight.T

    sent = send_rows(expert_in, ffn_gain, routes_t, own, experts)
    mine = lax.all_to_all(
        sent.reshape(experts, SUB, MAIN), "ep", split_axis=0, concat_axis=0, tiled=True
    ).reshape(experts * SUB, MAIN)

    gate, up, down = w_gate[0], w_up[0], w_down[0]
    gate_b, up_b, down_b = swapped(gate, 0), swapped(up, 0), swapped(down, 0)
    ffn = lambda x: half_ffn(x, gate, gate_b, up, up_b, down, down_b)

    chunks = 2
    size = mine.shape[0] // chunks
    theirs = [swapped(mine[i * size : (i + 1) * size], 1) for i in range(chunks)]
    kept = ffn(mine)
    back = [swapped(ffn(t), 1) for t in theirs]
    results = (kept.astype(F32) + jnp.concatenate(back, axis=0).astype(F32)).astype(BF16)

    returned = lax.all_to_all(
        results.reshape(experts, SUB, MAIN), "ep", split_axis=0, concat_axis=0, tiled=True
    ).reshape(experts * SUB, MAIN)
    expert_out = combine(returned, routes_t, weight_t, own, tokens)

    before = passed_along(pool_in[rows_here - (WMAX - 1) :], ("ep", "tp"), 1)
    extended = jnp.concatenate([before, pool_in], axis=0).astype(F32)
    positions = (lax.axis_index(("ep", "tp")) * rows_here + jnp.arange(rows_here)).astype(F32)
    pooled = pooled_rows(extended, positions)
    group_count = w_pool.shape[0]
    grouped = jnp.einsum(
        "tgc,gcd->tgd",
        pooled.reshape(rows_here, group_count, GDIM),
        w_pool,
        preferred_element_type=F32,
    )
    scaled = (grouped.reshape(rows_here, -1) * pool_scale).astype(BF16)
    mixer_out = jnp.dot(scaled, w_out, preferred_element_type=F32).astype(BF16)
    return (mixer_out, expert_out)


def solution(mesh):
    placed = (
        P(("ep", "tp"), None),
        P(),
        P(),
        P(),
        P("ep", None),
        P(),
        P("ep", None),
        P("ep", None),
        P("ep", None, "tp"),
        P("ep", None, "tp"),
        P("ep", "tp", None),
    )
    return jax.shard_map(
        on_device,
        mesh=mesh,
        in_specs=placed,
        out_specs=(P(("ep", "tp"), None), P(("ep", "tp"), None)),
        check_vma=False,
    )
```

```python
from functools import partial

import jax
import jax.numpy as jnp
from jax import lax
from jax.experimental import pallas as pl
from jax.experimental.pallas import tpu as pltpu
from jax.sharding import PartitionSpec as P


GDIM = 128
WMAX = 16
K = 2
EPS = 0.05

CHUNKS = 2
SLOTS = 3
SUB = 8
LANES = 768
PIECE = 256
FOLD = LANES // PIECE
MAIN = 2 * LANES
WIDTH = MAIN + 2 * PIECE
GROUP = 128
DENSE = GROUP // SUB * SLOTS
BF16 = jnp.bfloat16
F32 = jnp.float32
VMEM = pl.BlockSpec(memory_space=pltpu.VMEM)


def passed_along(array, axis, by):
    length = lax.axis_size(axis)
    pairs = [(i, i + by) for i in range(length) if 0 <= i + by < length]
    return lax.ppermute(array, axis, pairs)


def swapped(array, flip):
    eps, tps = lax.axis_size("ep"), lax.axis_size("tp")
    pairs = []
    for e in range(eps):
        for y in range(tps):
            other = y ^ 1 if (e + flip) % 2 == 0 else tps - 1 - y
            pairs.append((e * tps + y, e * tps + other))
    return lax.ppermute(array, ("ep", "tp"), pairs)


def window_sizes(width):
    group_of = jnp.arange(width) // GDIM
    level = group_of % 4
    return jnp.where(
        level == 0, 2.0, jnp.where(level == 1, 4.0, jnp.where(level == 2, 8.0, 16.0))
    ).astype(F32)


def pooled_rows(extended, positions):
    extent = extended.shape[0] - (WMAX - 1)
    window = window_sizes(extended.shape[1])
    running = jnp.zeros((extent, extended.shape[1]), F32)
    picked = running
    for offset in range(WMAX):
        running = running + extended[WMAX - 1 - offset : WMAX - 1 - offset + extent]
        if offset + 1 in (2, 4, 8, 16):
            picked = jnp.where(window[None, :] == offset + 1, running, picked)
    counted = jnp.minimum(positions[:, None] + 1.0, window[None, :])
    return (picked / counted - extended[WMAX - 1 :]).astype(BF16)


def as_bf16(mask):
    return mask.astype(F32).astype(BF16)


def dot(a, b):
    return jnp.dot(a, b, preferred_element_type=F32)


def slot_ranks(routes_ref, rows, tokens, base):
    first, second = routes_ref[0:1, :], routes_ref[1:2, :]
    row = lax.broadcasted_iota(jnp.int32, (rows, tokens), 0)
    expert, sub = row // SUB, row % SUB
    by_first, by_second = expert == first, expert == second
    named = by_first | by_second
    before = lax.broadcasted_iota(jnp.int32, (tokens, tokens), 0) < lax.broadcasted_iota(
        jnp.int32, (tokens, tokens), 1
    )
    rank = dot(as_bf16(named), as_bf16(before)).astype(jnp.int32) - base
    return by_first, named, rank, sub


def main_place(sub, slot, half):
    return (sub == 2 * slot + half) & (sub < 2 * SLOTS) & (slot >= 0)


def tail_place(sub, slot, piece, c):
    return (sub >= 2 * SLOTS) & ((sub - 2 * SLOTS) * FOLD + c == 2 * slot + piece) & (slot >= 0)


def tail_used(piece, c):
    return any((r * FOLD + c - piece) % 2 == 0 for r in range(SUB - 2 * SLOTS))


def send_kernel(base, own_ref, rows_ref, gain_ref, routes_ref, out_ref):
    del own_ref
    tokens = rows_ref.shape[0]
    features = rows_ref[...].astype(F32)
    inverse = lax.rsqrt(jnp.mean(features * features, axis=-1, keepdims=True) + EPS)
    normed = (features * inverse * gain_ref[...]).astype(BF16)
    _, named, rank, sub = slot_ranks(routes_ref, out_ref.shape[0], tokens, base)
    low = as_bf16(named & main_place(sub, rank, 0))
    high = as_bf16(named & main_place(sub, rank, 1))
    for c in range(FOLD):
        columns = slice(c * PIECE, (c + 1) * PIECE)
        total = dot(low, normed[:, columns]) + dot(high, normed[:, LANES:][:, columns])
        for u in range(2):
            if tail_used(u, c):
                tail = as_bf16(named & tail_place(sub, rank, u, c))
                total += dot(tail, normed[:, MAIN + u * PIECE : MAIN + (u + 1) * PIECE])
        out_ref[:, columns] = total.astype(BF16)


def send_rows(expert_in, gain, routes_t, own, experts, chunk):
    tokens = expert_in.shape[0] // lax.axis_size("tp")
    width = expert_in.shape[1]
    return pl.pallas_call(
        partial(send_kernel, chunk * SLOTS),
        out_shape=jax.ShapeDtypeStruct((experts * SUB, LANES), BF16),
        grid_spec=pltpu.PrefetchScalarGridSpec(
            num_scalar_prefetch=1,
            grid=(1,),
            in_specs=[
                pl.BlockSpec((tokens, width), lambda i, own: (own[0], 0)),
                pl.BlockSpec((1, width), lambda i, own: (0, 0)),
                pl.BlockSpec((K, tokens), lambda i, own: (0, own[0])),
            ],
            out_specs=pl.BlockSpec((experts * SUB, LANES), lambda i, own: (0, 0)),
        ),
        cost_estimate=pl.CostEstimate(flops=2_000_000_000, bytes_accessed=2_100_000, transcendentals=128),
        name="send_rows",
    )(own, expert_in, gain.reshape(1, width), routes_t)


def group_place(shape, dense_axis, where):
    dense = lax.broadcasted_iota(jnp.int32, shape, dense_axis)
    row = lax.broadcasted_iota(jnp.int32, shape, 1 - dense_axis)
    return as_bf16((dense // SLOTS == row // SUB) & where(row % SUB, dense % SLOTS))


def ffn_kernel(x_ref, ga_ref, gb_ref, ua_ref, ub_ref, da_ref, db_ref, out_ref, dense_ref, total_ref):
    groups = x_ref.shape[0] // GROUP
    gather = partial(group_place, (DENSE, GROUP), 0)
    mains = [gather(lambda sub, slot, h=h: main_place(sub, slot, h)) for h in range(2)]
    tails = {
        (u, c): gather(lambda sub, slot, u=u, c=c: tail_place(sub, slot, u, c))
        for u in range(2)
        for c in range(FOLD)
        if tail_used(u, c)
    }
    for g in range(groups):
        rows, dense = slice(g * GROUP, (g + 1) * GROUP), slice(g * DENSE, (g + 1) * DENSE)
        for h in range(2):
            dense_ref[dense, h * LANES : (h + 1) * LANES] = dot(mains[h], x_ref[rows, :]).astype(BF16)
        for u in range(2):
            dense_ref[dense, MAIN + u * PIECE : MAIN + (u + 1) * PIECE] = sum(
                dot(tails[u, c], x_ref[rows, c * PIECE : (c + 1) * PIECE])
                for c in range(FOLD)
                if (u, c) in tails
            ).astype(BF16)
    x = dense_ref[...]
    hidden_a = (jax.nn.silu(dot(x, ga_ref[...])) * dot(x, ua_ref[...])).astype(BF16)
    hidden_b = (jax.nn.silu(dot(x, gb_ref[...])) * dot(x, ub_ref[...])).astype(BF16)
    for c in range(WIDTH // PIECE):
        columns = slice(c * PIECE, (c + 1) * PIECE)
        total_ref[:, columns] = (
            dot(hidden_a, da_ref[:, columns]) + dot(hidden_b, db_ref[:, columns])
        ).astype(BF16)
    scatter = partial(group_place, (GROUP, DENSE), 1)
    mains = [scatter(lambda sub, slot, h=h: main_place(sub, slot, h)) for h in range(2)]
    tails = {
        (u, c): scatter(lambda sub, slot, u=u, c=c: tail_place(sub, slot, u, c)) for u, c in tails
    }
    for g in range(groups):
        rows, dense = slice(g * GROUP, (g + 1) * GROUP), slice(g * DENSE, (g + 1) * DENSE)
        for c in range(FOLD):
            columns = slice(c * PIECE, (c + 1) * PIECE)
            total = sum(
                dot(mains[h], total_ref[dense, h * LANES + c * PIECE : h * LANES + (c + 1) * PIECE])
                for h in range(2)
            )
            for u in range(2):
                if (u, c) in tails:
                    total += dot(
                        tails[u, c], total_ref[dense, MAIN + u * PIECE : MAIN + (u + 1) * PIECE]
                    )
            out_ref[rows, columns] = total.astype(BF16)


def half_ffn(x, ga, gb, ua, ub, da, db):
    rows = x.shape[0]
    dense = rows // SUB * SLOTS
    hidden = ga.shape[1] + gb.shape[1]
    return pl.pallas_call(
        ffn_kernel,
        out_shape=jax.ShapeDtypeStruct(x.shape, BF16),
        in_specs=[VMEM] * 7,
        out_specs=VMEM,
        scratch_shapes=[pltpu.VMEM((dense, WIDTH), BF16), pltpu.VMEM((dense, WIDTH), BF16)],
        cost_estimate=pl.CostEstimate(
            flops=3_500_000_000,
            bytes_accessed=x.size * 4 + 6 * ga.size * 2,
            transcendentals=dense * hidden,
        ),
        compiler_params=pltpu.CompilerParams(vmem_limit_bytes=24 * 1024 * 1024),
        name="half_ffn",
    )(x, ga, gb, ua, ub, da, db)


def combine_kernel(own_ref, first_ref, second_ref, routes_ref, weight_ref, out_ref):
    del own_ref
    rows, tokens = first_ref.shape[0], out_ref.shape[0]
    by_first, named, rank, sub = slot_ranks(routes_ref, rows, tokens, 0)
    weight = jnp.where(by_first, weight_ref[0:1, :], weight_ref[1:2, :])

    def split(chosen):
        picked = jnp.where(chosen, weight, 0.0).T
        high = picked.astype(BF16)
        return high, (picked - high.astype(F32)).astype(BF16)

    parts = [[] for _ in range(WIDTH // PIECE)]
    for chunk, ref in enumerate((first_ref, second_ref)):
        slot = rank - chunk * SLOTS
        here = named & (slot < SLOTS)
        for h in range(2):
            chosen = split(here & main_place(sub, slot, h))
            for c in range(FOLD):
                parts[h * FOLD + c].append((chosen, ref, c))
        for u in range(2):
            for c in range(FOLD):
                if tail_used(u, c):
                    parts[2 * FOLD + u].append((split(here & tail_place(sub, slot, u, c)), ref, c))
    for j, terms in enumerate(parts):
        total = 0.0
        for (high, low), ref, c in terms:
            values = ref[:, c * PIECE : (c + 1) * PIECE]
            total += dot(high, values) + dot(low, values)
        out_ref[:, j * PIECE : (j + 1) * PIECE] = total.astype(BF16)


def combine(values, routes_t, weight_t, own, tokens):
    return pl.pallas_call(
        combine_kernel,
        out_shape=jax.ShapeDtypeStruct((tokens, WIDTH), BF16),
        grid_spec=pltpu.PrefetchScalarGridSpec(
            num_scalar_prefetch=1,
            grid=(1,),
            in_specs=[
                VMEM,
                VMEM,
                pl.BlockSpec((K, tokens), lambda i, own: (0, own[0])),
                pl.BlockSpec((K, tokens), lambda i, own: (0, own[0])),
            ],
            out_specs=pl.BlockSpec((tokens, WIDTH), lambda i, own: (0, 0)),
        ),
        cost_estimate=pl.CostEstimate(flops=2_000_000_000, bytes_accessed=2_100_000, transcendentals=0),
        compiler_params=pltpu.CompilerParams(vmem_limit_bytes=24 * 1024 * 1024),
        name="combine",
    )(own, *values, routes_t, weight_t)


def exchanged(rows):
    experts = rows.shape[0] // SUB
    out = lax.all_to_all(
        rows.reshape(experts, SUB, LANES), "ep", split_axis=0, concat_axis=0, tiled=True
    )
    return out.reshape(rows.shape)


def on_device(
    pool_in,
    w_pool,
    pool_scale,
    w_out,
    expert_in,
    ffn_gain,
    routes,
    route_weight,
    w_gate,
    w_up,
    w_down,
):
    rows_here = pool_in.shape[0]
    tokens = routes.shape[0] // lax.axis_size("tp")
    experts = lax.axis_size("ep") * w_gate.shape[0]
    own = lax.axis_index("tp").astype(jnp.int32).reshape(1)
    routes_t, weight_t = routes.T, route_weight.T
    before = passed_along(pool_in[rows_here - (WMAX - 1) :], ("ep", "tp"), 1)

    gate, up, down = w_gate[0], w_up[0], w_down[0]
    gate_b, up_b, down_b = swapped(gate, 0), swapped(up, 0), swapped(down, 0)
    ffn = lambda x: half_ffn(x, gate, gate_b, up, up_b, down, down_b)

    mine, back, kept, results, returned = [], [], [], [], []
    for n in range(CHUNKS):
        sent = send_rows(expert_in, ffn_gain, routes_t, own, experts, n)
        mine.append(exchanged(sent))
    for n in range(CHUNKS):
        theirs = swapped(mine[n], 1)
        partial_sum = ffn(theirs)
        back.append(swapped(partial_sum, 1))
        kept.append(ffn(mine[n]))
    for n in range(CHUNKS):
        results.append((kept[n].astype(F32) + back[n].astype(F32)).astype(BF16))
        returned.append(exchanged(results[n]))
    expert_out = combine(returned, routes_t, weight_t, own, tokens)

    extended = jnp.concatenate([before, pool_in], axis=0).astype(F32)
    positions = (
        lax.axis_index(("ep", "tp")) * rows_here + jnp.arange(rows_here)
    ).astype(F32)
    pooled = pooled_rows(extended, positions)
    group_count = w_pool.shape[0]
    grouped = jnp.einsum(
        "tgc,gcd->tgd",
        pooled.reshape(rows_here, group_count, GDIM),
        w_pool,
        preferred_element_type=F32,
    )
    scaled = (grouped.reshape(rows_here, -1) * pool_scale).astype(BF16)
    mixer_out = dot(scaled, w_out).astype(BF16)
    return (mixer_out, expert_out)


def solution(mesh):
    placed = (
        P(("ep", "tp"), None),
        P(),
        P(),
        P(),
        P("ep", None),
        P(),
        P("ep", None),
        P("ep", None),
        P("ep", None, "tp"),
        P("ep", None, "tp"),
        P("ep", "tp", None),
    )
    return jax.shard_map(
        on_device,
        mesh=mesh,
        in_specs=placed,
        out_specs=(P(("ep", "tp"), None), P(("ep", "tp"), None)),
        check_vma=False,
    )
```

```python
from functools import partial

import jax
import jax.numpy as jnp
from jax import lax
from jax.experimental import pallas as pl
from jax.experimental.pallas import tpu as pltpu
from jax.sharding import PartitionSpec as P


GDIM = 128
WMAX = 16
K = 2
EPS = 0.05

CHUNKS = 2
SLOTS = 3
SUB = 8
LANES = 768
PIECE = 256
FOLD = LANES // PIECE
MAIN = 2 * LANES
WIDTH = MAIN + 2 * PIECE
EXPERTS_G = 32
GROUP = EXPERTS_G * SUB
DENSE = EXPERTS_G * SLOTS
SMALL = 16 * 1024 * 1024
BF16 = jnp.bfloat16
F32 = jnp.float32
VMEM = pl.BlockSpec(memory_space=pltpu.VMEM)


def passed_along(array, axis, by):
    length = lax.axis_size(axis)
    pairs = [(i, i + by) for i in range(length) if 0 <= i + by < length]
    return lax.ppermute(array, axis, pairs)


def swapped(array, flip):
    eps, tps = lax.axis_size("ep"), lax.axis_size("tp")
    pairs = []
    for e in range(eps):
        for y in range(tps):
            other = y ^ 1 if (e + flip) % 2 == 0 else tps - 1 - y
            pairs.append((e * tps + y, e * tps + other))
    return lax.ppermute(array, ("ep", "tp"), pairs)


def window_sizes(width):
    group_of = jnp.arange(width) // GDIM
    level = group_of % 4
    return jnp.where(
        level == 0, 2.0, jnp.where(level == 1, 4.0, jnp.where(level == 2, 8.0, 16.0))
    ).astype(F32)


def pooled_rows(extended, positions):
    extent = extended.shape[0] - (WMAX - 1)
    window = window_sizes(extended.shape[1])
    running = jnp.zeros((extent, extended.shape[1]), F32)
    picked = running
    for offset in range(WMAX):
        running = running + extended[WMAX - 1 - offset : WMAX - 1 - offset + extent]
        if offset + 1 in (2, 4, 8, 16):
            picked = jnp.where(window[None, :] == offset + 1, running, picked)
    counted = jnp.minimum(positions[:, None] + 1.0, window[None, :])
    return (picked / counted - extended[WMAX - 1 :]).astype(BF16)


def as_bf16(mask):
    return mask.astype(F32).astype(BF16)


def dot(a, b):
    return jnp.dot(a, b, preferred_element_type=F32)


def slot_ranks(routes_ref, rows, tokens, base):
    first, second = routes_ref[0:1, :], routes_ref[1:2, :]
    row = lax.broadcasted_iota(jnp.int32, (rows, tokens), 0)
    expert, sub = row // SUB, row % SUB
    by_first, by_second = expert == first, expert == second
    named = by_first | by_second
    before = lax.broadcasted_iota(jnp.int32, (tokens, tokens), 0) < lax.broadcasted_iota(
        jnp.int32, (tokens, tokens), 1
    )
    rank = dot(as_bf16(named), as_bf16(before)).astype(jnp.int32) - base
    return by_first, named, rank, sub


def main_place(sub, slot, half):
    return (sub == 2 * slot + half) & (sub < 2 * SLOTS) & (slot >= 0)


def tail_place(sub, slot, piece, c):
    return (sub >= 2 * SLOTS) & ((sub - 2 * SLOTS) * FOLD + c == 2 * slot + piece) & (slot >= 0)


def tail_used(piece, c):
    return any((r * FOLD + c - piece) % 2 == 0 for r in range(SUB - 2 * SLOTS))


def send_kernel(base, own_ref, rows_ref, gain_ref, routes_ref, out_ref):
    del own_ref
    tokens = rows_ref.shape[0]
    features = rows_ref[...].astype(F32)
    inverse = lax.rsqrt(jnp.mean(features * features, axis=-1, keepdims=True) + EPS)
    normed = (features * inverse * gain_ref[...]).astype(BF16)
    _, named, rank, sub = slot_ranks(routes_ref, out_ref.shape[0], tokens, base)
    low = as_bf16(named & main_place(sub, rank, 0))
    high = as_bf16(named & main_place(sub, rank, 1))
    for c in range(FOLD):
        columns = slice(c * PIECE, (c + 1) * PIECE)
        total = dot(low, normed[:, columns]) + dot(high, normed[:, LANES:][:, columns])
        for u in range(2):
            if tail_used(u, c):
                tail = as_bf16(named & tail_place(sub, rank, u, c))
                total += dot(tail, normed[:, MAIN + u * PIECE : MAIN + (u + 1) * PIECE])
        out_ref[:, columns] = total.astype(BF16)


def send_rows(expert_in, gain, routes_t, own, experts, chunk):
    tokens = expert_in.shape[0] // lax.axis_size("tp")
    width = expert_in.shape[1]
    return pl.pallas_call(
        partial(send_kernel, chunk * SLOTS),
        out_shape=jax.ShapeDtypeStruct((experts * SUB, LANES), BF16),
        grid_spec=pltpu.PrefetchScalarGridSpec(
            num_scalar_prefetch=1,
            grid=(1,),
            in_specs=[
                pl.BlockSpec((tokens, width), lambda i, own: (own[0], 0)),
                pl.BlockSpec((1, width), lambda i, own: (0, 0)),
                pl.BlockSpec((K, tokens), lambda i, own: (0, own[0])),
            ],
            out_specs=pl.BlockSpec((experts * SUB, LANES), lambda i, own: (0, 0)),
        ),
        cost_estimate=pl.CostEstimate(flops=2_000_000_000, bytes_accessed=2_100_000, transcendentals=128),
        name="send_rows",
    )(own, expert_in, gain.reshape(1, width), routes_t)


def places(shape, dense_axis, where):
    dense = lax.broadcasted_iota(jnp.int32, shape, dense_axis)
    row = lax.broadcasted_iota(jnp.int32, shape, 1 - dense_axis)
    return as_bf16((dense % EXPERTS_G == row // SUB) & where(row % SUB, dense // EXPERTS_G))


def group_maps(shape, dense_axis, c):
    maps = [places(shape, dense_axis, lambda sub, slot, h=h: main_place(sub, slot, h)) for h in range(2)]
    for u in range(2):
        if tail_used(u, c):
            maps.append(places(shape, dense_axis, lambda sub, slot, u=u: tail_place(sub, slot, u, c)))
    return maps


def dense_columns(c):
    starts = [h * LANES + c * PIECE for h in range(2)]
    return starts + [MAIN + u * PIECE for u in range(2) if tail_used(u, c)]


def unpack_kernel(x_ref, out_ref):
    experts = x_ref.shape[0] // SUB
    tails = {}
    for c in range(FOLD):
        maps = jnp.concatenate(group_maps((DENSE, GROUP), 0, c), axis=0)
        for g in range(experts // EXPERTS_G):
            found = dot(maps, x_ref[g * GROUP : (g + 1) * GROUP, c * PIECE : (c + 1) * PIECE])
            for n, start in enumerate(dense_columns(c)):
                block = found[n * DENSE : (n + 1) * DENSE]
                if start >= MAIN:
                    tails[start, g] = tails[start, g] + block if (start, g) in tails else block
                    continue
                for k in range(SLOTS):
                    to = k * experts + g * EXPERTS_G
                    out_ref[to : to + EXPERTS_G, start : start + PIECE] = block[
                        k * EXPERTS_G : (k + 1) * EXPERTS_G
                    ].astype(BF16)
    for (start, g), block in tails.items():
        for k in range(SLOTS):
            to = k * experts + g * EXPERTS_G
            out_ref[to : to + EXPERTS_G, start : start + PIECE] = block[
                k * EXPERTS_G : (k + 1) * EXPERTS_G
            ].astype(BF16)


def unpack(x):
    rows = x.shape[0] // SUB * SLOTS
    return pl.pallas_call(
        unpack_kernel,
        out_shape=jax.ShapeDtypeStruct((rows, WIDTH), BF16),
        in_specs=[VMEM],
        out_specs=VMEM,
        cost_estimate=pl.CostEstimate(flops=800_000_000, bytes_accessed=x.size * 4, transcendentals=0),
        compiler_params=pltpu.CompilerParams(vmem_limit_bytes=SMALL),
        name="unpack",
    )(x)


def pack_kernel(a_ref, b_ref, out_ref):
    experts = out_ref.shape[0] // SUB
    for c in range(FOLD):
        maps = jnp.concatenate(group_maps((GROUP, DENSE), 1, c), axis=1)
        for g in range(experts // EXPERTS_G):
            pieces = []
            for start in dense_columns(c):
                for k in range(SLOTS):
                    here = slice(k * experts + g * EXPERTS_G, k * experts + (g + 1) * EXPERTS_G)
                    columns = slice(start, start + PIECE)
                    pieces.append(
                        (a_ref[here, columns].astype(F32) + b_ref[here, columns].astype(F32)).astype(BF16)
                    )
            out_ref[g * GROUP : (g + 1) * GROUP, c * PIECE : (c + 1) * PIECE] = dot(
                maps, jnp.concatenate(pieces, axis=0)
            ).astype(BF16)


def pack_sum(a, b):
    rows = a.shape[0] // SLOTS * SUB
    return pl.pallas_call(
        pack_kernel,
        out_shape=jax.ShapeDtypeStruct((rows, LANES), BF16),
        in_specs=[VMEM] * 2,
        out_specs=VMEM,
        cost_estimate=pl.CostEstimate(flops=800_000_000, bytes_accessed=a.size * 6, transcendentals=0),
        compiler_params=pltpu.CompilerParams(vmem_limit_bytes=SMALL),
        name="pack_sum",
    )(a, b)


def ffn_kernel(x_ref, ga_ref, gb_ref, ua_ref, ub_ref, da_ref, db_ref, out_ref):
    x = x_ref[...]
    hidden_a = (jax.nn.silu(dot(x, ga_ref[...])) * dot(x, ua_ref[...])).astype(BF16)
    hidden_b = (jax.nn.silu(dot(x, gb_ref[...])) * dot(x, ub_ref[...])).astype(BF16)
    step = 2 * PIECE
    for c in range(WIDTH // step):
        columns = slice(c * step, (c + 1) * step)
        out_ref[:, columns] = (
            dot(hidden_a, da_ref[:, columns]) + dot(hidden_b, db_ref[:, columns])
        ).astype(BF16)


def half_ffn(x, ga, gb, ua, ub, da, db):
    hidden = ga.shape[1] + gb.shape[1]
    return pl.pallas_call(
        ffn_kernel,
        out_shape=jax.ShapeDtypeStruct(x.shape, BF16),
        in_specs=[VMEM] * 7,
        out_specs=VMEM,
        cost_estimate=pl.CostEstimate(
            flops=3_000_000_000,
            bytes_accessed=x.size * 4 + 6 * ga.size * 2,
            transcendentals=x.shape[0] * hidden,
        ),
        compiler_params=pltpu.CompilerParams(vmem_limit_bytes=SMALL),
        name="half_ffn",
    )(x, ga, gb, ua, ub, da, db)


def combine_kernel(base, own_ref, values_ref, routes_ref, weight_ref, *refs):
    del own_ref
    *before_ref, out_ref = refs
    rows, tokens = values_ref.shape[0], out_ref.shape[0]
    routes = jnp.transpose(routes_ref[...].astype(F32)).astype(jnp.int32)
    weights = jnp.transpose(weight_ref[...])
    row = lax.broadcasted_iota(jnp.int32, (tokens, rows), 1)
    expert, sub = row // SUB, row % SUB
    by_first, by_second = expert == routes[:, 0:1], expert == routes[:, 1:2]
    named = by_first | by_second
    earlier = lax.broadcasted_iota(jnp.int32, (tokens, tokens), 1) < lax.broadcasted_iota(
        jnp.int32, (tokens, tokens), 0
    )
    slot = dot(as_bf16(earlier), as_bf16(named)).astype(jnp.int32) - base
    weight = jnp.where(
        named & (slot < SLOTS), jnp.where(by_first, weights[:, 0:1], weights[:, 1:2]), 0.0
    )
    high = weight.astype(BF16).astype(F32)
    low = weight - high

    def taken(chosen, columns):
        values = values_ref[:, columns]
        return dot(jnp.where(chosen, high, 0.0).astype(BF16), values) + dot(
            jnp.where(chosen, low, 0.0).astype(BF16), values
        )

    def put(total, columns):
        if before_ref:
            total += before_ref[0][:, columns]
        out_ref[:, columns] = total.astype(out_ref.dtype)

    for h in range(2):
        put(taken(main_place(sub, slot, h), slice(0, LANES)), slice(h * LANES, (h + 1) * LANES))
    for u in range(2):
        total = 0.0
        for c in range(FOLD):
            if tail_used(u, c):
                total += taken(tail_place(sub, slot, u, c), slice(c * PIECE, (c + 1) * PIECE))
        put(total, slice(MAIN + u * PIECE, MAIN + (u + 1) * PIECE))


def combine(chunk, values, routes_t, weight_t, own, tokens, before=None):
    rest = () if before is None else (before,)
    return pl.pallas_call(
        partial(combine_kernel, chunk * SLOTS),
        out_shape=jax.ShapeDtypeStruct((tokens, WIDTH), F32 if before is None else BF16),
        grid_spec=pltpu.PrefetchScalarGridSpec(
            num_scalar_prefetch=1,
            grid=(1,),
            in_specs=[
                VMEM,
                pl.BlockSpec((K, tokens), lambda i, own: (0, own[0])),
                pl.BlockSpec((K, tokens), lambda i, own: (0, own[0])),
            ]
            + [VMEM] * len(rest),
            out_specs=VMEM if before is None else pl.BlockSpec((tokens, WIDTH), lambda i, own: (0, 0)),
        ),
        cost_estimate=pl.CostEstimate(flops=1_500_000_000, bytes_accessed=2_100_000, transcendentals=0),
        compiler_params=pltpu.CompilerParams(vmem_limit_bytes=SMALL),
        name="combine",
    )(own, values, routes_t, weight_t, *rest)


def exchanged(rows):
    experts = rows.shape[0] // SUB
    out = lax.all_to_all(
        rows.reshape(experts, SUB, LANES), "ep", split_axis=0, concat_axis=0, tiled=True
    )
    return out.reshape(rows.shape)


def on_device(
    pool_in,
    w_pool,
    pool_scale,
    w_out,
    expert_in,
    ffn_gain,
    routes,
    route_weight,
    w_gate,
    w_up,
    w_down,
):
    rows_here = pool_in.shape[0]
    tokens = routes.shape[0] // lax.axis_size("tp")
    experts = lax.axis_size("ep") * w_gate.shape[0]
    own = lax.axis_index("tp").astype(jnp.int32).reshape(1)
    routes_t, weight_t = routes.T, route_weight.T
    before = passed_along(pool_in[rows_here - (WMAX - 1) :], ("ep", "tp"), 1)

    gate, up, down = w_gate[0], w_up[0], w_down[0]
    gate_b, up_b, down_b = swapped(gate, 0), swapped(up, 0), swapped(down, 0)
    ffn = lambda x: half_ffn(x, gate, gate_b, up, up_b, down, down_b)

    mine = []
    for n in range(CHUNKS):
        sent = send_rows(expert_in, ffn_gain, routes_t, own, experts, n)
        mine.append(exchanged(sent))
    expert_out = None
    for n in range(CHUNKS):
        rows = unpack(mine[n])
        theirs = swapped(rows, 1)
        partial_sum = ffn(theirs)
        back = swapped(partial_sum, 1)
        kept = ffn(rows)
        results = pack_sum(kept, back)
        returned = exchanged(results)
        expert_out = combine(n, returned, routes_t, weight_t, own, tokens, expert_out)

    extended = jnp.concatenate([before, pool_in], axis=0).astype(F32)
    positions = (
        lax.axis_index(("ep", "tp")) * rows_here + jnp.arange(rows_here)
    ).astype(F32)
    pooled = pooled_rows(extended, positions)
    group_count = w_pool.shape[0]
    grouped = jnp.einsum(
        "tgc,gcd->tgd",
        pooled.reshape(rows_here, group_count, GDIM),
        w_pool,
        preferred_element_type=F32,
    )
    scaled = (grouped.reshape(rows_here, -1) * pool_scale).astype(BF16)
    mixer_out = dot(scaled, w_out).astype(BF16)
    return (mixer_out, expert_out)


def solution(mesh):
    placed = (
        P(("ep", "tp"), None),
        P(),
        P(),
        P(),
        P("ep", None),
        P(),
        P("ep", None),
        P("ep", None),
        P("ep", None, "tp"),
        P("ep", None, "tp"),
        P("ep", "tp", None),
    )
    return jax.shard_map(
        on_device,
        mesh=mesh,
        in_specs=placed,
        out_specs=(P(("ep", "tp"), None), P(("ep", "tp"), None)),
        check_vma=False,
    )
```

```python
from functools import partial

import jax
import jax.numpy as jnp
from jax import lax
from jax.experimental import pallas as pl
from jax.experimental.pallas import tpu as pltpu
from jax.sharding import PartitionSpec as P


GDIM = 128
WMAX = 16
K = 2
EPS = 0.05

CHUNKS = 2
SLOTS = 3
SUB = 8
LANES = 768
PIECE = 256
FOLD = LANES // PIECE
MAIN = 2 * LANES
WIDTH = MAIN + 2 * PIECE
EXPERTS_G = 32
GROUP = EXPERTS_G * SUB
DENSE = EXPERTS_G * SLOTS
SMALL = 16 * 1024 * 1024
BF16 = jnp.bfloat16
F32 = jnp.float32
VMEM = pl.BlockSpec(memory_space=pltpu.VMEM)
HBM = pl.BlockSpec(memory_space=pltpu.HBM)


def passed_along(array, axis, by):
    length = lax.axis_size(axis)
    pairs = [(i, i + by) for i in range(length) if 0 <= i + by < length]
    return lax.ppermute(array, axis, pairs)


def swapped(array, flip):
    eps, tps = lax.axis_size("ep"), lax.axis_size("tp")
    pairs = []
    for e in range(eps):
        for y in range(tps):
            other = y ^ 1 if (e + flip) % 2 == 0 else tps - 1 - y
            pairs.append((e * tps + y, e * tps + other))
    return lax.ppermute(array, ("ep", "tp"), pairs)


def window_sizes(width):
    group_of = jnp.arange(width) // GDIM
    level = group_of % 4
    return jnp.where(
        level == 0, 2.0, jnp.where(level == 1, 4.0, jnp.where(level == 2, 8.0, 16.0))
    ).astype(F32)


def pooled_rows(extended, positions):
    extent = extended.shape[0] - (WMAX - 1)
    window = window_sizes(extended.shape[1])
    running = jnp.zeros((extent, extended.shape[1]), F32)
    picked = running
    for offset in range(WMAX):
        running = running + extended[WMAX - 1 - offset : WMAX - 1 - offset + extent]
        if offset + 1 in (2, 4, 8, 16):
            picked = jnp.where(window[None, :] == offset + 1, running, picked)
    counted = jnp.minimum(positions[:, None] + 1.0, window[None, :])
    return (picked / counted - extended[WMAX - 1 :]).astype(BF16)


def as_bf16(mask):
    return mask.astype(F32).astype(BF16)


def dot(a, b):
    return jnp.dot(a, b, preferred_element_type=F32)


def slot_ranks(routes_ref, rows, tokens, base):
    first, second = routes_ref[0:1, :], routes_ref[1:2, :]
    row = lax.broadcasted_iota(jnp.int32, (rows, tokens), 0)
    expert, sub = row // SUB, row % SUB
    by_first, by_second = expert == first, expert == second
    named = by_first | by_second
    before = lax.broadcasted_iota(jnp.int32, (tokens, tokens), 0) < lax.broadcasted_iota(
        jnp.int32, (tokens, tokens), 1
    )
    rank = dot(as_bf16(named), as_bf16(before)).astype(jnp.int32) - base
    return by_first, named, rank, sub


def main_place(sub, slot, half):
    return (sub == 2 * slot + half) & (sub < 2 * SLOTS) & (slot >= 0)


def tail_place(sub, slot, piece, c):
    return (sub >= 2 * SLOTS) & ((sub - 2 * SLOTS) * FOLD + c == 2 * slot + piece) & (slot >= 0)


def tail_used(piece, c):
    return any((r * FOLD + c - piece) % 2 == 0 for r in range(SUB - 2 * SLOTS))


def send_kernel(base, own_ref, rows_hbm, gain_ref, routes_ref, out_ref, rows_ref, sem):
    tokens = rows_ref.shape[0]
    copy = pltpu.make_async_copy(
        rows_hbm.at[pl.ds(pl.multiple_of(own_ref[0] * tokens, tokens), tokens)], rows_ref, sem
    )
    copy.start()
    _, named, rank, sub = slot_ranks(routes_ref, out_ref.shape[0], tokens, base)
    mains = jnp.concatenate([as_bf16(named & main_place(sub, rank, h)) for h in range(2)], axis=1)
    copy.wait()
    features = rows_ref[...].astype(F32)
    inverse = lax.rsqrt(jnp.mean(features * features, axis=-1, keepdims=True) + EPS)
    normed = (features * inverse * gain_ref[...]).astype(BF16)
    for c in range(FOLD):
        columns = slice(c * PIECE, (c + 1) * PIECE)
        used = [u for u in range(2) if tail_used(u, c)]
        tails = jnp.concatenate([as_bf16(named & tail_place(sub, rank, u, c)) for u in used], axis=1)
        total = dot(
            mains, jnp.concatenate([normed[:, columns], normed[:, LANES:][:, columns]], axis=0)
        ) + dot(
            tails,
            jnp.concatenate(
                [normed[:, MAIN + u * PIECE : MAIN + (u + 1) * PIECE] for u in used], axis=0
            ),
        )
        out_ref[:, columns] = total.astype(BF16)


def send_rows(expert_in, gain, routes_t, own, experts, chunk):
    tokens = expert_in.shape[0] // lax.axis_size("tp")
    width = expert_in.shape[1]
    return pl.pallas_call(
        partial(send_kernel, chunk * SLOTS),
        out_shape=jax.ShapeDtypeStruct((experts * SUB, LANES), BF16),
        grid_spec=pltpu.PrefetchScalarGridSpec(
            num_scalar_prefetch=1,
            grid=(1,),
            in_specs=[
                HBM,
                pl.BlockSpec((1, width), lambda i, own: (0, 0)),
                pl.BlockSpec((K, tokens), lambda i, own: (0, own[0])),
            ],
            out_specs=VMEM,
            scratch_shapes=[pltpu.VMEM((tokens, width), BF16), pltpu.SemaphoreType.DMA],
        ),
        cost_estimate=pl.CostEstimate(flops=2_000_000_000, bytes_accessed=2_100_000, transcendentals=128),
        name="send_rows",
    )(own, expert_in, gain.reshape(1, width), routes_t)


def places(shape, dense_axis, where):
    dense = lax.broadcasted_iota(jnp.int32, shape, dense_axis)
    row = lax.broadcasted_iota(jnp.int32, shape, 1 - dense_axis)
    return as_bf16((dense % EXPERTS_G == row // SUB) & where(row % SUB, dense // EXPERTS_G))


def group_maps(shape, dense_axis, c):
    maps = [places(shape, dense_axis, lambda sub, slot, h=h: main_place(sub, slot, h)) for h in range(2)]
    for u in range(2):
        if tail_used(u, c):
            maps.append(places(shape, dense_axis, lambda sub, slot, u=u: tail_place(sub, slot, u, c)))
    return maps


def dense_columns(c):
    starts = [h * LANES + c * PIECE for h in range(2)]
    return starts + [MAIN + u * PIECE for u in range(2) if tail_used(u, c)]


def unpack(x_ref, out_ref):
    experts = x_ref.shape[0] // SUB
    tails = {}
    for c in range(FOLD):
        maps = jnp.concatenate(group_maps((DENSE, GROUP), 0, c), axis=0)
        for g in range(experts // EXPERTS_G):
            found = dot(maps, x_ref[g * GROUP : (g + 1) * GROUP, c * PIECE : (c + 1) * PIECE])
            for n, start in enumerate(dense_columns(c)):
                block = found[n * DENSE : (n + 1) * DENSE]
                if start >= MAIN:
                    tails[start, g] = tails[start, g] + block if (start, g) in tails else block
                    continue
                for k in range(SLOTS):
                    to = k * experts + g * EXPERTS_G
                    out_ref[to : to + EXPERTS_G, start : start + PIECE] = block[
                        k * EXPERTS_G : (k + 1) * EXPERTS_G
                    ].astype(BF16)
    for (start, g), block in tails.items():
        for k in range(SLOTS):
            to = k * experts + g * EXPERTS_G
            out_ref[to : to + EXPERTS_G, start : start + PIECE] = block[
                k * EXPERTS_G : (k + 1) * EXPERTS_G
            ].astype(BF16)


def pack_kernel(a_ref, b_ref, out_ref):
    experts = out_ref.shape[0] // SUB
    for c in range(FOLD):
        maps = jnp.concatenate(group_maps((GROUP, DENSE), 1, c), axis=1)
        for g in range(experts // EXPERTS_G):
            pieces = []
            for start in dense_columns(c):
                for k in range(SLOTS):
                    here = slice(k * experts + g * EXPERTS_G, k * experts + (g + 1) * EXPERTS_G)
                    columns = slice(start, start + PIECE)
                    pieces.append(
                        (a_ref[here, columns].astype(F32) + b_ref[here, columns].astype(F32)).astype(BF16)
                    )
            out_ref[g * GROUP : (g + 1) * GROUP, c * PIECE : (c + 1) * PIECE] = dot(
                maps, jnp.concatenate(pieces, axis=0)
            ).astype(BF16)


def pack_sum(a, b):
    rows = a.shape[0] // SLOTS * SUB
    return pl.pallas_call(
        pack_kernel,
        out_shape=jax.ShapeDtypeStruct((rows, LANES), BF16),
        in_specs=[VMEM] * 2,
        out_specs=VMEM,
        cost_estimate=pl.CostEstimate(flops=800_000_000, bytes_accessed=a.size * 6, transcendentals=0),
        compiler_params=pltpu.CompilerParams(vmem_limit_bytes=SMALL),
        name="pack_sum",
    )(a, b)


def ffn_kernel(x_ref, *refs):
    sources, out_ref, dense_ref, held, sems = refs[:6], refs[6], refs[7], refs[8:14], refs[14]
    copies = [
        pltpu.make_async_copy(source, ref, sems.at[n])
        for n, (source, ref) in enumerate(zip(sources, held))
    ]
    for copy in copies:
        copy.start()
    ga_ref, ua_ref, gb_ref, ub_ref, da_ref, db_ref = held
    unpack(x_ref, dense_ref)
    x = dense_ref[...]
    copies[0].wait()
    copies[1].wait()
    hidden_a = (jax.nn.silu(dot(x, ga_ref[...])) * dot(x, ua_ref[...])).astype(BF16)
    copies[2].wait()
    copies[3].wait()
    hidden_b = (jax.nn.silu(dot(x, gb_ref[...])) * dot(x, ub_ref[...])).astype(BF16)
    copies[4].wait()
    copies[5].wait()
    step = 2 * PIECE
    for c in range(WIDTH // step):
        columns = slice(c * step, (c + 1) * step)
        out_ref[:, columns] = (
            dot(hidden_a, da_ref[:, columns]) + dot(hidden_b, db_ref[:, columns])
        ).astype(BF16)


def half_ffn(x, ga, gb, ua, ub, da, db):
    weights = (ga, ua, gb, ub, da, db)
    dense = x.shape[0] // SUB * SLOTS
    hidden = ga.shape[1] + gb.shape[1]
    return pl.pallas_call(
        ffn_kernel,
        out_shape=jax.ShapeDtypeStruct((dense, WIDTH), BF16),
        in_specs=[VMEM] + [HBM] * 6,
        out_specs=VMEM,
        scratch_shapes=[pltpu.VMEM((dense, WIDTH), BF16)]
        + [pltpu.VMEM(w.shape, BF16) for w in weights]
        + [pltpu.SemaphoreType.DMA((6,))],
        cost_estimate=pl.CostEstimate(
            flops=3_500_000_000,
            bytes_accessed=x.size * 4 + 6 * ga.size * 2,
            transcendentals=dense * hidden,
        ),
        compiler_params=pltpu.CompilerParams(vmem_limit_bytes=SMALL),
        name="half_ffn",
    )(x, *weights)


def combine_kernel(base, own_ref, values_ref, routes_ref, weight_ref, *refs):
    del own_ref
    *before_ref, out_ref = refs
    rows, tokens = values_ref.shape[0], out_ref.shape[0]
    routes = jnp.transpose(routes_ref[...].astype(F32)).astype(jnp.int32)
    weights = jnp.transpose(weight_ref[...])
    row = lax.broadcasted_iota(jnp.int32, (tokens, rows), 1)
    expert, sub = row // SUB, row % SUB
    by_first, by_second = expert == routes[:, 0:1], expert == routes[:, 1:2]
    named = by_first | by_second
    earlier = lax.broadcasted_iota(jnp.int32, (tokens, tokens), 1) < lax.broadcasted_iota(
        jnp.int32, (tokens, tokens), 0
    )
    slot = dot(as_bf16(earlier), as_bf16(named)).astype(jnp.int32) - base
    weight = jnp.where(
        named & (slot < SLOTS), jnp.where(by_first, weights[:, 0:1], weights[:, 1:2]), 0.0
    )
    high = weight.astype(BF16).astype(F32)
    low = weight - high

    def split(chosen):
        return [jnp.where(chosen, part, 0.0).astype(BF16) for part in (high, low)]

    totals = {}
    mains = [part for h in range(2) for part in split(main_place(sub, slot, h))]
    for c in range(FOLD):
        maps = list(mains)
        for u in range(2):
            if tail_used(u, c):
                maps += split(tail_place(sub, slot, u, c))
        found = dot(jnp.concatenate(maps, axis=0), values_ref[:, c * PIECE : (c + 1) * PIECE])
        for n, start in enumerate(dense_columns(c)):
            block = found[2 * n * tokens : (2 * n + 1) * tokens] + found[(2 * n + 1) * tokens : (2 * n + 2) * tokens]
            totals[start] = totals[start] + block if start in totals else block
    for start, total in totals.items():
        columns = slice(start, start + PIECE)
        if before_ref:
            total += before_ref[0][:, columns]
        out_ref[:, columns] = total.astype(out_ref.dtype)


def combine(chunk, values, routes_t, weight_t, own, tokens, before=None):
    rest = () if before is None else (before,)
    return pl.pallas_call(
        partial(combine_kernel, chunk * SLOTS),
        out_shape=jax.ShapeDtypeStruct((tokens, WIDTH), F32 if before is None else BF16),
        grid_spec=pltpu.PrefetchScalarGridSpec(
            num_scalar_prefetch=1,
            grid=(1,),
            in_specs=[
                VMEM,
                pl.BlockSpec((K, tokens), lambda i, own: (0, own[0])),
                pl.BlockSpec((K, tokens), lambda i, own: (0, own[0])),
            ]
            + [VMEM] * len(rest),
            out_specs=VMEM if before is None else pl.BlockSpec((tokens, WIDTH), lambda i, own: (0, 0)),
        ),
        cost_estimate=pl.CostEstimate(flops=1_500_000_000, bytes_accessed=2_100_000, transcendentals=0),
        compiler_params=pltpu.CompilerParams(vmem_limit_bytes=SMALL),
        name="combine",
    )(own, values, routes_t, weight_t, *rest)


def exchanged(rows):
    experts = rows.shape[0] // SUB
    out = lax.all_to_all(
        rows.reshape(experts, SUB, LANES), "ep", split_axis=0, concat_axis=0, tiled=True
    )
    return out.reshape(rows.shape)


def on_device(
    pool_in,
    w_pool,
    pool_scale,
    w_out,
    expert_in,
    ffn_gain,
    routes,
    route_weight,
    w_gate,
    w_up,
    w_down,
):
    rows_here = pool_in.shape[0]
    tokens = routes.shape[0] // lax.axis_size("tp")
    experts = lax.axis_size("ep") * w_gate.shape[0]
    own = lax.axis_index("tp").astype(jnp.int32).reshape(1)
    routes_t, weight_t = routes.T, route_weight.T
    before = passed_along(pool_in[rows_here - (WMAX - 1) :], ("ep", "tp"), 1)

    gate, up, down = w_gate[0], w_up[0], w_down[0]
    gate_b = swapped(gate, 0)
    up_b, down_b = swapped(up, 0), swapped(down, 0)
    ffn = lambda x: half_ffn(x, gate, gate_b, up, up_b, down, down_b)

    mine = []
    for n in range(CHUNKS):
        sent = send_rows(expert_in, ffn_gain, routes_t, own, experts, n)
        mine.append(exchanged(sent))
    expert_out = None
    for n in range(CHUNKS):
        theirs = swapped(mine[n], 1)
        partial_sum = ffn(theirs)
        back = swapped(partial_sum, 1)
        kept = ffn(mine[n])
        results = pack_sum(kept, back)
        returned = exchanged(results)
        expert_out = combine(n, returned, routes_t, weight_t, own, tokens, expert_out)

    extended = jnp.concatenate([before, pool_in], axis=0).astype(F32)
    positions = (
        lax.axis_index(("ep", "tp")) * rows_here + jnp.arange(rows_here)
    ).astype(F32)
    pooled = pooled_rows(extended, positions)
    group_count = w_pool.shape[0]
    grouped = jnp.einsum(
        "tgc,gcd->tgd",
        pooled.reshape(rows_here, group_count, GDIM),
        w_pool,
        preferred_element_type=F32,
    )
    scaled = (grouped.reshape(rows_here, -1) * pool_scale).astype(BF16)
    mixer_out = dot(scaled, w_out).astype(BF16)
    return (mixer_out, expert_out)


def solution(mesh):
    placed = (
        P(("ep", "tp"), None),
        P(),
        P(),
        P(),
        P("ep", None),
        P(),
        P("ep", None),
        P("ep", None),
        P("ep", None, "tp"),
        P("ep", None, "tp"),
        P("ep", "tp", None),
    )
    return jax.shard_map(
        on_device,
        mesh=mesh,
        in_specs=placed,
        out_specs=(P(("ep", "tp"), None), P(("ep", "tp"), None)),
        check_vma=False,
    )
```

```python
from functools import partial

import jax
import jax.numpy as jnp
from jax import lax
from jax.experimental import pallas as pl
from jax.experimental.pallas import tpu as pltpu
from jax.sharding import PartitionSpec as P


GDIM = 128
WMAX = 16
K = 2
EPS = 0.05

CHUNKS = 2
SLOTS = 3
SUB = 8
LANES = 768
PIECE = 256
FOLD = LANES // PIECE
MAIN = 2 * LANES
WIDTH = MAIN + 2 * PIECE
CORES = 2
EXPERTS_G = 32
GROUP = EXPERTS_G * SUB
DENSE = EXPERTS_G * SLOTS
SMALL = 16 * 1024 * 1024
LARGE = 52 * 1024 * 1024
BF16 = jnp.bfloat16
F32 = jnp.float32
VMEM = pl.BlockSpec(memory_space=pltpu.VMEM)
ANY = pl.BlockSpec(memory_space=pl.ANY)


def passed_along(array, axis, by):
    length = lax.axis_size(axis)
    pairs = [(i, i + by) for i in range(length) if 0 <= i + by < length]
    return lax.ppermute(array, axis, pairs)


def swapped(array, flip):
    eps, tps = lax.axis_size("ep"), lax.axis_size("tp")
    pairs = []
    for e in range(eps):
        for y in range(tps):
            other = y ^ 1 if (e + flip) % 2 == 0 else tps - 1 - y
            pairs.append((e * tps + y, e * tps + other))
    return lax.ppermute(array, ("ep", "tp"), pairs)


def window_sizes(width):
    group_of = jnp.arange(width) // GDIM
    level = group_of % 4
    return jnp.where(
        level == 0, 2.0, jnp.where(level == 1, 4.0, jnp.where(level == 2, 8.0, 16.0))
    ).astype(F32)


def pooled_rows(extended, positions):
    extent = extended.shape[0] - (WMAX - 1)
    window = window_sizes(extended.shape[1])
    running = jnp.zeros((extent, extended.shape[1]), F32)
    picked = running
    for offset in range(WMAX):
        running = running + extended[WMAX - 1 - offset : WMAX - 1 - offset + extent]
        if offset + 1 in (2, 4, 8, 16):
            picked = jnp.where(window[None, :] == offset + 1, running, picked)
    counted = jnp.minimum(positions[:, None] + 1.0, window[None, :])
    return (picked / counted - extended[WMAX - 1 :]).astype(BF16)


def as_bf16(mask):
    return mask.astype(F32).astype(BF16)


def dot(a, b):
    return jnp.dot(a, b, preferred_element_type=F32)


def slot_ranks(meta, core, rows, base):
    tokens = meta.shape[1]
    row = lax.broadcasted_iota(jnp.int32, (rows, tokens), 0)
    expert, sub = (row // SUB * CORES + core).astype(F32), row % SUB
    by_first, by_second = expert == meta[0:1, :], expert == meta[1:2, :]
    named = by_first | by_second
    before = lax.broadcasted_iota(jnp.int32, (tokens, tokens), 0) < lax.broadcasted_iota(
        jnp.int32, (tokens, tokens), 1
    )
    rank = dot(as_bf16(named), as_bf16(before)).astype(jnp.int32) - base
    return named, rank, sub


def main_place(sub, slot, half):
    return (sub == 2 * slot + half) & (sub < 2 * SLOTS) & (slot >= 0)


def tail_place(sub, slot, piece, c):
    return (sub >= 2 * SLOTS) & ((sub - 2 * SLOTS) * FOLD + c == 2 * slot + piece) & (slot >= 0)


def tail_used(piece, c):
    return any((r * FOLD + c - piece) % 2 == 0 for r in range(SUB - 2 * SLOTS))


def norm_kernel(place_ref, rows_ref, gain_ref, out_ref):
    del place_ref
    features = rows_ref[...].astype(F32)
    inverse = lax.rsqrt(jnp.mean(features * features, axis=-1, keepdims=True) + EPS)
    out_ref[...] = (features * inverse * gain_ref[...]).astype(BF16)


def normalized(expert_in, gain, place):
    tokens, width = expert_in.shape[0] // lax.axis_size("tp"), expert_in.shape[1]
    return pl.pallas_call(
        norm_kernel,
        out_shape=jax.ShapeDtypeStruct((tokens, width), BF16),
        grid_spec=pltpu.PrefetchScalarGridSpec(
            num_scalar_prefetch=1,
            grid=(1,),
            in_specs=[
                pl.BlockSpec((tokens, width), lambda i, place: (place[0], 0)),
                pl.BlockSpec((1, width), lambda i, place: (0, 0)),
            ],
            out_specs=pl.BlockSpec((tokens, width), lambda i, place: (0, 0)),
        ),
        cost_estimate=pl.CostEstimate(flops=1_000_000_000, bytes_accessed=1_100_000, transcendentals=128),
        name="normalized",
    )(place, expert_in, gain.reshape(1, width))


def send_kernel(base, place_ref, own_ref, twin_ref, own_meta_ref, twin_meta_ref, out_ref):
    for side, (normed, meta_ref) in enumerate(((own_ref, own_meta_ref), (twin_ref, twin_meta_ref))):
        named, rank, sub = slot_ranks(meta_ref[...], place_ref[1], out_ref.shape[0], base)
        mains = jnp.concatenate([as_bf16(named & main_place(sub, rank, h)) for h in range(2)], axis=1)
        for c in range(FOLD):
            used = [u for u in range(2) if tail_used(u, c)]
            tails = [as_bf16(named & tail_place(sub, rank, u, c)) for u in used]
            total = dot(
                mains,
                jnp.concatenate(
                    [normed[:, h * LANES + c * PIECE : h * LANES + (c + 1) * PIECE] for h in range(2)],
                    axis=0,
                ),
            ) + dot(
                jnp.concatenate(tails, axis=1),
                jnp.concatenate(
                    [normed[:, MAIN + u * PIECE : MAIN + (u + 1) * PIECE] for u in used], axis=0
                ),
            )
            out_ref[:, side * LANES + c * PIECE : side * LANES + (c + 1) * PIECE] = total.astype(BF16)


def send_rows(own, twin, own_meta, twin_meta, place, chips, chunk):
    tokens = own.shape[0]
    meta = pl.BlockSpec((2 * K, tokens), lambda i, place: (0, place[0]))
    return pl.pallas_call(
        partial(send_kernel, chunk * SLOTS),
        out_shape=jax.ShapeDtypeStruct((chips * SUB, CORES * LANES), BF16),
        grid_spec=pltpu.PrefetchScalarGridSpec(
            num_scalar_prefetch=1,
            grid=(1,),
            in_specs=[VMEM, VMEM, meta, meta],
            out_specs=VMEM,
        ),
        cost_estimate=pl.CostEstimate(flops=2_000_000_000, bytes_accessed=2_100_000, transcendentals=0),
        compiler_params=pltpu.CompilerParams(vmem_limit_bytes=SMALL),
        name="send_rows",
    )(place, own, twin, own_meta, twin_meta)


def places(shape, dense_axis, where):
    dense = lax.broadcasted_iota(jnp.int32, shape, dense_axis)
    row = lax.broadcasted_iota(jnp.int32, shape, 1 - dense_axis)
    return as_bf16((dense % EXPERTS_G == row // SUB) & where(row % SUB, dense // EXPERTS_G))


def main_maps(shape, dense_axis):
    return [places(shape, dense_axis, lambda sub, slot, h=h: main_place(sub, slot, h)) for h in range(2)]


def tail_maps(shape, dense_axis, c):
    return [
        places(shape, dense_axis, lambda sub, slot, u=u: tail_place(sub, slot, u, c))
        for u in range(2)
        if tail_used(u, c)
    ]


def dense_columns(c):
    starts = [h * LANES + c * PIECE for h in range(2)]
    return starts + [MAIN + u * PIECE for u in range(2) if tail_used(u, c)]


def unpack(x_ref, out_ref):
    mains = main_maps((DENSE, GROUP), 0)
    tails = {}

    def put(block, side, start):
        for k in range(SLOTS):
            to = (k * CORES + side) * EXPERTS_G
            out_ref[to : to + EXPERTS_G, start : start + PIECE] = block[
                k * EXPERTS_G : (k + 1) * EXPERTS_G
            ].astype(BF16)

    for c in range(FOLD):
        maps = jnp.concatenate(mains + tail_maps((DENSE, GROUP), 0, c), axis=0)
        for side in range(CORES):
            at = side * LANES + c * PIECE
            found = dot(maps, x_ref[:, at : at + PIECE])
            for n, start in enumerate(dense_columns(c)):
                block = found[n * DENSE : (n + 1) * DENSE]
                if start < MAIN:
                    put(block, side, start)
                else:
                    tails[start, side] = tails[start, side] + block if (start, side) in tails else block
    for (start, side), block in tails.items():
        put(block, side, start)


def pack_kernel(a_ref, b_ref, out_ref):
    mains = main_maps((GROUP, DENSE), 1)
    for c in range(FOLD):
        maps = jnp.concatenate(mains + tail_maps((GROUP, DENSE), 1, c), axis=1)
        for side in range(CORES):
            pieces = []
            for start in dense_columns(c):
                columns = slice(start, start + PIECE)
                for k in range(SLOTS):
                    to = (k * CORES + side) * EXPERTS_G
                    here = slice(to, to + EXPERTS_G)
                    pieces.append(
                        (a_ref[here, columns].astype(F32) + b_ref[here, columns].astype(F32)).astype(BF16)
                    )
            at = side * LANES + c * PIECE
            out_ref[:, at : at + PIECE] = dot(maps, jnp.concatenate(pieces, axis=0)).astype(BF16)


def pack_sum(a, b):
    return pl.pallas_call(
        pack_kernel,
        out_shape=jax.ShapeDtypeStruct((GROUP, CORES * LANES), BF16),
        in_specs=[VMEM] * 2,
        out_specs=VMEM,
        cost_estimate=pl.CostEstimate(flops=800_000_000, bytes_accessed=a.size * 6, transcendentals=0),
        compiler_params=pltpu.CompilerParams(vmem_limit_bytes=SMALL),
        name="pack_sum",
    )(a, b)


def ffn_kernel(*refs):
    sources, out_ref, dense_ref, held, sems = refs[:7], refs[7], refs[8], refs[9:16], refs[16]
    rows, *copies = [
        pltpu.make_async_copy(source, ref, sems.at[n])
        for n, (source, ref) in enumerate(zip(sources, held))
    ]
    rows.start()
    for copy in copies:
        copy.start()
    x_ref, ga_ref, ua_ref, gb_ref, ub_ref, da_ref, db_ref = held
    rows.wait()
    unpack(x_ref, dense_ref)
    x = dense_ref[...]
    copies[0].wait()
    copies[1].wait()
    hidden_a = (jax.nn.silu(dot(x, ga_ref[...])) * dot(x, ua_ref[...])).astype(BF16)
    copies[2].wait()
    copies[3].wait()
    hidden_b = (jax.nn.silu(dot(x, gb_ref[...])) * dot(x, ub_ref[...])).astype(BF16)
    copies[4].wait()
    copies[5].wait()
    step = 2 * PIECE
    for c in range(WIDTH // step):
        columns = slice(c * step, (c + 1) * step)
        out_ref[:, columns] = (
            dot(hidden_a, da_ref[:, columns]) + dot(hidden_b, db_ref[:, columns])
        ).astype(BF16)


def half_ffn(x, ga, gb, ua, ub, da, db):
    operands = (x, ga, ua, gb, ub, da, db)
    dense = x.size // WIDTH // SUB * SUB
    hidden = ga.shape[1] + gb.shape[1]
    return pl.pallas_call(
        ffn_kernel,
        out_shape=jax.ShapeDtypeStruct((dense, WIDTH), BF16),
        in_specs=[ANY] * 7,
        out_specs=VMEM,
        scratch_shapes=[pltpu.VMEM((dense, WIDTH), BF16)]
        + [pltpu.VMEM(operand.shape, BF16) for operand in operands]
        + [pltpu.SemaphoreType.DMA((7,))],
        cost_estimate=pl.CostEstimate(
            flops=3_500_000_000,
            bytes_accessed=x.size * 4 + 6 * ga.size * 2,
            transcendentals=dense * hidden,
        ),
        compiler_params=pltpu.CompilerParams(vmem_limit_bytes=LARGE),
        name="half_ffn",
    )(*operands)


def combine_kernel(base, last, place_ref, values_ref, own_meta_ref, twin_meta_ref, *refs):
    if last:
        sources, out_refs, before_refs, sems = refs[:2], refs[2:4], refs[4:6], refs[6]
        copies = [
            pltpu.make_async_copy(source, ref, sems.at[n])
            for n, (source, ref) in enumerate(zip(sources, before_refs))
        ]
        for copy in copies:
            copy.start()
    else:
        out_refs = refs
    rows = values_ref.shape[0]
    for side, meta_ref in enumerate((own_meta_ref, twin_meta_ref)):
        tokens = meta_ref.shape[1]
        meta = jnp.transpose(meta_ref[...])
        row = lax.broadcasted_iota(jnp.int32, (tokens, rows), 1)
        expert, sub = (row // SUB * CORES + place_ref[1]).astype(F32), row % SUB
        by_first, by_second = expert == meta[:, 0:1], expert == meta[:, 1:2]
        named = by_first | by_second
        earlier = lax.broadcasted_iota(jnp.int32, (tokens, tokens), 1) < lax.broadcasted_iota(
            jnp.int32, (tokens, tokens), 0
        )
        slot = dot(as_bf16(earlier), as_bf16(named)).astype(jnp.int32) - base
        weight = jnp.where(
            named & (slot < SLOTS), jnp.where(by_first, meta[:, 2:3], meta[:, 3:4]), 0.0
        )
        high = weight.astype(BF16).astype(F32)
        low = weight - high

        def split(chosen):
            return [jnp.where(chosen, part, 0.0).astype(BF16) for part in (high, low)]

        totals = {}
        mains = [part for h in range(2) for part in split(main_place(sub, slot, h))]
        for c in range(FOLD):
            maps = list(mains)
            for u in range(2):
                if tail_used(u, c):
                    maps += split(tail_place(sub, slot, u, c))
            at = side * LANES + c * PIECE
            found = dot(jnp.concatenate(maps, axis=0), values_ref[:, at : at + PIECE])
            for n, start in enumerate(dense_columns(c)):
                block = (
                    found[2 * n * tokens : (2 * n + 1) * tokens]
                    + found[(2 * n + 1) * tokens : (2 * n + 2) * tokens]
                )
                totals[start] = totals[start] + block if start in totals else block
        if last:
            copies[side].wait()
        for start, total in totals.items():
            columns = slice(start, start + PIECE)
            if last:
                total += before_refs[side][:, columns]
            out_refs[side][:, columns] = total.astype(out_refs[side].dtype)


def combine(chunk, values, own_meta, twin_meta, place, tokens, before):
    last = bool(before)
    meta = pl.BlockSpec((2 * K, tokens), lambda i, place: (0, place[0]))
    return pl.pallas_call(
        partial(combine_kernel, chunk * SLOTS, last),
        out_shape=[
            jax.ShapeDtypeStruct((tokens, WIDTH), F32),
            jax.ShapeDtypeStruct((tokens, WIDTH), BF16 if last else F32),
        ],
        grid_spec=pltpu.PrefetchScalarGridSpec(
            num_scalar_prefetch=1,
            grid=(1,),
            in_specs=[VMEM, meta, meta] + [ANY] * len(before),
            out_specs=[VMEM] * 2,
            scratch_shapes=[pltpu.VMEM((tokens, WIDTH), F32)] * 2 + [pltpu.SemaphoreType.DMA((2,))]
            if last
            else [],
        ),
        cost_estimate=pl.CostEstimate(flops=1_500_000_000, bytes_accessed=2_100_000, transcendentals=0),
        compiler_params=pltpu.CompilerParams(vmem_limit_bytes=LARGE),
        name="combine",
    )(place, values, own_meta, twin_meta, *before)


def exchanged(rows):
    chips = rows.shape[0] // SUB
    out = lax.all_to_all(
        rows.reshape(chips, SUB, CORES * LANES),
        "ep",
        split_axis=0,
        concat_axis=0,
        tiled=True,
        axis_index_groups=[[CORES * i + c for i in range(chips)] for c in range(CORES)],
    )
    return out.reshape(rows.shape)


def twin_of(array):
    return lax.ppermute(array, "ep", [(i, i ^ 1) for i in range(lax.axis_size("ep"))])


def on_device(
    pool_in,
    w_pool,
    pool_scale,
    w_out,
    expert_in,
    ffn_gain,
    routes,
    route_weight,
    w_gate,
    w_up,
    w_down,
):
    rows_here = pool_in.shape[0]
    tokens = routes.shape[0] // lax.axis_size("tp")
    chips = lax.axis_size("ep") * w_gate.shape[0] // CORES
    place = jnp.stack([lax.axis_index("tp"), lax.axis_index("ep") % CORES]).astype(jnp.int32)
    own_meta = jnp.concatenate([routes.T.astype(F32), route_weight.T], axis=0)
    twin_meta = twin_of(own_meta)
    own_rows = normalized(expert_in, ffn_gain, place)
    twin_rows = twin_of(own_rows)
    before = passed_along(pool_in[rows_here - (WMAX - 1) :], ("ep", "tp"), 1)

    gate, up, down = w_gate[0], w_up[0], w_down[0]
    gate_b = swapped(gate, 0)
    up_b, down_b = swapped(up, 0), swapped(down, 0)
    ffn = lambda x: half_ffn(x, gate, gate_b, up, up_b, down, down_b)

    mine = []
    for n in range(CHUNKS):
        sent = send_rows(own_rows, twin_rows, own_meta, twin_meta, place, chips, n)
        mine.append(exchanged(sent))
    summed = ()
    for n in range(CHUNKS):
        theirs = swapped(mine[n], 1)
        partial_sum = ffn(theirs)
        back = swapped(partial_sum, 1)
        kept = ffn(mine[n])
        results = pack_sum(kept, back)
        returned = exchanged(results)
        summed = combine(n, returned, own_meta, twin_meta, place, tokens, summed)
    other = twin_of(summed[1])
    expert_out = (summed[0] + other.astype(F32)).astype(BF16)

    extended = jnp.concatenate([before, pool_in], axis=0).astype(F32)
    positions = (
        lax.axis_index(("ep", "tp")) * rows_here + jnp.arange(rows_here)
    ).astype(F32)
    pooled = pooled_rows(extended, positions)
    group_count = w_pool.shape[0]
    grouped = jnp.einsum(
        "tgc,gcd->tgd",
        pooled.reshape(rows_here, group_count, GDIM),
        w_pool,
        preferred_element_type=F32,
    )
    scaled = (grouped.reshape(rows_here, -1) * pool_scale).astype(BF16)
    mixer_out = dot(scaled, w_out).astype(BF16)
    return (mixer_out, expert_out)


def solution(mesh):
    placed = (
        P(("ep", "tp"), None),
        P(),
        P(),
        P(),
        P("ep", None),
        P(),
        P("ep", None),
        P("ep", None),
        P("ep", None, "tp"),
        P("ep", None, "tp"),
        P("ep", "tp", None),
    )
    return jax.shard_map(
        on_device,
        mesh=mesh,
        in_specs=placed,
        out_specs=(P(("ep", "tp"), None), P(("ep", "tp"), None)),
        check_vma=False,
    )
```

```python
from functools import partial

import jax
import jax.numpy as jnp
from jax import lax
from jax.experimental import pallas as pl
from jax.experimental.pallas import tpu as pltpu
from jax.sharding import PartitionSpec as P


GDIM = 128
WMAX = 16
K = 2
EPS = 0.05

CHUNKS = 2
SLOTS = 3
SUB = 8
LANES = 768
PIECE = 256
FOLD = LANES // PIECE
MAIN = 2 * LANES
WIDTH = MAIN + 2 * PIECE
EXPERTS_G = 32
GROUP = EXPERTS_G * SUB
DENSE = EXPERTS_G * SLOTS
SMALL = 16 * 1024 * 1024
LARGE = 52 * 1024 * 1024
LARGER = 53 * 1024 * 1024
BF16 = jnp.bfloat16
F32 = jnp.float32
VMEM = pl.BlockSpec(memory_space=pltpu.VMEM)
ANY = pl.BlockSpec(memory_space=pl.ANY)


def passed_along(array, axis, by):
    length = lax.axis_size(axis)
    pairs = [(i, i + by) for i in range(length) if 0 <= i + by < length]
    return lax.ppermute(array, axis, pairs)


def swapped(array, flip):
    eps, tps = lax.axis_size("ep"), lax.axis_size("tp")
    pairs = []
    for e in range(eps):
        for y in range(tps):
            other = y ^ 1 if (e + flip) % 2 == 0 else tps - 1 - y
            pairs.append((e * tps + y, e * tps + other))
    return lax.ppermute(array, ("ep", "tp"), pairs)


def window_sizes(width):
    group_of = jnp.arange(width) // GDIM
    level = group_of % 4
    return jnp.where(
        level == 0, 2.0, jnp.where(level == 1, 4.0, jnp.where(level == 2, 8.0, 16.0))
    ).astype(F32)


def pooled_rows(extended, positions):
    extent = extended.shape[0] - (WMAX - 1)
    window = window_sizes(extended.shape[1])
    running = jnp.zeros((extent, extended.shape[1]), F32)
    picked = running
    for offset in range(WMAX):
        running = running + extended[WMAX - 1 - offset : WMAX - 1 - offset + extent]
        if offset + 1 in (2, 4, 8, 16):
            picked = jnp.where(window[None, :] == offset + 1, running, picked)
    counted = jnp.minimum(positions[:, None] + 1.0, window[None, :])
    return (picked / counted - extended[WMAX - 1 :]).astype(BF16)


def as_bf16(mask):
    return mask.astype(F32).astype(BF16)


def dot(a, b):
    return jnp.dot(a, b, preferred_element_type=F32)


def slot_ranks(routes_ref, rows, tokens, base):
    first, second = routes_ref[0:1, :], routes_ref[1:2, :]
    row = lax.broadcasted_iota(jnp.int32, (rows, tokens), 0)
    expert, sub = row // SUB, row % SUB
    by_first, by_second = expert == first, expert == second
    named = by_first | by_second
    before = lax.broadcasted_iota(jnp.int32, (tokens, tokens), 0) < lax.broadcasted_iota(
        jnp.int32, (tokens, tokens), 1
    )
    rank = dot(as_bf16(named), as_bf16(before)).astype(jnp.int32) - base
    return by_first, named, rank, sub


def main_place(sub, slot, half):
    return (sub == 2 * slot + half) & (sub < 2 * SLOTS) & (slot >= 0)


def tail_place(sub, slot, piece, c):
    return (sub >= 2 * SLOTS) & ((sub - 2 * SLOTS) * FOLD + c == 2 * slot + piece) & (slot >= 0)


def tail_used(piece, c):
    return any((r * FOLD + c - piece) % 2 == 0 for r in range(SUB - 2 * SLOTS))


def send_kernel(base, own_ref, rows_hbm, gain_ref, routes_ref, out_ref, rows_ref, normed_ref, sems):
    tokens = rows_ref.shape[0]
    half = tokens // 2
    copies = []
    for n in range(2):
        here = pl.ds(pl.multiple_of(own_ref[0] * tokens + n * half, half), half)
        copies.append(
            pltpu.make_async_copy(
                rows_hbm.at[here], rows_ref.at[pl.ds(n * half, half)], sems.at[n]
            )
        )
        copies[n].start()
    _, named, rank, sub = slot_ranks(routes_ref, out_ref.shape[0], tokens, base)
    mains = jnp.concatenate([as_bf16(named & main_place(sub, rank, h)) for h in range(2)], axis=1)
    for n in range(2):
        here = slice(n * half, (n + 1) * half)
        copies[n].wait()
        features = rows_ref[here, :].astype(F32)
        inverse = lax.rsqrt(jnp.mean(features * features, axis=-1, keepdims=True) + EPS)
        normed_ref[here, :] = (features * inverse * gain_ref[...]).astype(BF16)
    for c in range(FOLD):
        used = [u for u in range(2) if tail_used(u, c)]
        tails = [as_bf16(named & tail_place(sub, rank, u, c)) for u in used]
        starts = [h * LANES + c * PIECE for h in range(2)] + [MAIN + u * PIECE for u in used]
        out_ref[:, c * PIECE : (c + 1) * PIECE] = dot(
            jnp.concatenate([mains, *tails], axis=1),
            jnp.concatenate([normed_ref[:, start : start + PIECE] for start in starts], axis=0),
        ).astype(BF16)


def send_rows(expert_in, gain, routes_t, own, experts, chunk):
    tokens = expert_in.shape[0] // lax.axis_size("tp")
    width = expert_in.shape[1]
    return pl.pallas_call(
        partial(send_kernel, chunk * SLOTS),
        out_shape=jax.ShapeDtypeStruct((experts * SUB, LANES), BF16),
        grid_spec=pltpu.PrefetchScalarGridSpec(
            num_scalar_prefetch=1,
            grid=(1,),
            in_specs=[
                ANY,
                pl.BlockSpec((1, width), lambda i, own: (0, 0)),
                pl.BlockSpec((K, tokens), lambda i, own: (0, own[0])),
            ],
            out_specs=VMEM,
            scratch_shapes=[pltpu.VMEM((tokens, width), BF16)] * 2 + [pltpu.SemaphoreType.DMA((2,))],
        ),
        cost_estimate=pl.CostEstimate(flops=2_000_000_000, bytes_accessed=2_100_000, transcendentals=128),
        name="send_rows",
    )(own, expert_in, gain.reshape(1, width), routes_t)


def places(shape, dense_axis, where):
    dense = lax.broadcasted_iota(jnp.int32, shape, dense_axis)
    row = lax.broadcasted_iota(jnp.int32, shape, 1 - dense_axis)
    return as_bf16((dense % EXPERTS_G == row // SUB) & where(row % SUB, dense // EXPERTS_G))


def main_maps(shape, dense_axis):
    return [places(shape, dense_axis, lambda sub, slot, h=h: main_place(sub, slot, h)) for h in range(2)]


def tail_maps(shape, dense_axis, c):
    return [
        places(shape, dense_axis, lambda sub, slot, u=u: tail_place(sub, slot, u, c))
        for u in range(2)
        if tail_used(u, c)
    ]


def dense_columns(c):
    starts = [h * LANES + c * PIECE for h in range(2)]
    return starts + [MAIN + u * PIECE for u in range(2) if tail_used(u, c)]


def unpack(x_ref, out_ref):
    experts = x_ref.shape[0] // SUB
    mains = main_maps((DENSE, GROUP), 0)
    tails = {}

    def put(block, g, start):
        for k in range(SLOTS):
            to = k * experts + g * EXPERTS_G
            out_ref[to : to + EXPERTS_G, start : start + PIECE] = block[
                k * EXPERTS_G : (k + 1) * EXPERTS_G
            ].astype(BF16)

    for c in range(FOLD):
        maps = jnp.concatenate(mains + tail_maps((DENSE, GROUP), 0, c), axis=0)
        for g in range(experts // EXPERTS_G):
            found = dot(maps, x_ref[g * GROUP : (g + 1) * GROUP, c * PIECE : (c + 1) * PIECE])
            for n, start in enumerate(dense_columns(c)):
                block = found[n * DENSE : (n + 1) * DENSE]
                if start < MAIN:
                    put(block, g, start)
                else:
                    tails[start, g] = tails[start, g] + block if (start, g) in tails else block
    for (start, g), block in tails.items():
        put(block, g, start)


def pack_kernel(a_ref, *refs):
    *b_refs, out_ref = refs
    experts = out_ref.shape[0] // SUB
    mains = main_maps((GROUP, DENSE), 1)
    for c in range(FOLD):
        maps = jnp.concatenate(mains + tail_maps((GROUP, DENSE), 1, c), axis=1)
        for g, b_ref in enumerate(b_refs):
            pieces = []
            for start in dense_columns(c):
                columns = slice(start, start + PIECE)
                for k in range(SLOTS):
                    at = k * experts + g * EXPERTS_G
                    own = a_ref[at : at + EXPERTS_G, columns].astype(F32)
                    other = b_ref[k * EXPERTS_G : (k + 1) * EXPERTS_G, columns].astype(F32)
                    pieces.append((own + other).astype(BF16))
            out_ref[g * GROUP : (g + 1) * GROUP, c * PIECE : (c + 1) * PIECE] = dot(
                maps, jnp.concatenate(pieces, axis=0)
            ).astype(BF16)


def pack_sum(a, parts):
    rows = a.shape[0] // SLOTS * SUB
    return pl.pallas_call(
        pack_kernel,
        out_shape=jax.ShapeDtypeStruct((rows, LANES), BF16),
        in_specs=[VMEM] * (1 + len(parts)),
        out_specs=VMEM,
        cost_estimate=pl.CostEstimate(flops=800_000_000, bytes_accessed=a.size * 6, transcendentals=0),
        compiler_params=pltpu.CompilerParams(vmem_limit_bytes=SMALL),
        name="pack_sum",
    )(a, *parts)


def ffn_kernel(*refs):
    sources, out_ref, dense_ref, held, sems = refs[:7], refs[7], refs[8], refs[9:16], refs[16]
    rows, *copies = [
        pltpu.make_async_copy(source, ref, sems.at[n])
        for n, (source, ref) in enumerate(zip(sources, held))
    ]
    rows.start()
    for copy in copies:
        copy.start()
    x_ref, ga_ref, ua_ref, gb_ref, ub_ref, da_ref, db_ref = held
    rows.wait()
    unpack(x_ref, dense_ref)
    x = dense_ref[...]
    copies[0].wait()
    copies[1].wait()
    hidden_a = (jax.nn.silu(dot(x, ga_ref[...])) * dot(x, ua_ref[...])).astype(BF16)
    copies[2].wait()
    copies[3].wait()
    hidden_b = (jax.nn.silu(dot(x, gb_ref[...])) * dot(x, ub_ref[...])).astype(BF16)
    copies[4].wait()
    copies[5].wait()
    step = 2 * PIECE
    for c in range(WIDTH // step):
        columns = slice(c * step, (c + 1) * step)
        out_ref[:, columns] = (
            dot(hidden_a, da_ref[:, columns]) + dot(hidden_b, db_ref[:, columns])
        ).astype(BF16)


def half_ffn(x, ga, gb, ua, ub, da, db):
    operands = (x, ga, ua, gb, ub, da, db)
    dense = x.shape[0] // SUB * SLOTS
    hidden = ga.shape[1] + gb.shape[1]
    return pl.pallas_call(
        ffn_kernel,
        out_shape=jax.ShapeDtypeStruct((dense, WIDTH), BF16),
        in_specs=[ANY] * 7,
        out_specs=VMEM,
        scratch_shapes=[pltpu.VMEM((dense, WIDTH), BF16)]
        + [pltpu.VMEM(operand.shape, BF16) for operand in operands]
        + [pltpu.SemaphoreType.DMA((7,))],
        cost_estimate=pl.CostEstimate(
            flops=3_500_000_000,
            bytes_accessed=x.size * 4 + 6 * ga.size * 2,
            transcendentals=dense * hidden,
        ),
        compiler_params=pltpu.CompilerParams(vmem_limit_bytes=LARGER),
        name="half_ffn",
    )(*operands)


def combine_kernel(base, own_ref, values_ref, routes_ref, weight_ref, *refs):
    del own_ref
    copy = None
    if base:
        source, out_ref, before_ref, sem = refs
        copy = pltpu.make_async_copy(source, before_ref, sem)
        copy.start()
    else:
        (out_ref,) = refs
    rows, tokens = values_ref.shape[0], out_ref.shape[0]
    routes = jnp.transpose(routes_ref[...].astype(F32)).astype(jnp.int32)
    weights = jnp.transpose(weight_ref[...])
    row = lax.broadcasted_iota(jnp.int32, (tokens, rows), 1)
    expert, sub = row // SUB, row % SUB
    by_first, by_second = expert == routes[:, 0:1], expert == routes[:, 1:2]
    named = by_first | by_second
    earlier = lax.broadcasted_iota(jnp.int32, (tokens, tokens), 1) < lax.broadcasted_iota(
        jnp.int32, (tokens, tokens), 0
    )
    slot = dot(as_bf16(earlier), as_bf16(named)).astype(jnp.int32) - base
    weight = jnp.where(
        named & (slot < SLOTS), jnp.where(by_first, weights[:, 0:1], weights[:, 1:2]), 0.0
    )
    high = weight.astype(BF16).astype(F32)
    low = weight - high

    def split(chosen):
        return [jnp.where(chosen, part, 0.0).astype(BF16) for part in (high, low)]

    totals = {}
    mains = [part for h in range(2) for part in split(main_place(sub, slot, h))]
    for c in range(FOLD):
        maps = list(mains)
        for u in range(2):
            if tail_used(u, c):
                maps += split(tail_place(sub, slot, u, c))
        found = dot(jnp.concatenate(maps, axis=0), values_ref[:, c * PIECE : (c + 1) * PIECE])
        for n, start in enumerate(dense_columns(c)):
            block = found[2 * n * tokens : (2 * n + 1) * tokens] + found[(2 * n + 1) * tokens : (2 * n + 2) * tokens]
            totals[start] = totals[start] + block if start in totals else block
    if copy is not None:
        copy.wait()
    for start, total in totals.items():
        columns = slice(start, start + PIECE)
        if copy is not None:
            total += before_ref[:, columns]
        out_ref[:, columns] = total.astype(out_ref.dtype)


def combine(chunk, values, routes_t, weight_t, own, tokens, before=None):
    rest = () if before is None else (before,)
    return pl.pallas_call(
        partial(combine_kernel, chunk * SLOTS),
        out_shape=jax.ShapeDtypeStruct((tokens, WIDTH), F32 if before is None else BF16),
        grid_spec=pltpu.PrefetchScalarGridSpec(
            num_scalar_prefetch=1,
            grid=(1,),
            in_specs=[
                VMEM,
                pl.BlockSpec((K, tokens), lambda i, own: (0, own[0])),
                pl.BlockSpec((K, tokens), lambda i, own: (0, own[0])),
            ]
            + [ANY] * len(rest),
            out_specs=VMEM if before is None else pl.BlockSpec((tokens, WIDTH), lambda i, own: (0, 0)),
            scratch_shapes=[pltpu.VMEM((tokens, WIDTH), F32), pltpu.SemaphoreType.DMA] if rest else [],
        ),
        cost_estimate=pl.CostEstimate(flops=1_500_000_000, bytes_accessed=2_100_000, transcendentals=0),
        compiler_params=pltpu.CompilerParams(vmem_limit_bytes=LARGE),
        name="combine",
    )(own, values, routes_t, weight_t, *rest)


def exchanged(rows):
    experts = rows.shape[0] // SUB
    out = lax.all_to_all(
        rows.reshape(experts, SUB, LANES), "ep", split_axis=0, concat_axis=0, tiled=True
    )
    return out.reshape(rows.shape)


def on_device(
    pool_in,
    w_pool,
    pool_scale,
    w_out,
    expert_in,
    ffn_gain,
    routes,
    route_weight,
    w_gate,
    w_up,
    w_down,
):
    rows_here = pool_in.shape[0]
    tokens = routes.shape[0] // lax.axis_size("tp")
    experts = lax.axis_size("ep") * w_gate.shape[0]
    own = lax.axis_index("tp").astype(jnp.int32).reshape(1)
    routes_t, weight_t = routes.T, route_weight.T
    before = passed_along(pool_in[rows_here - (WMAX - 1) :], ("ep", "tp"), 1)

    gate, up, down = w_gate[0], w_up[0], w_down[0]
    gate_b, up_b = swapped(gate, 0), swapped(up, 0)
    down_b = swapped(down, 0)
    ffn = lambda x: half_ffn(x, gate, gate_b, up, up_b, down, down_b)

    mine = []
    for n in range(CHUNKS):
        sent = send_rows(expert_in, ffn_gain, routes_t, own, experts, n)
        mine.append(exchanged(sent))
    expert_out = None
    for n in range(CHUNKS):
        back = []
        halves = mine[n].shape[0] // GROUP
        theirs = []
        for g in range(halves):
            theirs.append(swapped(mine[n][g * GROUP : (g + 1) * GROUP], 1))
        for g in range(halves):
            partial_sum = ffn(theirs[g])
            back.append(swapped(partial_sum, 1))
        kept = ffn(mine[n])
        results = pack_sum(kept, back)
        returned = exchanged(results)
        expert_out = combine(n, returned, routes_t, weight_t, own, tokens, expert_out)

    extended = jnp.concatenate([before, pool_in], axis=0).astype(F32)
    positions = (
        lax.axis_index(("ep", "tp")) * rows_here + jnp.arange(rows_here)
    ).astype(F32)
    pooled = pooled_rows(extended, positions)
    group_count = w_pool.shape[0]
    grouped = jnp.einsum(
        "tgc,gcd->tgd",
        pooled.reshape(rows_here, group_count, GDIM),
        w_pool,
        preferred_element_type=F32,
    )
    scaled = (grouped.reshape(rows_here, -1) * pool_scale).astype(BF16)
    mixer_out = dot(scaled, w_out).astype(BF16)
    return (mixer_out, expert_out)


def solution(mesh):
    placed = (
        P(("ep", "tp"), None),
        P(),
        P(),
        P(),
        P("ep", None),
        P(),
        P("ep", None),
        P("ep", None),
        P("ep", None, "tp"),
        P("ep", None, "tp"),
        P("ep", "tp", None),
    )
    return jax.shard_map(
        on_device,
        mesh=mesh,
        in_specs=placed,
        out_specs=(P(("ep", "tp"), None), P(("ep", "tp"), None)),
        check_vma=False,
    )
```

```python
from functools import partial

import jax
import jax.numpy as jnp
from jax import lax
from jax.experimental import pallas as pl
from jax.experimental.pallas import tpu as pltpu
from jax.sharding import PartitionSpec as P


GDIM = 128
WMAX = 16
K = 2
EPS = 0.05

CHUNKS = 2
SLOTS = 3
SUB = 8
LANES = 768
PIECE = 256
FOLD = LANES // PIECE
MAIN = 2 * LANES
WIDTH = MAIN + 2 * PIECE
EXPERTS_G = 32
GROUP = EXPERTS_G * SUB
DENSE = EXPERTS_G * SLOTS
SMALL = 16 * 1024 * 1024
LARGE = 52 * 1024 * 1024
BF16 = jnp.bfloat16
F32 = jnp.float32
VMEM = pl.BlockSpec(memory_space=pltpu.VMEM)
ANY = pl.BlockSpec(memory_space=pl.ANY)


def passed_along(array, axis, by):
    length = lax.axis_size(axis)
    pairs = [(i, i + by) for i in range(length) if 0 <= i + by < length]
    return lax.ppermute(array, axis, pairs)


def swapped(array, flip):
    eps, tps = lax.axis_size("ep"), lax.axis_size("tp")
    pairs = []
    for e in range(eps):
        for y in range(tps):
            other = y ^ 1 if (e + flip) % 2 == 0 else tps - 1 - y
            pairs.append((e * tps + y, e * tps + other))
    return lax.ppermute(array, ("ep", "tp"), pairs)


def window_sizes(width):
    group_of = jnp.arange(width) // GDIM
    level = group_of % 4
    return jnp.where(
        level == 0, 2.0, jnp.where(level == 1, 4.0, jnp.where(level == 2, 8.0, 16.0))
    ).astype(F32)


def pooled_rows(extended, positions):
    extent = extended.shape[0] - (WMAX - 1)
    window = window_sizes(extended.shape[1])
    running = jnp.zeros((extent, extended.shape[1]), F32)
    picked = running
    for offset in range(WMAX):
        running = running + extended[WMAX - 1 - offset : WMAX - 1 - offset + extent]
        if offset + 1 in (2, 4, 8, 16):
            picked = jnp.where(window[None, :] == offset + 1, running, picked)
    counted = jnp.minimum(positions[:, None] + 1.0, window[None, :])
    return (picked / counted - extended[WMAX - 1 :]).astype(BF16)


def as_bf16(mask):
    return mask.astype(F32).astype(BF16)


def dot(a, b):
    return jnp.dot(a, b, preferred_element_type=F32)


def slot_ranks(routes_ref, rows, tokens, base):
    first, second = routes_ref[0:1, :], routes_ref[1:2, :]
    row = lax.broadcasted_iota(jnp.int32, (rows, tokens), 0)
    expert, sub = row // SUB, row % SUB
    by_first, by_second = expert == first, expert == second
    named = by_first | by_second
    before = lax.broadcasted_iota(jnp.int32, (tokens, tokens), 0) < lax.broadcasted_iota(
        jnp.int32, (tokens, tokens), 1
    )
    rank = dot(as_bf16(named), as_bf16(before)).astype(jnp.int32) - base
    return by_first, named, rank, sub


def main_place(sub, slot, half):
    return (sub == 2 * slot + half) & (sub < 2 * SLOTS) & (slot >= 0)


def tail_place(sub, slot, piece, c):
    return (sub >= 2 * SLOTS) & ((sub - 2 * SLOTS) * FOLD + c == 2 * slot + piece) & (slot >= 0)


def tail_used(piece, c):
    return any((r * FOLD + c - piece) % 2 == 0 for r in range(SUB - 2 * SLOTS))


def send_kernel(base, own_ref, rows_hbm, gain_ref, routes_ref, out_ref, rows_ref, normed_ref, sems):
    tokens = rows_ref.shape[0]
    half = tokens // 2
    copies = []
    for n in range(2):
        here = pl.ds(pl.multiple_of(own_ref[0] * tokens + n * half, half), half)
        copies.append(
            pltpu.make_async_copy(
                rows_hbm.at[here], rows_ref.at[pl.ds(n * half, half)], sems.at[n]
            )
        )
        copies[n].start()
    _, named, rank, sub = slot_ranks(routes_ref, out_ref.shape[0], tokens, base)
    mains = jnp.concatenate([as_bf16(named & main_place(sub, rank, h)) for h in range(2)], axis=1)
    for n in range(2):
        here = slice(n * half, (n + 1) * half)
        copies[n].wait()
        features = rows_ref[here, :].astype(F32)
        inverse = lax.rsqrt(jnp.mean(features * features, axis=-1, keepdims=True) + EPS)
        normed_ref[here, :] = (features * inverse * gain_ref[...]).astype(BF16)
    for c in range(FOLD):
        used = [u for u in range(2) if tail_used(u, c)]
        tails = [as_bf16(named & tail_place(sub, rank, u, c)) for u in used]
        starts = [h * LANES + c * PIECE for h in range(2)] + [MAIN + u * PIECE for u in used]
        out_ref[:, c * PIECE : (c + 1) * PIECE] = dot(
            jnp.concatenate([mains, *tails], axis=1),
            jnp.concatenate([normed_ref[:, start : start + PIECE] for start in starts], axis=0),
        ).astype(BF16)


def send_rows(expert_in, gain, routes_t, own, experts, chunk):
    tokens = expert_in.shape[0] // lax.axis_size("tp")
    width = expert_in.shape[1]
    return pl.pallas_call(
        partial(send_kernel, chunk * SLOTS),
        out_shape=jax.ShapeDtypeStruct((experts * SUB, LANES), BF16),
        grid_spec=pltpu.PrefetchScalarGridSpec(
            num_scalar_prefetch=1,
            grid=(1,),
            in_specs=[
                ANY,
                pl.BlockSpec((1, width), lambda i, own: (0, 0)),
                pl.BlockSpec((K, tokens), lambda i, own: (0, own[0])),
            ],
            out_specs=VMEM,
            scratch_shapes=[pltpu.VMEM((tokens, width), BF16)] * 2 + [pltpu.SemaphoreType.DMA((2,))],
        ),
        cost_estimate=pl.CostEstimate(flops=2_000_000_000, bytes_accessed=2_100_000, transcendentals=128),
        name="send_rows",
    )(own, expert_in, gain.reshape(1, width), routes_t)


def places(shape, dense_axis, where):
    dense = lax.broadcasted_iota(jnp.int32, shape, dense_axis)
    row = lax.broadcasted_iota(jnp.int32, shape, 1 - dense_axis)
    return as_bf16((dense % EXPERTS_G == row // SUB) & where(row % SUB, dense // EXPERTS_G))


def main_maps(shape, dense_axis):
    return [places(shape, dense_axis, lambda sub, slot, h=h: main_place(sub, slot, h)) for h in range(2)]


def tail_maps(shape, dense_axis, c):
    return [
        places(shape, dense_axis, lambda sub, slot, u=u: tail_place(sub, slot, u, c))
        for u in range(2)
        if tail_used(u, c)
    ]


def dense_columns(c):
    starts = [h * LANES + c * PIECE for h in range(2)]
    return starts + [MAIN + u * PIECE for u in range(2) if tail_used(u, c)]


def unpack(x_ref, out_ref):
    experts = x_ref.shape[0] // SUB
    mains = main_maps((DENSE, GROUP), 0)
    tails = {}

    def put(block, g, start):
        for k in range(SLOTS):
            to = k * experts + g * EXPERTS_G
            out_ref[to : to + EXPERTS_G, start : start + PIECE] = block[
                k * EXPERTS_G : (k + 1) * EXPERTS_G
            ].astype(BF16)

    for c in range(FOLD):
        maps = jnp.concatenate(mains + tail_maps((DENSE, GROUP), 0, c), axis=0)
        for g in range(experts // EXPERTS_G):
            found = dot(maps, x_ref[g * GROUP : (g + 1) * GROUP, c * PIECE : (c + 1) * PIECE])
            for n, start in enumerate(dense_columns(c)):
                block = found[n * DENSE : (n + 1) * DENSE]
                if start < MAIN:
                    put(block, g, start)
                else:
                    tails[start, g] = tails[start, g] + block if (start, g) in tails else block
    for (start, g), block in tails.items():
        put(block, g, start)


def pack_kernel(a_ref, b_ref, out_ref):
    experts = out_ref.shape[0] // SUB
    mains = main_maps((GROUP, DENSE), 1)
    for c in range(FOLD):
        maps = jnp.concatenate(mains + tail_maps((GROUP, DENSE), 1, c), axis=1)
        for g in range(experts // EXPERTS_G):
            pieces = []
            for start in dense_columns(c):
                columns = slice(start, start + PIECE)
                for k in range(SLOTS):
                    to = k * experts + g * EXPERTS_G
                    here = slice(to, to + EXPERTS_G)
                    pieces.append(
                        (a_ref[here, columns].astype(F32) + b_ref[here, columns].astype(F32)).astype(BF16)
                    )
            out_ref[g * GROUP : (g + 1) * GROUP, c * PIECE : (c + 1) * PIECE] = dot(
                maps, jnp.concatenate(pieces, axis=0)
            ).astype(BF16)


def pack_sum(a, b):
    rows = a.shape[0] // SLOTS * SUB
    return pl.pallas_call(
        pack_kernel,
        out_shape=jax.ShapeDtypeStruct((rows, LANES), BF16),
        in_specs=[VMEM] * 2,
        out_specs=VMEM,
        cost_estimate=pl.CostEstimate(flops=800_000_000, bytes_accessed=a.size * 6, transcendentals=0),
        compiler_params=pltpu.CompilerParams(vmem_limit_bytes=SMALL),
        name="pack_sum",
    )(a, b)


def ffn_kernel(*refs):
    sources, out_ref, dense_ref, held, sems = refs[:7], refs[7], refs[8], refs[9:16], refs[16]
    rows, *copies = [
        pltpu.make_async_copy(source, ref, sems.at[n])
        for n, (source, ref) in enumerate(zip(sources, held))
    ]
    rows.start()
    for copy in copies:
        copy.start()
    x_ref, ga_ref, ua_ref, gb_ref, ub_ref, da_ref, db_ref = held
    rows.wait()
    unpack(x_ref, dense_ref)
    x = dense_ref[...]
    copies[0].wait()
    copies[1].wait()
    hidden_a = (jax.nn.silu(dot(x, ga_ref[...])) * dot(x, ua_ref[...])).astype(BF16)
    copies[2].wait()
    copies[3].wait()
    hidden_b = (jax.nn.silu(dot(x, gb_ref[...])) * dot(x, ub_ref[...])).astype(BF16)
    copies[4].wait()
    copies[5].wait()
    step = 2 * PIECE
    for c in range(WIDTH // step):
        columns = slice(c * step, (c + 1) * step)
        out_ref[:, columns] = (
            dot(hidden_a, da_ref[:, columns]) + dot(hidden_b, db_ref[:, columns])
        ).astype(BF16)


def half_ffn(x, ga, gb, ua, ub, da, db):
    operands = (x, ga, ua, gb, ub, da, db)
    dense = x.shape[0] // SUB * SLOTS
    hidden = ga.shape[1] + gb.shape[1]
    return pl.pallas_call(
        ffn_kernel,
        out_shape=jax.ShapeDtypeStruct((dense, WIDTH), BF16),
        in_specs=[ANY] * 7,
        out_specs=VMEM,
        scratch_shapes=[pltpu.VMEM((dense, WIDTH), BF16)]
        + [pltpu.VMEM(operand.shape, BF16) for operand in operands]
        + [pltpu.SemaphoreType.DMA((7,))],
        cost_estimate=pl.CostEstimate(
            flops=3_500_000_000,
            bytes_accessed=x.size * 4 + 6 * ga.size * 2,
            transcendentals=dense * hidden,
        ),
        compiler_params=pltpu.CompilerParams(vmem_limit_bytes=LARGE),
        name="half_ffn",
    )(*operands)


def combine_kernel(base, own_ref, values_ref, routes_ref, weight_ref, *refs):
    del own_ref
    copy = None
    if base:
        source, out_ref, before_ref, sem = refs
        copy = pltpu.make_async_copy(source, before_ref, sem)
        copy.start()
    else:
        (out_ref,) = refs
    rows, tokens = values_ref.shape[0], out_ref.shape[0]
    routes = jnp.transpose(routes_ref[...].astype(F32)).astype(jnp.int32)
    weights = jnp.transpose(weight_ref[...])
    row = lax.broadcasted_iota(jnp.int32, (tokens, rows), 1)
    expert, sub = row // SUB, row % SUB
    by_first, by_second = expert == routes[:, 0:1], expert == routes[:, 1:2]
    named = by_first | by_second
    earlier = lax.broadcasted_iota(jnp.int32, (tokens, tokens), 1) < lax.broadcasted_iota(
        jnp.int32, (tokens, tokens), 0
    )
    slot = dot(as_bf16(earlier), as_bf16(named)).astype(jnp.int32) - base
    weight = jnp.where(
        named & (slot < SLOTS), jnp.where(by_first, weights[:, 0:1], weights[:, 1:2]), 0.0
    )
    high = weight.astype(BF16).astype(F32)
    low = weight - high

    def split(chosen):
        return [jnp.where(chosen, part, 0.0).astype(BF16) for part in (high, low)]

    totals = {}
    mains = [part for h in range(2) for part in split(main_place(sub, slot, h))]
    for c in range(FOLD):
        maps = list(mains)
        for u in range(2):
            if tail_used(u, c):
                maps += split(tail_place(sub, slot, u, c))
        found = dot(jnp.concatenate(maps, axis=0), values_ref[:, c * PIECE : (c + 1) * PIECE])
        for n, start in enumerate(dense_columns(c)):
            block = found[2 * n * tokens : (2 * n + 1) * tokens] + found[(2 * n + 1) * tokens : (2 * n + 2) * tokens]
            totals[start] = totals[start] + block if start in totals else block
    if copy is not None:
        copy.wait()
    for start, total in totals.items():
        columns = slice(start, start + PIECE)
        if copy is not None:
            total += before_ref[:, columns]
        out_ref[:, columns] = total.astype(out_ref.dtype)


def combine(chunk, values, routes_t, weight_t, own, tokens, before=None):
    rest = () if before is None else (before,)
    return pl.pallas_call(
        partial(combine_kernel, chunk * SLOTS),
        out_shape=jax.ShapeDtypeStruct((tokens, WIDTH), F32 if before is None else BF16),
        grid_spec=pltpu.PrefetchScalarGridSpec(
            num_scalar_prefetch=1,
            grid=(1,),
            in_specs=[
                VMEM,
                pl.BlockSpec((K, tokens), lambda i, own: (0, own[0])),
                pl.BlockSpec((K, tokens), lambda i, own: (0, own[0])),
            ]
            + [ANY] * len(rest),
            out_specs=VMEM if before is None else pl.BlockSpec((tokens, WIDTH), lambda i, own: (0, 0)),
            scratch_shapes=[pltpu.VMEM((tokens, WIDTH), F32), pltpu.SemaphoreType.DMA] if rest else [],
        ),
        cost_estimate=pl.CostEstimate(flops=1_500_000_000, bytes_accessed=2_100_000, transcendentals=0),
        compiler_params=pltpu.CompilerParams(vmem_limit_bytes=LARGE),
        name="combine",
    )(own, values, routes_t, weight_t, *rest)


def exchanged(rows):
    experts = rows.shape[0] // SUB
    out = lax.all_to_all(
        rows.reshape(experts, SUB, LANES), "ep", split_axis=0, concat_axis=0, tiled=True
    )
    return out.reshape(rows.shape)


def on_device(
    pool_in,
    w_pool,
    pool_scale,
    w_out,
    expert_in,
    ffn_gain,
    routes,
    route_weight,
    w_gate,
    w_up,
    w_down,
):
    rows_here = pool_in.shape[0]
    tokens = routes.shape[0] // lax.axis_size("tp")
    experts = lax.axis_size("ep") * w_gate.shape[0]
    own = lax.axis_index("tp").astype(jnp.int32).reshape(1)
    routes_t, weight_t = routes.T, route_weight.T
    before = passed_along(pool_in[rows_here - (WMAX - 1) :], ("ep", "tp"), 1)

    gate, up, down = w_gate[0], w_up[0], w_down[0]
    gate_b, up_b = swapped(gate, 0), swapped(up, 0)
    down_b = swapped(down, 0)
    ffn = lambda x: half_ffn(x, gate, gate_b, up, up_b, down, down_b)

    mine = []
    for n in range(CHUNKS):
        sent = send_rows(expert_in, ffn_gain, routes_t, own, experts, n)
        mine.append(exchanged(sent))
    expert_out = None
    for n in range(CHUNKS):
        theirs = swapped(mine[n], 1)
        partial_sum = ffn(theirs)
        back = swapped(partial_sum, 1)
        kept = ffn(mine[n])
        results = pack_sum(kept, back)
        returned = exchanged(results)
        expert_out = combine(n, returned, routes_t, weight_t, own, tokens, expert_out)

    extended = jnp.concatenate([before, pool_in], axis=0).astype(F32)
    positions = (
        lax.axis_index(("ep", "tp")) * rows_here + jnp.arange(rows_here)
    ).astype(F32)
    pooled = pooled_rows(extended, positions)
    group_count = w_pool.shape[0]
    grouped = jnp.einsum(
        "tgc,gcd->tgd",
        pooled.reshape(rows_here, group_count, GDIM),
        w_pool,
        preferred_element_type=F32,
    )
    scaled = (grouped.reshape(rows_here, -1) * pool_scale).astype(BF16)
    mixer_out = dot(scaled, w_out).astype(BF16)
    return (mixer_out, expert_out)


def solution(mesh):
    placed = (
        P(("ep", "tp"), None),
        P(),
        P(),
        P(),
        P("ep", None),
        P(),
        P("ep", None),
        P("ep", None),
        P("ep", None, "tp"),
        P("ep", None, "tp"),
        P("ep", "tp", None),
    )
    return jax.shard_map(
        on_device,
        mesh=mesh,
        in_specs=placed,
        out_specs=(P(("ep", "tp"), None), P(("ep", "tp"), None)),
        check_vma=False,
    )
```

```python
from functools import partial

import jax
import jax.numpy as jnp
from jax import lax
from jax.experimental import pallas as pl
from jax.experimental.pallas import tpu as pltpu
from jax.sharding import PartitionSpec as P


GDIM = 128
WMAX = 16
K = 2
EPS = 0.05

CHUNKS = 2
SLOTS = 3
SUB = 8
LANES = 768
PIECE = 256
FOLD = LANES // PIECE
MAIN = 2 * LANES
WIDTH = MAIN + 2 * PIECE
EXPERTS_G = 32
GROUP = EXPERTS_G * SUB
DENSE = EXPERTS_G * SLOTS
SMALL = 16 * 1024 * 1024
LARGE = 52 * 1024 * 1024
BF16 = jnp.bfloat16
F32 = jnp.float32
VMEM = pl.BlockSpec(memory_space=pltpu.VMEM)
ANY = pl.BlockSpec(memory_space=pl.ANY)


def passed_along(array, axis, by):
    length = lax.axis_size(axis)
    pairs = [(i, i + by) for i in range(length) if 0 <= i + by < length]
    return lax.ppermute(array, axis, pairs)


def swapped(array, flip):
    eps, tps = lax.axis_size("ep"), lax.axis_size("tp")
    pairs = []
    for e in range(eps):
        for y in range(tps):
            other = y ^ 1 if (e + flip) % 2 == 0 else tps - 1 - y
            pairs.append((e * tps + y, e * tps + other))
    return lax.ppermute(array, ("ep", "tp"), pairs)


def window_sizes(width):
    group_of = jnp.arange(width) // GDIM
    level = group_of % 4
    return jnp.where(
        level == 0, 2.0, jnp.where(level == 1, 4.0, jnp.where(level == 2, 8.0, 16.0))
    ).astype(F32)


def pooled_rows(extended, positions):
    extent = extended.shape[0] - (WMAX - 1)
    window = window_sizes(extended.shape[1])
    running = jnp.zeros((extent, extended.shape[1]), F32)
    picked = running
    for offset in range(WMAX):
        running = running + extended[WMAX - 1 - offset : WMAX - 1 - offset + extent]
        if offset + 1 in (2, 4, 8, 16):
            picked = jnp.where(window[None, :] == offset + 1, running, picked)
    counted = jnp.minimum(positions[:, None] + 1.0, window[None, :])
    return (picked / counted - extended[WMAX - 1 :]).astype(BF16)


def as_bf16(mask):
    return mask.astype(F32).astype(BF16)


def dot(a, b):
    return jnp.dot(a, b, preferred_element_type=F32)


def slot_ranks(routes_ref, rows, tokens, base):
    first, second = routes_ref[0:1, :], routes_ref[1:2, :]
    row = lax.broadcasted_iota(jnp.int32, (rows, tokens), 0)
    expert, sub = row // SUB, row % SUB
    by_first, by_second = expert == first, expert == second
    named = by_first | by_second
    before = lax.broadcasted_iota(jnp.int32, (tokens, tokens), 0) < lax.broadcasted_iota(
        jnp.int32, (tokens, tokens), 1
    )
    rank = dot(as_bf16(named), as_bf16(before)).astype(jnp.int32) - base
    return by_first, named, rank, sub


def main_place(sub, slot, half):
    return (sub == 2 * slot + half) & (sub < 2 * SLOTS) & (slot >= 0)


def tail_place(sub, slot, piece, c):
    return (sub >= 2 * SLOTS) & ((sub - 2 * SLOTS) * FOLD + c == 2 * slot + piece) & (slot >= 0)


def tail_used(piece, c):
    return any((r * FOLD + c - piece) % 2 == 0 for r in range(SUB - 2 * SLOTS))


def send_kernel(
    base,
    own_ref,
    rows_hbm,
    gain_hbm,
    routes_hbm,
    out_hbm,
    rows_ref,
    normed_ref,
    gain_ref,
    routes_ref,
    out_ref,
    sems,
    out_sems,
):
    tokens = rows_ref.shape[0]
    half = tokens // 2
    first = pl.multiple_of(own_ref[0] * tokens, tokens)
    fetches = [
        pltpu.make_async_copy(routes_hbm.at[:, pl.ds(first, tokens)], routes_ref, sems.at[2]),
        pltpu.make_async_copy(gain_hbm, gain_ref, sems.at[3]),
    ]
    halves = [
        pltpu.make_async_copy(
            rows_hbm.at[pl.ds(pl.multiple_of(first + n * half, half), half)],
            rows_ref.at[pl.ds(n * half, half)],
            sems.at[n],
        )
        for n in range(2)
    ]
    for copy in fetches + halves:
        copy.start()
    fetches[0].wait()
    _, named, rank, sub = slot_ranks(routes_ref, out_ref.shape[0], tokens, base)
    mains = jnp.concatenate([as_bf16(named & main_place(sub, rank, h)) for h in range(2)], axis=1)
    fetches[1].wait()
    for n in range(2):
        here = slice(n * half, (n + 1) * half)
        halves[n].wait()
        features = rows_ref[here, :].astype(F32)
        inverse = lax.rsqrt(jnp.mean(features * features, axis=-1, keepdims=True) + EPS)
        normed_ref[here, :] = (features * inverse * gain_ref[...]).astype(BF16)
    outs = []
    for c in range(FOLD):
        used = [u for u in range(2) if tail_used(u, c)]
        tails = [as_bf16(named & tail_place(sub, rank, u, c)) for u in used]
        starts = [h * LANES + c * PIECE for h in range(2)] + [MAIN + u * PIECE for u in used]
        out_ref[:, c * PIECE : (c + 1) * PIECE] = dot(
            jnp.concatenate([mains, *tails], axis=1),
            jnp.concatenate([normed_ref[:, start : start + PIECE] for start in starts], axis=0),
        ).astype(BF16)
        outs.append(column_copy(out_ref, out_hbm, c * PIECE, PIECE, out_sems.at[c]))
        outs[-1].start()
    for copy in outs:
        copy.wait()


def column_copy(source, target, at, width, sem):
    columns = pl.ds(at, width)
    return pltpu.make_async_copy(source.at[:, columns], target.at[:, columns], sem)


def send_rows(expert_in, gain, routes_t, own, experts, chunk):
    tokens = expert_in.shape[0] // lax.axis_size("tp")
    width = expert_in.shape[1]
    return pl.pallas_call(
        partial(send_kernel, chunk * SLOTS),
        out_shape=jax.ShapeDtypeStruct((experts * SUB, LANES), BF16),
        grid_spec=pltpu.PrefetchScalarGridSpec(
            num_scalar_prefetch=1,
            grid=(1,),
            in_specs=[ANY] * 3,
            out_specs=ANY,
            scratch_shapes=[
                pltpu.VMEM((tokens, width), BF16),
                pltpu.VMEM((tokens, width), BF16),
                pltpu.VMEM((1, width), F32),
                pltpu.VMEM((K, tokens), jnp.int32),
                pltpu.VMEM((experts * SUB, LANES), BF16),
                pltpu.SemaphoreType.DMA((4,)),
                pltpu.SemaphoreType.DMA((FOLD,)),
            ],
        ),
        cost_estimate=pl.CostEstimate(flops=2_000_000_000, bytes_accessed=2_100_000, transcendentals=128),
        name="send_rows",
    )(own, expert_in, gain.reshape(1, width), routes_t)


def places(shape, dense_axis, where):
    dense = lax.broadcasted_iota(jnp.int32, shape, dense_axis)
    row = lax.broadcasted_iota(jnp.int32, shape, 1 - dense_axis)
    return as_bf16((dense % EXPERTS_G == row // SUB) & where(row % SUB, dense // EXPERTS_G))


def main_maps(shape, dense_axis):
    return [places(shape, dense_axis, lambda sub, slot, h=h: main_place(sub, slot, h)) for h in range(2)]


def tail_maps(shape, dense_axis, c):
    return [
        places(shape, dense_axis, lambda sub, slot, u=u: tail_place(sub, slot, u, c))
        for u in range(2)
        if tail_used(u, c)
    ]


def dense_columns(c):
    starts = [h * LANES + c * PIECE for h in range(2)]
    return starts + [MAIN + u * PIECE for u in range(2) if tail_used(u, c)]


def unpack(x_ref, out_ref):
    experts = x_ref.shape[0] // SUB
    mains = main_maps((DENSE, GROUP), 0)
    tails = {}

    def put(block, g, start):
        for k in range(SLOTS):
            to = k * experts + g * EXPERTS_G
            out_ref[to : to + EXPERTS_G, start : start + PIECE] = block[
                k * EXPERTS_G : (k + 1) * EXPERTS_G
            ].astype(BF16)

    for c in range(FOLD):
        maps = jnp.concatenate(mains + tail_maps((DENSE, GROUP), 0, c), axis=0)
        for g in range(experts // EXPERTS_G):
            found = dot(maps, x_ref[g * GROUP : (g + 1) * GROUP, c * PIECE : (c + 1) * PIECE])
            for n, start in enumerate(dense_columns(c)):
                block = found[n * DENSE : (n + 1) * DENSE]
                if start < MAIN:
                    put(block, g, start)
                else:
                    tails[start, g] = tails[start, g] + block if (start, g) in tails else block
    for (start, g), block in tails.items():
        put(block, g, start)


def pack_kernel(a_ref, b_ref, out_hbm, out_ref, sems):
    copies = []
    experts = out_ref.shape[0] // SUB
    mains = main_maps((GROUP, DENSE), 1)
    for c in range(FOLD):
        maps = jnp.concatenate(mains + tail_maps((GROUP, DENSE), 1, c), axis=1)
        for g in range(experts // EXPERTS_G):
            pieces = []
            for start in dense_columns(c):
                columns = slice(start, start + PIECE)
                for k in range(SLOTS):
                    to = k * experts + g * EXPERTS_G
                    here = slice(to, to + EXPERTS_G)
                    pieces.append(
                        (a_ref[here, columns].astype(F32) + b_ref[here, columns].astype(F32)).astype(BF16)
                    )
            out_ref[g * GROUP : (g + 1) * GROUP, c * PIECE : (c + 1) * PIECE] = dot(
                maps, jnp.concatenate(pieces, axis=0)
            ).astype(BF16)
        copies.append(column_copy(out_ref, out_hbm, c * PIECE, PIECE, sems.at[c]))
        copies[-1].start()
    for copy in copies:
        copy.wait()


def pack_sum(a, b):
    rows = a.shape[0] // SLOTS * SUB
    return pl.pallas_call(
        pack_kernel,
        out_shape=jax.ShapeDtypeStruct((rows, LANES), BF16),
        in_specs=[VMEM] * 2,
        out_specs=ANY,
        scratch_shapes=[pltpu.VMEM((rows, LANES), BF16), pltpu.SemaphoreType.DMA((FOLD,))],
        cost_estimate=pl.CostEstimate(flops=800_000_000, bytes_accessed=a.size * 6, transcendentals=0),
        compiler_params=pltpu.CompilerParams(vmem_limit_bytes=SMALL),
        name="pack_sum",
    )(a, b)


def ffn_kernel(*refs):
    sources, out_ref, dense_ref, held, sems = refs[:7], refs[7], refs[8], refs[9:16], refs[16]
    rows, *copies = [
        pltpu.make_async_copy(source, ref, sems.at[n])
        for n, (source, ref) in enumerate(zip(sources, held))
    ]
    rows.start()
    for copy in copies[:4]:
        copy.start()
    x_ref, ga_ref, ua_ref, gb_ref, ub_ref, da_ref, db_ref = held
    rows.wait()
    for copy in copies[4:]:
        copy.start()
    unpack(x_ref, dense_ref)
    x = dense_ref[...]
    copies[0].wait()
    copies[1].wait()
    hidden_a = (jax.nn.silu(dot(x, ga_ref[...])) * dot(x, ua_ref[...])).astype(BF16)
    copies[2].wait()
    copies[3].wait()
    hidden_b = (jax.nn.silu(dot(x, gb_ref[...])) * dot(x, ub_ref[...])).astype(BF16)
    copies[4].wait()
    copies[5].wait()
    step = 2 * PIECE
    for c in range(WIDTH // step):
        columns = slice(c * step, (c + 1) * step)
        out_ref[:, columns] = (
            dot(hidden_a, da_ref[:, columns]) + dot(hidden_b, db_ref[:, columns])
        ).astype(BF16)


def half_ffn(x, ga, gb, ua, ub, da, db):
    operands = (x, ga, ua, gb, ub, da, db)
    dense = x.shape[0] // SUB * SLOTS
    hidden = ga.shape[1] + gb.shape[1]
    return pl.pallas_call(
        ffn_kernel,
        out_shape=jax.ShapeDtypeStruct((dense, WIDTH), BF16),
        in_specs=[ANY] * 7,
        out_specs=VMEM,
        scratch_shapes=[pltpu.VMEM((dense, WIDTH), BF16)]
        + [pltpu.VMEM(operand.shape, BF16) for operand in operands]
        + [pltpu.SemaphoreType.DMA((7,))],
        cost_estimate=pl.CostEstimate(
            flops=3_500_000_000,
            bytes_accessed=x.size * 4 + 6 * ga.size * 2,
            transcendentals=dense * hidden,
        ),
        compiler_params=pltpu.CompilerParams(vmem_limit_bytes=LARGE),
        name="half_ffn",
    )(*operands)


def combine_kernel(base, own_ref, values_ref, routes_ref, weight_ref, *refs):
    first = bool(base == 0)
    if first:
        (out_ref,) = refs
    else:
        source, out_hbm, before_ref, out_ref, sem, out_sems = refs
        fetch = pltpu.make_async_copy(source, before_ref, sem)
        fetch.start()
    rows, tokens = values_ref.shape[0], out_ref.shape[0]
    lanes = pl.ds(pl.multiple_of(own_ref[0] * tokens, tokens), tokens)
    routes = jnp.transpose(routes_ref[:, lanes].astype(F32)).astype(jnp.int32)
    weights = jnp.transpose(weight_ref[:, lanes])
    row = lax.broadcasted_iota(jnp.int32, (tokens, rows), 1)
    expert, sub = row // SUB, row % SUB
    by_first, by_second = expert == routes[:, 0:1], expert == routes[:, 1:2]
    named = by_first | by_second
    earlier = lax.broadcasted_iota(jnp.int32, (tokens, tokens), 1) < lax.broadcasted_iota(
        jnp.int32, (tokens, tokens), 0
    )
    slot = dot(as_bf16(earlier), as_bf16(named)).astype(jnp.int32) - base
    weight = jnp.where(
        named & (slot < SLOTS), jnp.where(by_first, weights[:, 0:1], weights[:, 1:2]), 0.0
    )
    high = weight.astype(BF16).astype(F32)
    low = weight - high

    def split(chosen):
        return [jnp.where(chosen, part, 0.0).astype(BF16) for part in (high, low)]

    copies = []

    def put(total, start):
        columns = slice(start, start + PIECE)
        if first:
            out_ref[:, columns] = total
            return
        if not copies:
            fetch.wait()
        out_ref[:, columns] = (total + before_ref[:, columns]).astype(BF16)
        copies.append(column_copy(out_ref, out_hbm, start, PIECE, out_sems.at[len(copies)]))
        copies[-1].start()

    tails = {}
    mains = [part for h in range(2) for part in split(main_place(sub, slot, h))]
    for c in range(FOLD):
        maps = list(mains)
        for u in range(2):
            if tail_used(u, c):
                maps += split(tail_place(sub, slot, u, c))
        found = dot(jnp.concatenate(maps, axis=0), values_ref[:, c * PIECE : (c + 1) * PIECE])
        for n, start in enumerate(dense_columns(c)):
            at = 2 * n * tokens
            block = found[at : at + tokens] + found[at + tokens : at + 2 * tokens]
            if start < MAIN:
                put(block, start)
            else:
                tails[start] = tails[start] + block if start in tails else block
    for start, total in tails.items():
        put(total, start)
    for copy in copies:
        copy.wait()


def combine(chunk, values, routes_t, weight_t, own, tokens, before=None):
    first = before is None
    pieces = WIDTH // PIECE
    return pl.pallas_call(
        partial(combine_kernel, chunk * SLOTS),
        out_shape=jax.ShapeDtypeStruct((tokens, WIDTH), F32 if first else BF16),
        grid_spec=pltpu.PrefetchScalarGridSpec(
            num_scalar_prefetch=1,
            grid=(1,),
            in_specs=[VMEM] * 3 + ([] if first else [ANY]),
            out_specs=VMEM if first else ANY,
            scratch_shapes=[]
            if first
            else [
                pltpu.VMEM((tokens, WIDTH), F32),
                pltpu.VMEM((tokens, WIDTH), BF16),
                pltpu.SemaphoreType.DMA,
                pltpu.SemaphoreType.DMA((pieces,)),
            ],
        ),
        cost_estimate=pl.CostEstimate(flops=1_500_000_000, bytes_accessed=2_100_000, transcendentals=0),
        compiler_params=pltpu.CompilerParams(vmem_limit_bytes=LARGE),
        name="combine",
    )(own, values, routes_t, weight_t, *(() if first else (before,)))


def exchanged(rows):
    experts = rows.shape[0] // SUB
    out = lax.all_to_all(
        rows.reshape(experts, SUB, LANES), "ep", split_axis=0, concat_axis=0, tiled=True
    )
    return out.reshape(rows.shape)


def on_device(
    pool_in,
    w_pool,
    pool_scale,
    w_out,
    expert_in,
    ffn_gain,
    routes,
    route_weight,
    w_gate,
    w_up,
    w_down,
):
    rows_here = pool_in.shape[0]
    tokens = routes.shape[0] // lax.axis_size("tp")
    experts = lax.axis_size("ep") * w_gate.shape[0]
    own = lax.axis_index("tp").astype(jnp.int32).reshape(1)
    routes_t, weight_t = routes.T, route_weight.T
    before = passed_along(pool_in[rows_here - (WMAX - 1) :], ("ep", "tp"), 1)

    gate, up, down = w_gate[0], w_up[0], w_down[0]
    gate_b, up_b = swapped(gate, 0), swapped(up, 0)
    down_b = swapped(down, 0)
    ffn = lambda x: half_ffn(x, gate, gate_b, up, up_b, down, down_b)

    mine = []
    for n in range(CHUNKS):
        sent = send_rows(expert_in, ffn_gain, routes_t, own, experts, n)
        mine.append(exchanged(sent))
    expert_out = None
    for n in range(CHUNKS):
        theirs = swapped(mine[n], 1)
        partial_sum = ffn(theirs)
        back = swapped(partial_sum, 1)
        kept = ffn(mine[n])
        results = pack_sum(kept, back)
        returned = exchanged(results)
        expert_out = combine(n, returned, routes_t, weight_t, own, tokens, expert_out)

    extended = jnp.concatenate([before, pool_in], axis=0).astype(F32)
    positions = (lax.axis_index(("ep", "tp")) * rows_here + jnp.arange(rows_here)).astype(F32)
    pooled = pooled_rows(extended, positions)
    group_count = w_pool.shape[0]
    grouped = jnp.einsum(
        "tgc,gcd->tgd",
        pooled.reshape(rows_here, group_count, GDIM),
        w_pool,
        preferred_element_type=F32,
    )
    scaled = (grouped.reshape(rows_here, -1) * pool_scale).astype(BF16)
    mixer_out = dot(scaled, w_out).astype(BF16)
    return (mixer_out, expert_out)


def solution(mesh):
    placed = (
        P(("ep", "tp"), None),
        P(),
        P(),
        P(),
        P("ep", None),
        P(),
        P("ep", None),
        P("ep", None),
        P("ep", None, "tp"),
        P("ep", None, "tp"),
        P("ep", "tp", None),
    )
    return jax.shard_map(
        on_device,
        mesh=mesh,
        in_specs=placed,
        out_specs=(P(("ep", "tp"), None), P(("ep", "tp"), None)),
        check_vma=False,
    )
```

```python
from functools import partial

import jax
import jax.numpy as jnp
from jax import lax
from jax.experimental import pallas as pl
from jax.experimental.pallas import tpu as pltpu
from jax.sharding import PartitionSpec as P


GDIM = 128
WMAX = 16
K = 2
EPS = 0.05

CHUNKS = 2
SLOTS = 3
SUB = 8
LANES = 768
PIECE = 256
FOLD = LANES // PIECE
MAIN = 2 * LANES
WIDTH = MAIN + 2 * PIECE
EXPERTS_G = 32
GROUP = EXPERTS_G * SUB
DENSE = EXPERTS_G * SLOTS
SMALL = 16 * 1024 * 1024
LARGE = 52 * 1024 * 1024
BF16 = jnp.bfloat16
F32 = jnp.float32
VMEM = pl.BlockSpec(memory_space=pltpu.VMEM)
ANY = pl.BlockSpec(memory_space=pl.ANY)


def passed_along(array, axis, by):
    length = lax.axis_size(axis)
    pairs = [(i, i + by) for i in range(length) if 0 <= i + by < length]
    return lax.ppermute(array, axis, pairs)


def swapped(array, flip):
    eps, tps = lax.axis_size("ep"), lax.axis_size("tp")
    pairs = []
    for e in range(eps):
        for y in range(tps):
            other = y ^ 1 if (e + flip) % 2 == 0 else tps - 1 - y
            pairs.append((e * tps + y, e * tps + other))
    return lax.ppermute(array, ("ep", "tp"), pairs)


def window_sizes(width):
    group_of = jnp.arange(width) // GDIM
    level = group_of % 4
    return jnp.where(
        level == 0, 2.0, jnp.where(level == 1, 4.0, jnp.where(level == 2, 8.0, 16.0))
    ).astype(F32)


def pooled_rows(extended, positions):
    extent = extended.shape[0] - (WMAX - 1)
    window = window_sizes(extended.shape[1])
    running = jnp.zeros((extent, extended.shape[1]), F32)
    picked = running
    for offset in range(WMAX):
        running = running + extended[WMAX - 1 - offset : WMAX - 1 - offset + extent]
        if offset + 1 in (2, 4, 8, 16):
            picked = jnp.where(window[None, :] == offset + 1, running, picked)
    counted = jnp.minimum(positions[:, None] + 1.0, window[None, :])
    return (picked / counted - extended[WMAX - 1 :]).astype(BF16)


def as_bf16(mask):
    return mask.astype(F32).astype(BF16)


def dot(a, b):
    return jnp.dot(a, b, preferred_element_type=F32)


def slot_ranks(routes_ref, rows, tokens, base):
    first, second = routes_ref[0:1, :], routes_ref[1:2, :]
    row = lax.broadcasted_iota(jnp.int32, (rows, tokens), 0)
    expert, sub = row // SUB, row % SUB
    by_first, by_second = expert == first, expert == second
    named = by_first | by_second
    before = lax.broadcasted_iota(jnp.int32, (tokens, tokens), 0) < lax.broadcasted_iota(
        jnp.int32, (tokens, tokens), 1
    )
    rank = dot(as_bf16(named), as_bf16(before)).astype(jnp.int32) - base
    return by_first, named, rank, sub


def main_place(sub, slot, half):
    return (sub == 2 * slot + half) & (sub < 2 * SLOTS) & (slot >= 0)


def tail_place(sub, slot, piece, c):
    return (sub >= 2 * SLOTS) & ((sub - 2 * SLOTS) * FOLD + c == 2 * slot + piece) & (slot >= 0)


def tail_used(piece, c):
    return any((r * FOLD + c - piece) % 2 == 0 for r in range(SUB - 2 * SLOTS))


def send_kernel(
    base,
    own_ref,
    rows_hbm,
    gain_hbm,
    routes_hbm,
    out_hbm,
    rows_ref,
    normed_ref,
    gain_ref,
    routes_ref,
    out_ref,
    sems,
    out_sems,
):
    tokens = rows_ref.shape[0]
    half = tokens // 2
    first = pl.multiple_of(own_ref[0] * tokens, tokens)
    fetches = [
        pltpu.make_async_copy(routes_hbm.at[:, pl.ds(first, tokens)], routes_ref, sems.at[2]),
        pltpu.make_async_copy(gain_hbm, gain_ref, sems.at[3]),
    ]
    halves = [
        pltpu.make_async_copy(
            rows_hbm.at[pl.ds(pl.multiple_of(first + n * half, half), half)],
            rows_ref.at[pl.ds(n * half, half)],
            sems.at[n],
        )
        for n in range(2)
    ]
    for copy in fetches + halves:
        copy.start()
    fetches[0].wait()
    _, named, rank, sub = slot_ranks(routes_ref, out_ref.shape[0], tokens, base)
    mains = jnp.concatenate([as_bf16(named & main_place(sub, rank, h)) for h in range(2)], axis=1)
    fetches[1].wait()
    for n in range(2):
        here = slice(n * half, (n + 1) * half)
        halves[n].wait()
        features = rows_ref[here, :].astype(F32)
        inverse = lax.rsqrt(jnp.mean(features * features, axis=-1, keepdims=True) + EPS)
        normed_ref[here, :] = (features * inverse * gain_ref[...]).astype(BF16)
    outs = []
    for c in range(FOLD):
        used = [u for u in range(2) if tail_used(u, c)]
        tails = [as_bf16(named & tail_place(sub, rank, u, c)) for u in used]
        starts = [h * LANES + c * PIECE for h in range(2)] + [MAIN + u * PIECE for u in used]
        out_ref[:, c * PIECE : (c + 1) * PIECE] = dot(
            jnp.concatenate([mains, *tails], axis=1),
            jnp.concatenate([normed_ref[:, start : start + PIECE] for start in starts], axis=0),
        ).astype(BF16)
        outs.append(column_copy(out_ref, out_hbm, c * PIECE, PIECE, out_sems.at[c]))
        outs[-1].start()
    for copy in outs:
        copy.wait()


def column_copy(source, target, at, width, sem):
    columns = pl.ds(at, width)
    return pltpu.make_async_copy(source.at[:, columns], target.at[:, columns], sem)


def send_rows(expert_in, gain, routes_t, own, experts, chunk):
    tokens = expert_in.shape[0] // lax.axis_size("tp")
    width = expert_in.shape[1]
    return pl.pallas_call(
        partial(send_kernel, chunk * SLOTS),
        out_shape=jax.ShapeDtypeStruct((experts * SUB, LANES), BF16),
        grid_spec=pltpu.PrefetchScalarGridSpec(
            num_scalar_prefetch=1,
            grid=(1,),
            in_specs=[ANY] * 3,
            out_specs=ANY,
            scratch_shapes=[
                pltpu.VMEM((tokens, width), BF16),
                pltpu.VMEM((tokens, width), BF16),
                pltpu.VMEM((1, width), F32),
                pltpu.VMEM((K, tokens), jnp.int32),
                pltpu.VMEM((experts * SUB, LANES), BF16),
                pltpu.SemaphoreType.DMA((4,)),
                pltpu.SemaphoreType.DMA((FOLD,)),
            ],
        ),
        cost_estimate=pl.CostEstimate(flops=2_000_000_000, bytes_accessed=2_100_000, transcendentals=128),
        name="send_rows",
    )(own, expert_in, gain.reshape(1, width), routes_t)


def places(shape, dense_axis, where):
    dense = lax.broadcasted_iota(jnp.int32, shape, dense_axis)
    row = lax.broadcasted_iota(jnp.int32, shape, 1 - dense_axis)
    return as_bf16((dense % EXPERTS_G == row // SUB) & where(row % SUB, dense // EXPERTS_G))


def main_maps(shape, dense_axis):
    return [places(shape, dense_axis, lambda sub, slot, h=h: main_place(sub, slot, h)) for h in range(2)]


def tail_maps(shape, dense_axis, c):
    return [
        places(shape, dense_axis, lambda sub, slot, u=u: tail_place(sub, slot, u, c))
        for u in range(2)
        if tail_used(u, c)
    ]


def dense_columns(c):
    starts = [h * LANES + c * PIECE for h in range(2)]
    return starts + [MAIN + u * PIECE for u in range(2) if tail_used(u, c)]


def unpack(x_ref, out_ref):
    experts = x_ref.shape[0] // SUB
    mains = main_maps((DENSE, GROUP), 0)
    tails = {}

    def put(block, g, start):
        for k in range(SLOTS):
            to = k * experts + g * EXPERTS_G
            out_ref[to : to + EXPERTS_G, start : start + PIECE] = block[
                k * EXPERTS_G : (k + 1) * EXPERTS_G
            ].astype(BF16)

    for c in range(FOLD):
        maps = jnp.concatenate(mains + tail_maps((DENSE, GROUP), 0, c), axis=0)
        for g in range(experts // EXPERTS_G):
            found = dot(maps, x_ref[g * GROUP : (g + 1) * GROUP, c * PIECE : (c + 1) * PIECE])
            for n, start in enumerate(dense_columns(c)):
                block = found[n * DENSE : (n + 1) * DENSE]
                if start < MAIN:
                    put(block, g, start)
                else:
                    tails[start, g] = tails[start, g] + block if (start, g) in tails else block
    for (start, g), block in tails.items():
        put(block, g, start)


def pack_kernel(a_ref, b_ref, out_hbm, out_ref, sems):
    copies = []
    experts = out_ref.shape[0] // SUB
    mains = main_maps((GROUP, DENSE), 1)
    for c in range(FOLD):
        maps = jnp.concatenate(mains + tail_maps((GROUP, DENSE), 1, c), axis=1)
        for g in range(experts // EXPERTS_G):
            pieces = []
            for start in dense_columns(c):
                columns = slice(start, start + PIECE)
                for k in range(SLOTS):
                    to = k * experts + g * EXPERTS_G
                    here = slice(to, to + EXPERTS_G)
                    pieces.append(
                        (a_ref[here, columns].astype(F32) + b_ref[here, columns].astype(F32)).astype(BF16)
                    )
            out_ref[g * GROUP : (g + 1) * GROUP, c * PIECE : (c + 1) * PIECE] = dot(
                maps, jnp.concatenate(pieces, axis=0)
            ).astype(BF16)
        copies.append(column_copy(out_ref, out_hbm, c * PIECE, PIECE, sems.at[c]))
        copies[-1].start()
    for copy in copies:
        copy.wait()


def pack_sum(a, b):
    rows = a.shape[0] // SLOTS * SUB
    return pl.pallas_call(
        pack_kernel,
        out_shape=jax.ShapeDtypeStruct((rows, LANES), BF16),
        in_specs=[VMEM] * 2,
        out_specs=ANY,
        scratch_shapes=[pltpu.VMEM((rows, LANES), BF16), pltpu.SemaphoreType.DMA((FOLD,))],
        cost_estimate=pl.CostEstimate(flops=800_000_000, bytes_accessed=a.size * 6, transcendentals=0),
        compiler_params=pltpu.CompilerParams(vmem_limit_bytes=SMALL),
        name="pack_sum",
    )(a, b)


def ffn_kernel(*refs):
    sources, out_ref, dense_ref, held, sems = refs[:7], refs[7], refs[8], refs[9:16], refs[16]
    rows, *copies = [
        pltpu.make_async_copy(source, ref, sems.at[n])
        for n, (source, ref) in enumerate(zip(sources, held))
    ]
    rows.start()
    for copy in copies[:2]:
        copy.start()
    x_ref, ga_ref, ua_ref, gb_ref, ub_ref, da_ref, db_ref = held
    rows.wait()
    for copy in copies[2:4]:
        copy.start()
    unpack(x_ref, dense_ref)
    x = dense_ref[...]
    copies[0].wait()
    copies[1].wait()
    for copy in copies[4:]:
        copy.start()
    hidden_a = (jax.nn.silu(dot(x, ga_ref[...])) * dot(x, ua_ref[...])).astype(BF16)
    copies[2].wait()
    copies[3].wait()
    hidden_b = (jax.nn.silu(dot(x, gb_ref[...])) * dot(x, ub_ref[...])).astype(BF16)
    copies[4].wait()
    copies[5].wait()
    step = 2 * PIECE
    for c in range(WIDTH // step):
        columns = slice(c * step, (c + 1) * step)
        out_ref[:, columns] = (
            dot(hidden_a, da_ref[:, columns]) + dot(hidden_b, db_ref[:, columns])
        ).astype(BF16)


def half_ffn(x, ga, gb, ua, ub, da, db):
    operands = (x, ga, ua, gb, ub, da, db)
    dense = x.shape[0] // SUB * SLOTS
    hidden = ga.shape[1] + gb.shape[1]
    return pl.pallas_call(
        ffn_kernel,
        out_shape=jax.ShapeDtypeStruct((dense, WIDTH), BF16),
        in_specs=[ANY] * 7,
        out_specs=VMEM,
        scratch_shapes=[pltpu.VMEM((dense, WIDTH), BF16)]
        + [pltpu.VMEM(operand.shape, BF16) for operand in operands]
        + [pltpu.SemaphoreType.DMA((7,))],
        cost_estimate=pl.CostEstimate(
            flops=3_500_000_000,
            bytes_accessed=x.size * 4 + 6 * ga.size * 2,
            transcendentals=dense * hidden,
        ),
        compiler_params=pltpu.CompilerParams(vmem_limit_bytes=LARGE),
        name="half_ffn",
    )(*operands)


def combine_kernel(base, own_ref, values_ref, routes_ref, weight_ref, *refs):
    del own_ref
    copy = None
    if base:
        source, out_ref, before_ref, sem = refs
        copy = pltpu.make_async_copy(source, before_ref, sem)
        copy.start()
    else:
        (out_ref,) = refs
    rows, tokens = values_ref.shape[0], out_ref.shape[0]
    routes = jnp.transpose(routes_ref[...].astype(F32)).astype(jnp.int32)
    weights = jnp.transpose(weight_ref[...])
    row = lax.broadcasted_iota(jnp.int32, (tokens, rows), 1)
    expert, sub = row // SUB, row % SUB
    by_first, by_second = expert == routes[:, 0:1], expert == routes[:, 1:2]
    named = by_first | by_second
    earlier = lax.broadcasted_iota(jnp.int32, (tokens, tokens), 1) < lax.broadcasted_iota(
        jnp.int32, (tokens, tokens), 0
    )
    slot = dot(as_bf16(earlier), as_bf16(named)).astype(jnp.int32) - base
    weight = jnp.where(
        named & (slot < SLOTS), jnp.where(by_first, weights[:, 0:1], weights[:, 1:2]), 0.0
    )
    high = weight.astype(BF16).astype(F32)
    low = weight - high

    def split(chosen):
        return [jnp.where(chosen, part, 0.0).astype(BF16) for part in (high, low)]

    totals = {}
    mains = [part for h in range(2) for part in split(main_place(sub, slot, h))]
    for c in range(FOLD):
        maps = list(mains)
        for u in range(2):
            if tail_used(u, c):
                maps += split(tail_place(sub, slot, u, c))
        found = dot(jnp.concatenate(maps, axis=0), values_ref[:, c * PIECE : (c + 1) * PIECE])
        for n, start in enumerate(dense_columns(c)):
            block = found[2 * n * tokens : (2 * n + 1) * tokens] + found[(2 * n + 1) * tokens : (2 * n + 2) * tokens]
            totals[start] = totals[start] + block if start in totals else block
    if copy is not None:
        copy.wait()
    for start, total in totals.items():
        columns = slice(start, start + PIECE)
        if copy is not None:
            total += before_ref[:, columns]
        out_ref[:, columns] = total.astype(out_ref.dtype)


def combine(chunk, values, routes_t, weight_t, own, tokens, before=None):
    rest = () if before is None else (before,)
    return pl.pallas_call(
        partial(combine_kernel, chunk * SLOTS),
        out_shape=jax.ShapeDtypeStruct((tokens, WIDTH), F32 if before is None else BF16),
        grid_spec=pltpu.PrefetchScalarGridSpec(
            num_scalar_prefetch=1,
            grid=(1,),
            in_specs=[
                VMEM,
                pl.BlockSpec((K, tokens), lambda i, own: (0, own[0])),
                pl.BlockSpec((K, tokens), lambda i, own: (0, own[0])),
            ]
            + [ANY] * len(rest),
            out_specs=VMEM if before is None else pl.BlockSpec((tokens, WIDTH), lambda i, own: (0, 0)),
            scratch_shapes=[pltpu.VMEM((tokens, WIDTH), F32), pltpu.SemaphoreType.DMA] if rest else [],
        ),
        cost_estimate=pl.CostEstimate(flops=1_500_000_000, bytes_accessed=2_100_000, transcendentals=0),
        compiler_params=pltpu.CompilerParams(vmem_limit_bytes=LARGE),
        name="combine",
    )(own, values, routes_t, weight_t, *rest)


def exchanged(rows):
    experts = rows.shape[0] // SUB
    out = lax.all_to_all(
        rows.reshape(experts, SUB, LANES), "ep", split_axis=0, concat_axis=0, tiled=True
    )
    return out.reshape(rows.shape)


def on_device(
    pool_in,
    w_pool,
    pool_scale,
    w_out,
    expert_in,
    ffn_gain,
    routes,
    route_weight,
    w_gate,
    w_up,
    w_down,
):
    rows_here = pool_in.shape[0]
    tokens = routes.shape[0] // lax.axis_size("tp")
    experts = lax.axis_size("ep") * w_gate.shape[0]
    own = lax.axis_index("tp").astype(jnp.int32).reshape(1)
    routes_t, weight_t = routes.T, route_weight.T
    before = passed_along(pool_in[rows_here - (WMAX - 1) :], ("ep", "tp"), 1)

    gate, up, down = w_gate[0], w_up[0], w_down[0]
    gate_b = swapped(gate, 0)
    up_b = swapped(up, 0)
    down_b = swapped(down, 0)
    ffn = lambda x: half_ffn(x, gate, gate_b, up, up_b, down, down_b)

    mine = []
    for n in range(CHUNKS):
        sent = send_rows(expert_in, ffn_gain, routes_t, own, experts, n)
        mine.append(exchanged(sent))
    expert_out = None
    for n in range(CHUNKS):
        theirs = swapped(mine[n], 1)
        partial_sum = ffn(theirs)
        back = swapped(partial_sum, 1)
        kept = ffn(mine[n])
        results = pack_sum(kept, back)
        returned = exchanged(results)
        expert_out = combine(n, returned, routes_t, weight_t, own, tokens, expert_out)

    extended = jnp.concatenate([before, pool_in], axis=0).astype(F32)
    positions = (
        lax.axis_index(("ep", "tp")) * rows_here + jnp.arange(rows_here)
    ).astype(F32)
    pooled = pooled_rows(extended, positions)
    group_count = w_pool.shape[0]
    grouped = jnp.einsum(
        "tgc,gcd->tgd",
        pooled.reshape(rows_here, group_count, GDIM),
        w_pool,
        preferred_element_type=F32,
    )
    scaled = (grouped.reshape(rows_here, -1) * pool_scale).astype(BF16)
    mixer_out = dot(scaled, w_out).astype(BF16)
    return (mixer_out, expert_out)


def solution(mesh):
    placed = (
        P(("ep", "tp"), None),
        P(),
        P(),
        P(),
        P("ep", None),
        P(),
        P("ep", None),
        P("ep", None),
        P("ep", None, "tp"),
        P("ep", None, "tp"),
        P("ep", "tp", None),
    )
    return jax.shard_map(
        on_device,
        mesh=mesh,
        in_specs=placed,
        out_specs=(P(("ep", "tp"), None), P(("ep", "tp"), None)),
        check_vma=False,
    )
```

```python
from functools import partial

import jax
import jax.numpy as jnp
from jax import lax
from jax.experimental import pallas as pl
from jax.experimental.pallas import tpu as pltpu
from jax.sharding import PartitionSpec as P


GDIM = 128
WMAX = 16
K = 2
EPS = 0.05

CHUNKS = 2
SLOTS = 3
SUB = 8
LANES = 768
PIECE = 256
FOLD = LANES // PIECE
MAIN = 2 * LANES
WIDTH = MAIN + 2 * PIECE
EXPERTS_G = 32
GROUP = EXPERTS_G * SUB
DENSE = EXPERTS_G * SLOTS
SMALL = 16 * 1024 * 1024
LARGE = 52 * 1024 * 1024
BF16 = jnp.bfloat16
F32 = jnp.float32
VMEM = pl.BlockSpec(memory_space=pltpu.VMEM)
ANY = pl.BlockSpec(memory_space=pl.ANY)


def passed_along(array, axis, by):
    length = lax.axis_size(axis)
    pairs = [(i, i + by) for i in range(length) if 0 <= i + by < length]
    return lax.ppermute(array, axis, pairs)


def swapped(array, flip):
    eps, tps = lax.axis_size("ep"), lax.axis_size("tp")
    pairs = []
    for e in range(eps):
        for y in range(tps):
            other = y ^ 1 if (e + flip) % 2 == 0 else tps - 1 - y
            pairs.append((e * tps + y, e * tps + other))
    return lax.ppermute(array, ("ep", "tp"), pairs)


def window_sizes(width):
    group_of = jnp.arange(width) // GDIM
    level = group_of % 4
    return jnp.where(
        level == 0, 2.0, jnp.where(level == 1, 4.0, jnp.where(level == 2, 8.0, 16.0))
    ).astype(F32)


def pooled_rows(extended, positions):
    extent = extended.shape[0] - (WMAX - 1)
    window = window_sizes(extended.shape[1])
    running = jnp.zeros((extent, extended.shape[1]), F32)
    picked = running
    for offset in range(WMAX):
        running = running + extended[WMAX - 1 - offset : WMAX - 1 - offset + extent]
        if offset + 1 in (2, 4, 8, 16):
            picked = jnp.where(window[None, :] == offset + 1, running, picked)
    counted = jnp.minimum(positions[:, None] + 1.0, window[None, :])
    return (picked / counted - extended[WMAX - 1 :]).astype(BF16)


def as_bf16(mask):
    return mask.astype(F32).astype(BF16)


def dot(a, b):
    return jnp.dot(a, b, preferred_element_type=F32)


def slot_ranks(routes_ref, rows, tokens, base):
    first, second = routes_ref[0:1, :], routes_ref[1:2, :]
    row = lax.broadcasted_iota(jnp.int32, (rows, tokens), 0)
    expert, sub = row // SUB, row % SUB
    by_first, by_second = expert == first, expert == second
    named = by_first | by_second
    before = lax.broadcasted_iota(jnp.int32, (tokens, tokens), 0) < lax.broadcasted_iota(
        jnp.int32, (tokens, tokens), 1
    )
    rank = dot(as_bf16(named), as_bf16(before)).astype(jnp.int32) - base
    return by_first, named, rank, sub


def main_place(sub, slot, half):
    return (sub == 2 * slot + half) & (sub < 2 * SLOTS) & (slot >= 0)


def tail_place(sub, slot, piece, c):
    return (sub >= 2 * SLOTS) & ((sub - 2 * SLOTS) * FOLD + c == 2 * slot + piece) & (slot >= 0)


def tail_used(piece, c):
    return any((r * FOLD + c - piece) % 2 == 0 for r in range(SUB - 2 * SLOTS))


def send_kernel(
    base,
    own_ref,
    rows_hbm,
    gain_hbm,
    routes_hbm,
    out_hbm,
    rows_ref,
    normed_ref,
    gain_ref,
    routes_ref,
    out_ref,
    sems,
    out_sems,
):
    tokens = rows_ref.shape[0]
    half = tokens // 2
    first = pl.multiple_of(own_ref[0] * tokens, tokens)
    fetches = [
        pltpu.make_async_copy(routes_hbm.at[:, pl.ds(first, tokens)], routes_ref, sems.at[2]),
        pltpu.make_async_copy(gain_hbm, gain_ref, sems.at[3]),
    ]
    halves = [
        pltpu.make_async_copy(
            rows_hbm.at[pl.ds(pl.multiple_of(first + n * half, half), half)],
            rows_ref.at[pl.ds(n * half, half)],
            sems.at[n],
        )
        for n in range(2)
    ]
    for copy in fetches + halves:
        copy.start()
    fetches[0].wait()
    _, named, rank, sub = slot_ranks(routes_ref, out_ref.shape[0], tokens, base)
    mains = jnp.concatenate([as_bf16(named & main_place(sub, rank, h)) for h in range(2)], axis=1)
    fetches[1].wait()
    for n in range(2):
        here = slice(n * half, (n + 1) * half)
        halves[n].wait()
        features = rows_ref[here, :].astype(F32)
        inverse = lax.rsqrt(jnp.mean(features * features, axis=-1, keepdims=True) + EPS)
        normed_ref[here, :] = (features * inverse * gain_ref[...]).astype(BF16)
    outs = []
    for c in range(FOLD):
        used = [u for u in range(2) if tail_used(u, c)]
        tails = [as_bf16(named & tail_place(sub, rank, u, c)) for u in used]
        starts = [h * LANES + c * PIECE for h in range(2)] + [MAIN + u * PIECE for u in used]
        out_ref[:, c * PIECE : (c + 1) * PIECE] = dot(
            jnp.concatenate([mains, *tails], axis=1),
            jnp.concatenate([normed_ref[:, start : start + PIECE] for start in starts], axis=0),
        ).astype(BF16)
        outs.append(column_copy(out_ref, out_hbm, c * PIECE, PIECE, out_sems.at[c]))
        outs[-1].start()
    for copy in outs:
        copy.wait()


def column_copy(source, target, at, width, sem):
    columns = pl.ds(at, width)
    return pltpu.make_async_copy(source.at[:, columns], target.at[:, columns], sem)


def send_rows(expert_in, gain, routes_t, own, experts, chunk):
    tokens = expert_in.shape[0] // lax.axis_size("tp")
    width = expert_in.shape[1]
    return pl.pallas_call(
        partial(send_kernel, chunk * SLOTS),
        out_shape=jax.ShapeDtypeStruct((experts * SUB, LANES), BF16),
        grid_spec=pltpu.PrefetchScalarGridSpec(
            num_scalar_prefetch=1,
            grid=(1,),
            in_specs=[ANY] * 3,
            out_specs=ANY,
            scratch_shapes=[
                pltpu.VMEM((tokens, width), BF16),
                pltpu.VMEM((tokens, width), BF16),
                pltpu.VMEM((1, width), F32),
                pltpu.VMEM((K, tokens), jnp.int32),
                pltpu.VMEM((experts * SUB, LANES), BF16),
                pltpu.SemaphoreType.DMA((4,)),
                pltpu.SemaphoreType.DMA((FOLD,)),
            ],
        ),
        cost_estimate=pl.CostEstimate(flops=2_000_000_000, bytes_accessed=2_100_000, transcendentals=128),
        name="send_rows",
    )(own, expert_in, gain.reshape(1, width), routes_t)


def places(shape, dense_axis, where):
    dense = lax.broadcasted_iota(jnp.int32, shape, dense_axis)
    row = lax.broadcasted_iota(jnp.int32, shape, 1 - dense_axis)
    return as_bf16((dense % EXPERTS_G == row // SUB) & where(row % SUB, dense // EXPERTS_G))


def main_maps(shape, dense_axis):
    return [places(shape, dense_axis, lambda sub, slot, h=h: main_place(sub, slot, h)) for h in range(2)]


def tail_maps(shape, dense_axis, c):
    return [
        places(shape, dense_axis, lambda sub, slot, u=u: tail_place(sub, slot, u, c))
        for u in range(2)
        if tail_used(u, c)
    ]


def dense_columns(c):
    starts = [h * LANES + c * PIECE for h in range(2)]
    return starts + [MAIN + u * PIECE for u in range(2) if tail_used(u, c)]


def unpack(x_ref, out_ref):
    experts = x_ref.shape[0] // SUB
    mains = main_maps((DENSE, GROUP), 0)
    tails = {}

    def put(block, g, start):
        for k in range(SLOTS):
            to = k * experts + g * EXPERTS_G
            out_ref[to : to + EXPERTS_G, start : start + PIECE] = block[
                k * EXPERTS_G : (k + 1) * EXPERTS_G
            ].astype(BF16)

    for c in range(FOLD):
        maps = jnp.concatenate(mains + tail_maps((DENSE, GROUP), 0, c), axis=0)
        for g in range(experts // EXPERTS_G):
            found = dot(maps, x_ref[g * GROUP : (g + 1) * GROUP, c * PIECE : (c + 1) * PIECE])
            for n, start in enumerate(dense_columns(c)):
                block = found[n * DENSE : (n + 1) * DENSE]
                if start < MAIN:
                    put(block, g, start)
                else:
                    tails[start, g] = tails[start, g] + block if (start, g) in tails else block
    for (start, g), block in tails.items():
        put(block, g, start)


def pack_kernel(a_ref, b_ref, out_hbm, out_ref, sems):
    copies = []
    experts = out_ref.shape[0] // SUB
    mains = main_maps((GROUP, DENSE), 1)
    for c in range(FOLD):
        maps = jnp.concatenate(mains + tail_maps((GROUP, DENSE), 1, c), axis=1)
        for g in range(experts // EXPERTS_G):
            pieces = []
            for start in dense_columns(c):
                columns = slice(start, start + PIECE)
                for k in range(SLOTS):
                    to = k * experts + g * EXPERTS_G
                    here = slice(to, to + EXPERTS_G)
                    pieces.append(
                        (a_ref[here, columns].astype(F32) + b_ref[here, columns].astype(F32)).astype(BF16)
                    )
            out_ref[g * GROUP : (g + 1) * GROUP, c * PIECE : (c + 1) * PIECE] = dot(
                maps, jnp.concatenate(pieces, axis=0)
            ).astype(BF16)
        copies.append(column_copy(out_ref, out_hbm, c * PIECE, PIECE, sems.at[c]))
        copies[-1].start()
    for copy in copies:
        copy.wait()


def pack_sum(a, b):
    rows = a.shape[0] // SLOTS * SUB
    return pl.pallas_call(
        pack_kernel,
        out_shape=jax.ShapeDtypeStruct((rows, LANES), BF16),
        in_specs=[VMEM] * 2,
        out_specs=ANY,
        scratch_shapes=[pltpu.VMEM((rows, LANES), BF16), pltpu.SemaphoreType.DMA((FOLD,))],
        cost_estimate=pl.CostEstimate(flops=800_000_000, bytes_accessed=a.size * 6, transcendentals=0),
        compiler_params=pltpu.CompilerParams(vmem_limit_bytes=SMALL),
        name="pack_sum",
    )(a, b)


def ffn_kernel(*refs):
    sources, out_ref, dense_ref, held, sems = refs[:7], refs[7], refs[8], refs[9:16], refs[16]
    rows, *copies = [
        pltpu.make_async_copy(source, ref, sems.at[n])
        for n, (source, ref) in enumerate(zip(sources, held))
    ]
    rows.start()
    for copy in copies:
        copy.start()
    x_ref, ga_ref, ua_ref, gb_ref, ub_ref, da_ref, db_ref = held
    rows.wait()
    unpack(x_ref, dense_ref)
    x = dense_ref[...]
    copies[0].wait()
    copies[1].wait()
    hidden_a = (jax.nn.silu(dot(x, ga_ref[...])) * dot(x, ua_ref[...])).astype(BF16)
    copies[2].wait()
    copies[3].wait()
    hidden_b = (jax.nn.silu(dot(x, gb_ref[...])) * dot(x, ub_ref[...])).astype(BF16)
    copies[4].wait()
    copies[5].wait()
    step = 2 * PIECE
    for c in range(WIDTH // step):
        columns = slice(c * step, (c + 1) * step)
        out_ref[:, columns] = (
            dot(hidden_a, da_ref[:, columns]) + dot(hidden_b, db_ref[:, columns])
        ).astype(BF16)


def half_ffn(x, ga, gb, ua, ub, da, db):
    operands = (x, ga, ua, gb, ub, da, db)
    dense = x.shape[0] // SUB * SLOTS
    hidden = ga.shape[1] + gb.shape[1]
    return pl.pallas_call(
        ffn_kernel,
        out_shape=jax.ShapeDtypeStruct((dense, WIDTH), BF16),
        in_specs=[ANY] * 7,
        out_specs=VMEM,
        scratch_shapes=[pltpu.VMEM((dense, WIDTH), BF16)]
        + [pltpu.VMEM(operand.shape, BF16) for operand in operands]
        + [pltpu.SemaphoreType.DMA((7,))],
        cost_estimate=pl.CostEstimate(
            flops=3_500_000_000,
            bytes_accessed=x.size * 4 + 6 * ga.size * 2,
            transcendentals=dense * hidden,
        ),
        compiler_params=pltpu.CompilerParams(vmem_limit_bytes=LARGE),
        name="half_ffn",
    )(*operands)


def combine_kernel(base, own_ref, values_ref, routes_ref, weight_ref, *refs):
    del own_ref
    copy = None
    if base:
        source, out_ref, before_ref, sem = refs
        copy = pltpu.make_async_copy(source, before_ref, sem)
        copy.start()
    else:
        (out_ref,) = refs
    rows, tokens = values_ref.shape[0], out_ref.shape[0]
    routes = jnp.transpose(routes_ref[...].astype(F32)).astype(jnp.int32)
    weights = jnp.transpose(weight_ref[...])
    row = lax.broadcasted_iota(jnp.int32, (tokens, rows), 1)
    expert, sub = row // SUB, row % SUB
    by_first, by_second = expert == routes[:, 0:1], expert == routes[:, 1:2]
    named = by_first | by_second
    earlier = lax.broadcasted_iota(jnp.int32, (tokens, tokens), 1) < lax.broadcasted_iota(
        jnp.int32, (tokens, tokens), 0
    )
    slot = dot(as_bf16(earlier), as_bf16(named)).astype(jnp.int32) - base
    weight = jnp.where(
        named & (slot < SLOTS), jnp.where(by_first, weights[:, 0:1], weights[:, 1:2]), 0.0
    )
    high = weight.astype(BF16).astype(F32)
    low = weight - high

    def split(chosen):
        return [jnp.where(chosen, part, 0.0).astype(BF16) for part in (high, low)]

    totals = {}
    mains = [part for h in range(2) for part in split(main_place(sub, slot, h))]
    for c in range(FOLD):
        maps = list(mains)
        for u in range(2):
            if tail_used(u, c):
                maps += split(tail_place(sub, slot, u, c))
        found = dot(jnp.concatenate(maps, axis=0), values_ref[:, c * PIECE : (c + 1) * PIECE])
        for n, start in enumerate(dense_columns(c)):
            block = found[2 * n * tokens : (2 * n + 1) * tokens] + found[(2 * n + 1) * tokens : (2 * n + 2) * tokens]
            totals[start] = totals[start] + block if start in totals else block
    if copy is not None:
        copy.wait()
    for start, total in totals.items():
        columns = slice(start, start + PIECE)
        if copy is not None:
            total += before_ref[:, columns]
        out_ref[:, columns] = total.astype(out_ref.dtype)


def combine(chunk, values, routes_t, weight_t, own, tokens, before=None):
    rest = () if before is None else (before,)
    return pl.pallas_call(
        partial(combine_kernel, chunk * SLOTS),
        out_shape=jax.ShapeDtypeStruct((tokens, WIDTH), F32 if before is None else BF16),
        grid_spec=pltpu.PrefetchScalarGridSpec(
            num_scalar_prefetch=1,
            grid=(1,),
            in_specs=[
                VMEM,
                pl.BlockSpec((K, tokens), lambda i, own: (0, own[0])),
                pl.BlockSpec((K, tokens), lambda i, own: (0, own[0])),
            ]
            + [ANY] * len(rest),
            out_specs=VMEM if before is None else pl.BlockSpec((tokens, WIDTH), lambda i, own: (0, 0)),
            scratch_shapes=[pltpu.VMEM((tokens, WIDTH), F32), pltpu.SemaphoreType.DMA] if rest else [],
        ),
        cost_estimate=pl.CostEstimate(flops=1_500_000_000, bytes_accessed=2_100_000, transcendentals=0),
        compiler_params=pltpu.CompilerParams(vmem_limit_bytes=LARGE),
        name="combine",
    )(own, values, routes_t, weight_t, *rest)


def exchanged(rows):
    experts = rows.shape[0] // SUB
    out = lax.all_to_all(
        rows.reshape(experts, SUB, LANES), "ep", split_axis=0, concat_axis=0, tiled=True
    )
    return out.reshape(rows.shape)


def on_device(
    pool_in,
    w_pool,
    pool_scale,
    w_out,
    expert_in,
    ffn_gain,
    routes,
    route_weight,
    w_gate,
    w_up,
    w_down,
):
    rows_here = pool_in.shape[0]
    tokens = routes.shape[0] // lax.axis_size("tp")
    experts = lax.axis_size("ep") * w_gate.shape[0]
    own = lax.axis_index("tp").astype(jnp.int32).reshape(1)
    routes_t, weight_t = routes.T, route_weight.T
    before = passed_along(pool_in[rows_here - (WMAX - 1) :], ("ep", "tp"), 1)

    gate, up, down = w_gate[0], w_up[0], w_down[0]
    gate_b, up_b = swapped(gate, 0), swapped(up, 0)
    down_b = swapped(down, 0)
    ffn = lambda x: half_ffn(x, gate, gate_b, up, up_b, down, down_b)

    mine = []
    for n in range(CHUNKS):
        sent = send_rows(expert_in, ffn_gain, routes_t, own, experts, n)
        mine.append(exchanged(sent))
    expert_out = None
    for n in range(CHUNKS):
        theirs = swapped(mine[n], 1)
        partial_sum = ffn(theirs)
        back = swapped(partial_sum, 1)
        kept = ffn(mine[n])
        results = pack_sum(kept, back)
        returned = exchanged(results)
        expert_out = combine(n, returned, routes_t, weight_t, own, tokens, expert_out)

    extended = jnp.concatenate([before, pool_in], axis=0).astype(F32)
    positions = (
        lax.axis_index(("ep", "tp")) * rows_here + jnp.arange(rows_here)
    ).astype(F32)
    pooled = pooled_rows(extended, positions)
    group_count = w_pool.shape[0]
    grouped = jnp.einsum(
        "tgc,gcd->tgd",
        pooled.reshape(rows_here, group_count, GDIM),
        w_pool,
        preferred_element_type=F32,
    )
    scaled = (grouped.reshape(rows_here, -1) * pool_scale).astype(BF16)
    mixer_out = dot(scaled, w_out).astype(BF16)
    return (mixer_out, expert_out)


def solution(mesh):
    placed = (
        P(("ep", "tp"), None),
        P(),
        P(),
        P(),
        P("ep", None),
        P(),
        P("ep", None),
        P("ep", None),
        P("ep", None, "tp"),
        P("ep", None, "tp"),
        P("ep", "tp", None),
    )
    return jax.shard_map(
        on_device,
        mesh=mesh,
        in_specs=placed,
        out_specs=(P(("ep", "tp"), None), P(("ep", "tp"), None)),
        check_vma=False,
    )
```

```python
from functools import partial

import jax
import jax.numpy as jnp
from jax import lax
from jax.experimental import pallas as pl
from jax.experimental.pallas import tpu as pltpu
from jax.sharding import PartitionSpec as P


GDIM = 128
WMAX = 16
K = 2
EPS = 0.05

CHUNKS = 2
SLOTS = 3
SUB = 8
LANES = 768
PIECE = 256
FOLD = LANES // PIECE
MAIN = 2 * LANES
WIDTH = MAIN + 2 * PIECE
EXPERTS_G = 32
GROUP = EXPERTS_G * SUB
DENSE = EXPERTS_G * SLOTS
SMALL = 16 * 1024 * 1024
LARGE = 52 * 1024 * 1024
BF16 = jnp.bfloat16
F32 = jnp.float32
VMEM = pl.BlockSpec(memory_space=pltpu.VMEM)
ANY = pl.BlockSpec(memory_space=pl.ANY)


def passed_along(array, axis, by):
    length = lax.axis_size(axis)
    pairs = [(i, i + by) for i in range(length) if 0 <= i + by < length]
    return lax.ppermute(array, axis, pairs)


def swapped(array, flip):
    eps, tps = lax.axis_size("ep"), lax.axis_size("tp")
    pairs = []
    for e in range(eps):
        for y in range(tps):
            other = y ^ 1 if (e + flip) % 2 == 0 else tps - 1 - y
            pairs.append((e * tps + y, e * tps + other))
    return lax.ppermute(array, ("ep", "tp"), pairs)


def window_sizes(width):
    group_of = jnp.arange(width) // GDIM
    level = group_of % 4
    return jnp.where(
        level == 0, 2.0, jnp.where(level == 1, 4.0, jnp.where(level == 2, 8.0, 16.0))
    ).astype(F32)


def pooled_rows(extended, positions):
    extent = extended.shape[0] - (WMAX - 1)
    window = window_sizes(extended.shape[1])
    running = jnp.zeros((extent, extended.shape[1]), F32)
    picked = running
    for offset in range(WMAX):
        running = running + extended[WMAX - 1 - offset : WMAX - 1 - offset + extent]
        if offset + 1 in (2, 4, 8, 16):
            picked = jnp.where(window[None, :] == offset + 1, running, picked)
    counted = jnp.minimum(positions[:, None] + 1.0, window[None, :])
    return (picked / counted - extended[WMAX - 1 :]).astype(BF16)


def as_bf16(mask):
    return mask.astype(F32).astype(BF16)


def dot(a, b):
    return jnp.dot(a, b, preferred_element_type=F32)


def slot_ranks(routes_ref, rows, tokens, base):
    first, second = routes_ref[0:1, :], routes_ref[1:2, :]
    row = lax.broadcasted_iota(jnp.int32, (rows, tokens), 0)
    expert, sub = row // SUB, row % SUB
    by_first, by_second = expert == first, expert == second
    named = by_first | by_second
    before = lax.broadcasted_iota(jnp.int32, (tokens, tokens), 0) < lax.broadcasted_iota(
        jnp.int32, (tokens, tokens), 1
    )
    rank = dot(as_bf16(named), as_bf16(before)).astype(jnp.int32) - base
    return by_first, named, rank, sub


def main_place(sub, slot, half):
    return (sub == 2 * slot + half) & (sub < 2 * SLOTS) & (slot >= 0)


def tail_place(sub, slot, piece, c):
    return (sub >= 2 * SLOTS) & ((sub - 2 * SLOTS) * FOLD + c == 2 * slot + piece) & (slot >= 0)


def tail_used(piece, c):
    return any((r * FOLD + c - piece) % 2 == 0 for r in range(SUB - 2 * SLOTS))


def send_kernel(
    base,
    own_ref,
    rows_hbm,
    gain_hbm,
    routes_hbm,
    out_hbm,
    rows_ref,
    normed_ref,
    gain_ref,
    routes_ref,
    out_ref,
    sems,
    out_sems,
):
    tokens = rows_ref.shape[0]
    half = tokens // 2
    first = pl.multiple_of(own_ref[0] * tokens, tokens)
    fetches = [
        pltpu.make_async_copy(routes_hbm.at[:, pl.ds(first, tokens)], routes_ref, sems.at[2]),
        pltpu.make_async_copy(gain_hbm, gain_ref, sems.at[3]),
    ]
    halves = [
        pltpu.make_async_copy(
            rows_hbm.at[pl.ds(pl.multiple_of(first + n * half, half), half)],
            rows_ref.at[pl.ds(n * half, half)],
            sems.at[n],
        )
        for n in range(2)
    ]
    for copy in fetches + halves:
        copy.start()
    fetches[0].wait()
    _, named, rank, sub = slot_ranks(routes_ref, out_ref.shape[0], tokens, base)
    mains = jnp.concatenate([as_bf16(named & main_place(sub, rank, h)) for h in range(2)], axis=1)
    fetches[1].wait()
    for n in range(2):
        here = slice(n * half, (n + 1) * half)
        halves[n].wait()
        features = rows_ref[here, :].astype(F32)
        inverse = lax.rsqrt(jnp.mean(features * features, axis=-1, keepdims=True) + EPS)
        normed_ref[here, :] = (features * inverse * gain_ref[...]).astype(BF16)
    outs = []
    for c in range(FOLD):
        used = [u for u in range(2) if tail_used(u, c)]
        tails = [as_bf16(named & tail_place(sub, rank, u, c)) for u in used]
        starts = [h * LANES + c * PIECE for h in range(2)] + [MAIN + u * PIECE for u in used]
        out_ref[:, c * PIECE : (c + 1) * PIECE] = dot(
            jnp.concatenate([mains, *tails], axis=1),
            jnp.concatenate([normed_ref[:, start : start + PIECE] for start in starts], axis=0),
        ).astype(BF16)
        outs.append(column_copy(out_ref, out_hbm, c * PIECE, PIECE, out_sems.at[c]))
        outs[-1].start()
    for copy in outs:
        copy.wait()


def column_copy(source, target, at, width, sem):
    columns = pl.ds(at, width)
    return pltpu.make_async_copy(source.at[:, columns], target.at[:, columns], sem)


def send_rows(expert_in, gain, routes_t, own, experts, chunk):
    tokens = expert_in.shape[0] // lax.axis_size("tp")
    width = expert_in.shape[1]
    return pl.pallas_call(
        partial(send_kernel, chunk * SLOTS),
        out_shape=jax.ShapeDtypeStruct((experts * SUB, LANES), BF16),
        grid_spec=pltpu.PrefetchScalarGridSpec(
            num_scalar_prefetch=1,
            grid=(1,),
            in_specs=[ANY] * 3,
            out_specs=ANY,
            scratch_shapes=[
                pltpu.VMEM((tokens, width), BF16),
                pltpu.VMEM((tokens, width), BF16),
                pltpu.VMEM((1, width), F32),
                pltpu.VMEM((K, tokens), jnp.int32),
                pltpu.VMEM((experts * SUB, LANES), BF16),
                pltpu.SemaphoreType.DMA((4,)),
                pltpu.SemaphoreType.DMA((FOLD,)),
            ],
        ),
        cost_estimate=pl.CostEstimate(flops=2_000_000_000, bytes_accessed=2_100_000, transcendentals=128),
        name="send_rows",
    )(own, expert_in, gain.reshape(1, width), routes_t)


def places(shape, dense_axis, where):
    dense = lax.broadcasted_iota(jnp.int32, shape, dense_axis)
    row = lax.broadcasted_iota(jnp.int32, shape, 1 - dense_axis)
    return as_bf16((dense % EXPERTS_G == row // SUB) & where(row % SUB, dense // EXPERTS_G))


def main_maps(shape, dense_axis):
    return [places(shape, dense_axis, lambda sub, slot, h=h: main_place(sub, slot, h)) for h in range(2)]


def tail_maps(shape, dense_axis, c):
    return [
        places(shape, dense_axis, lambda sub, slot, u=u: tail_place(sub, slot, u, c))
        for u in range(2)
        if tail_used(u, c)
    ]


def dense_columns(c):
    starts = [h * LANES + c * PIECE for h in range(2)]
    return starts + [MAIN + u * PIECE for u in range(2) if tail_used(u, c)]


def unpack(x_ref, out_ref):
    experts = x_ref.shape[0] // SUB
    mains = main_maps((DENSE, GROUP), 0)
    tails = {}

    def put(block, g, start):
        for k in range(SLOTS):
            to = k * experts + g * EXPERTS_G
            out_ref[to : to + EXPERTS_G, start : start + PIECE] = block[
                k * EXPERTS_G : (k + 1) * EXPERTS_G
            ].astype(BF16)

    for c in range(FOLD):
        maps = jnp.concatenate(mains + tail_maps((DENSE, GROUP), 0, c), axis=0)
        for g in range(experts // EXPERTS_G):
            found = dot(maps, x_ref[g * GROUP : (g + 1) * GROUP, c * PIECE : (c + 1) * PIECE])
            for n, start in enumerate(dense_columns(c)):
                block = found[n * DENSE : (n + 1) * DENSE]
                if start < MAIN:
                    put(block, g, start)
                else:
                    tails[start, g] = tails[start, g] + block if (start, g) in tails else block
    for (start, g), block in tails.items():
        put(block, g, start)


def pack_kernel(a_ref, b_ref, out_hbm, out_ref, sems):
    copies = []
    experts = out_ref.shape[0] // SUB
    mains = main_maps((GROUP, DENSE), 1)
    for c in range(FOLD):
        maps = jnp.concatenate(mains + tail_maps((GROUP, DENSE), 1, c), axis=1)
        for g in range(experts // EXPERTS_G):
            pieces = []
            for start in dense_columns(c):
                columns = slice(start, start + PIECE)
                for k in range(SLOTS):
                    to = k * experts + g * EXPERTS_G
                    here = slice(to, to + EXPERTS_G)
                    pieces.append(
                        (a_ref[here, columns].astype(F32) + b_ref[here, columns].astype(F32)).astype(BF16)
                    )
            out_ref[g * GROUP : (g + 1) * GROUP, c * PIECE : (c + 1) * PIECE] = dot(
                maps, jnp.concatenate(pieces, axis=0)
            ).astype(BF16)
        copies.append(column_copy(out_ref, out_hbm, c * PIECE, PIECE, sems.at[c]))
        copies[-1].start()
    for copy in copies:
        copy.wait()


def pack_sum(a, b):
    rows = a.shape[0] // SLOTS * SUB
    return pl.pallas_call(
        pack_kernel,
        out_shape=jax.ShapeDtypeStruct((rows, LANES), BF16),
        in_specs=[VMEM] * 2,
        out_specs=ANY,
        scratch_shapes=[pltpu.VMEM((rows, LANES), BF16), pltpu.SemaphoreType.DMA((FOLD,))],
        cost_estimate=pl.CostEstimate(flops=800_000_000, bytes_accessed=a.size * 6, transcendentals=0),
        compiler_params=pltpu.CompilerParams(vmem_limit_bytes=SMALL),
        name="pack_sum",
    )(a, b)


def ffn_kernel(*refs):
    sources, out_ref, dense_ref, held, sems = refs[:7], refs[7], refs[8], refs[9:16], refs[16]

    def fetch(n, source, ref):
        half = source.shape[0] // 2
        return [
            pltpu.make_async_copy(
                source.at[pl.ds(part * half, half)], ref.at[pl.ds(part * half, half)], sems.at[2 * n + part]
            )
            for part in range(2)
        ]

    rows, *copies = [fetch(n, *pair) for n, pair in enumerate(zip(sources, held))]
    for part in rows:
        part.start()
    for copy in copies:
        for part in copy:
            part.start()
    x_ref, ga_ref, ua_ref, gb_ref, ub_ref, da_ref, db_ref = held
    for part in rows:
        part.wait()
    unpack(x_ref, dense_ref)
    x = dense_ref[...]
    for part in copies[0]:
        part.wait()
    for part in copies[1]:
        part.wait()
    hidden_a = (jax.nn.silu(dot(x, ga_ref[...])) * dot(x, ua_ref[...])).astype(BF16)
    for part in copies[2]:
        part.wait()
    for part in copies[3]:
        part.wait()
    hidden_b = (jax.nn.silu(dot(x, gb_ref[...])) * dot(x, ub_ref[...])).astype(BF16)
    for part in copies[4]:
        part.wait()
    for part in copies[5]:
        part.wait()
    step = 2 * PIECE
    for c in range(WIDTH // step):
        columns = slice(c * step, (c + 1) * step)
        out_ref[:, columns] = (
            dot(hidden_a, da_ref[:, columns]) + dot(hidden_b, db_ref[:, columns])
        ).astype(BF16)


def half_ffn(x, ga, gb, ua, ub, da, db):
    operands = (x, ga, ua, gb, ub, da, db)
    dense = x.shape[0] // SUB * SLOTS
    hidden = ga.shape[1] + gb.shape[1]
    return pl.pallas_call(
        ffn_kernel,
        out_shape=jax.ShapeDtypeStruct((dense, WIDTH), BF16),
        in_specs=[ANY] * 7,
        out_specs=VMEM,
        scratch_shapes=[pltpu.VMEM((dense, WIDTH), BF16)]
        + [pltpu.VMEM(operand.shape, BF16) for operand in operands]
        + [pltpu.SemaphoreType.DMA((14,))],
        cost_estimate=pl.CostEstimate(
            flops=3_500_000_000,
            bytes_accessed=x.size * 4 + 6 * ga.size * 2,
            transcendentals=dense * hidden,
        ),
        compiler_params=pltpu.CompilerParams(vmem_limit_bytes=LARGE),
        name="half_ffn",
    )(*operands)


def combine_kernel(base, own_ref, values_ref, routes_ref, weight_ref, *refs):
    del own_ref
    copy = None
    if base:
        source, out_ref, before_ref, sem = refs
        copy = pltpu.make_async_copy(source, before_ref, sem)
        copy.start()
    else:
        (out_ref,) = refs
    rows, tokens = values_ref.shape[0], out_ref.shape[0]
    routes = jnp.transpose(routes_ref[...].astype(F32)).astype(jnp.int32)
    weights = jnp.transpose(weight_ref[...])
    row = lax.broadcasted_iota(jnp.int32, (tokens, rows), 1)
    expert, sub = row // SUB, row % SUB
    by_first, by_second = expert == routes[:, 0:1], expert == routes[:, 1:2]
    named = by_first | by_second
    earlier = lax.broadcasted_iota(jnp.int32, (tokens, tokens), 1) < lax.broadcasted_iota(
        jnp.int32, (tokens, tokens), 0
    )
    slot = dot(as_bf16(earlier), as_bf16(named)).astype(jnp.int32) - base
    weight = jnp.where(
        named & (slot < SLOTS), jnp.where(by_first, weights[:, 0:1], weights[:, 1:2]), 0.0
    )
    high = weight.astype(BF16).astype(F32)
    low = weight - high

    def split(chosen):
        return [jnp.where(chosen, part, 0.0).astype(BF16) for part in (high, low)]

    totals = {}
    mains = [part for h in range(2) for part in split(main_place(sub, slot, h))]
    for c in range(FOLD):
        maps = list(mains)
        for u in range(2):
            if tail_used(u, c):
                maps += split(tail_place(sub, slot, u, c))
        found = dot(jnp.concatenate(maps, axis=0), values_ref[:, c * PIECE : (c + 1) * PIECE])
        for n, start in enumerate(dense_columns(c)):
            block = found[2 * n * tokens : (2 * n + 1) * tokens] + found[(2 * n + 1) * tokens : (2 * n + 2) * tokens]
            totals[start] = totals[start] + block if start in totals else block
    if copy is not None:
        copy.wait()
    for start, total in totals.items():
        columns = slice(start, start + PIECE)
        if copy is not None:
            total += before_ref[:, columns]
        out_ref[:, columns] = total.astype(out_ref.dtype)


def combine(chunk, values, routes_t, weight_t, own, tokens, before=None):
    rest = () if before is None else (before,)
    return pl.pallas_call(
        partial(combine_kernel, chunk * SLOTS),
        out_shape=jax.ShapeDtypeStruct((tokens, WIDTH), F32 if before is None else BF16),
        grid_spec=pltpu.PrefetchScalarGridSpec(
            num_scalar_prefetch=1,
            grid=(1,),
            in_specs=[
                VMEM,
                pl.BlockSpec((K, tokens), lambda i, own: (0, own[0])),
                pl.BlockSpec((K, tokens), lambda i, own: (0, own[0])),
            ]
            + [ANY] * len(rest),
            out_specs=VMEM if before is None else pl.BlockSpec((tokens, WIDTH), lambda i, own: (0, 0)),
            scratch_shapes=[pltpu.VMEM((tokens, WIDTH), F32), pltpu.SemaphoreType.DMA] if rest else [],
        ),
        cost_estimate=pl.CostEstimate(flops=1_500_000_000, bytes_accessed=2_100_000, transcendentals=0),
        compiler_params=pltpu.CompilerParams(vmem_limit_bytes=LARGE),
        name="combine",
    )(own, values, routes_t, weight_t, *rest)


def exchanged(rows):
    experts = rows.shape[0] // SUB
    out = lax.all_to_all(
        rows.reshape(experts, SUB, LANES), "ep", split_axis=0, concat_axis=0, tiled=True
    )
    return out.reshape(rows.shape)


def on_device(
    pool_in,
    w_pool,
    pool_scale,
    w_out,
    expert_in,
    ffn_gain,
    routes,
    route_weight,
    w_gate,
    w_up,
    w_down,
):
    rows_here = pool_in.shape[0]
    tokens = routes.shape[0] // lax.axis_size("tp")
    experts = lax.axis_size("ep") * w_gate.shape[0]
    own = lax.axis_index("tp").astype(jnp.int32).reshape(1)
    routes_t, weight_t = routes.T, route_weight.T
    before = passed_along(pool_in[rows_here - (WMAX - 1) :], ("ep", "tp"), 1)

    gate, up, down = w_gate[0], w_up[0], w_down[0]
    gate_b, up_b = swapped(gate, 0), swapped(up, 0)
    down_b = swapped(down, 0)
    ffn = lambda x: half_ffn(x, gate, gate_b, up, up_b, down, down_b)

    mine = []
    for n in range(CHUNKS):
        sent = send_rows(expert_in, ffn_gain, routes_t, own, experts, n)
        mine.append(exchanged(sent))
    expert_out = None
    for n in range(CHUNKS):
        theirs = swapped(mine[n], 1)
        partial_sum = ffn(theirs)
        back = swapped(partial_sum, 1)
        kept = ffn(mine[n])
        results = pack_sum(kept, back)
        returned = exchanged(results)
        expert_out = combine(n, returned, routes_t, weight_t, own, tokens, expert_out)

    extended = jnp.concatenate([before, pool_in], axis=0).astype(F32)
    positions = (
        lax.axis_index(("ep", "tp")) * rows_here + jnp.arange(rows_here)
    ).astype(F32)
    pooled = pooled_rows(extended, positions)
    group_count = w_pool.shape[0]
    grouped = jnp.einsum(
        "tgc,gcd->tgd",
        pooled.reshape(rows_here, group_count, GDIM),
        w_pool,
        preferred_element_type=F32,
    )
    scaled = (grouped.reshape(rows_here, -1) * pool_scale).astype(BF16)
    mixer_out = dot(scaled, w_out).astype(BF16)
    return (mixer_out, expert_out)


def solution(mesh):
    placed = (
        P(("ep", "tp"), None),
        P(),
        P(),
        P(),
        P("ep", None),
        P(),
        P("ep", None),
        P("ep", None),
        P("ep", None, "tp"),
        P("ep", None, "tp"),
        P("ep", "tp", None),
    )
    return jax.shard_map(
        on_device,
        mesh=mesh,
        in_specs=placed,
        out_specs=(P(("ep", "tp"), None), P(("ep", "tp"), None)),
        check_vma=False,
    )
```
